32 devices in a mesh: sp: 8 (over z, core), tp: 4 (over y, x).
Axes of the slice: x: 2, y: 2, z: 4, core: 2. Of those that a mesh axis runs over, the one named last changes fastest.
Arguments:
- query_major: bfloat16 [1024, 3072], P('sp', 'tp'), may hold values from -256 to 256
- query_minor: bfloat16 [1024, 2048], P('sp', 'tp'), may hold values from -256 to 256
- latent_rows: bfloat16 [1024, 512], P('sp'), may hold values from -6 to 6
- rope_keys: bfloat16 [1024, 64], P('sp'), may hold values from -4 to 4
- key_up_major: bfloat16 [512, 2048], P(None, 'tp'), may hold values from -0.25 to 0.25
- value_up_major: bfloat16 [512, 2048], P(None, 'tp'), may hold values from -0.25 to 0.25
- key_up_minor: bfloat16 [512, 1024], P(None, 'tp'), may hold values from -0.25 to 0.25
- value_up_minor: bfloat16 [512, 1024], P(None, 'tp'), may hold values from -0.25 to 0.25
- out_major: bfloat16 [2048, 2048], P('tp'), may hold values from -0.625 to 0.625
- out_minor: bfloat16 [1024, 2048], P('tp'), may hold values from -0.625 to 0.625
- residual: bfloat16 [1024, 2048], P('sp', 'tp'), may hold values from -4 to 4
- norm_gain: float32 [2048], replicated, may hold values from 0.1 to 1.9
- expert_ids: int32 [1024, 2], P('sp'), may hold values from 0 to 7, all different within a row; in each aligned block of 128 rows (0 to 127, 128 to 255, ...) at most 64 rows name the same one
- expert_weights: float32 [1024, 2], P('sp'), may hold values from 0.2 to 1
- gate_proj: bfloat16 [8, 2048, 4096], P('sp', None, 'tp'), may hold values from -0.125 to 0.125
- up_proj: bfloat16 [8, 2048, 4096], P('sp', None, 'tp'), may hold values from -0.125 to 0.125
- down_proj: bfloat16 [8, 4096, 2048], P('sp', 'tp'), may hold values from -0.125 to 0.125
Outputs:
- mixed: bfloat16 [1024, 2048], P('sp', 'tp')
The draws below stay inside these ranges and needn't reach their ends.
Inputs may be any that keep to these rules, and one draw needn't show every extreme that they name: `expert_ids`: each row names 2 different experts. In each aligned block of 128 rows (the rows of one index of sp) no expert is named by more than 64 rows, and in some blocks one expert is named by exactly 64 rows.
All inputs are finite; a program needn't handle non-finite values.
Results may differ from the reference program's by a relative error of at most 0.02.
Values may be sent and summed in bfloat16 or wider, within the bound.
A program may use at most 64 MiB of HBM per device.

```python
import math
import jax
import jax.numpy as jnp
import numpy as np
from jax import lax

D = 2048
HEADS_MAJOR = 16
HEADS_MINOR = 16
NOPE_MAJOR = 128
VAL_MAJOR = 128
NOPE_MINOR = 64
VAL_MINOR = 64
ROPE = 64
LATENT = 512
FF = 4096
TOP = 2
TOK_DEV = 128
TOKENS = 1024
EXPERTS = 8
CAP = 64
N_SP = 8
N_TP = 4


def rope_base(key):
    inner_key = jax.random.fold_in(key, 101)
    values = jnp.clip(jax.random.normal(inner_key, (TOKENS, ROPE), jnp.float32), -4.0, 4.0)
    return values


def draw_rope_keys(key, part):
    values = rope_base(key)
    return values.astype(jnp.bfloat16)


def drawn_query(key, salt, head_count, nope_width):
    inner_key = jax.random.fold_in(key, salt)
    full_shape = (TOKENS, head_count, nope_width + ROPE)
    drawn = jnp.clip(jax.random.normal(inner_key, full_shape, jnp.float32), -4.0, 4.0)
    return drawn.reshape(TOKENS, head_count * (nope_width + ROPE)).astype(jnp.bfloat16)


def draw_query_major(key, part):
    return drawn_query(key, 201, HEADS_MAJOR, NOPE_MAJOR)


def draw_query_minor(key, part):
    return drawn_query(key, 202, HEADS_MINOR, NOPE_MINOR)


def draw_residual(key, part):
    column = jnp.arange(D, dtype=jnp.float32)
    ramp = 0.15 * 6.0 ** (column / D)
    inner_key = jax.random.fold_in(key, 301)
    drawn = jnp.clip(jax.random.normal(inner_key, (TOKENS, D), jnp.float32), -4.0, 4.0)
    return (drawn * ramp[None, :]).astype(jnp.bfloat16)


def with_spikes(entries, rng, source, target, parts, factor):
    owner, partner = [(jnp.arange(entries.shape[position]) // (entries.shape[position] // parts)).reshape([-1 if axis == position else 1 for axis in range(entries.ndim)]) for position in (source, target)]
    chosen = jax.random.permutation(rng, parts)[partner]
    strong = (owner == chosen) | (owner == (partner + parts // 2) % parts)
    return jnp.where(strong, factor * entries, entries)


def block_levels(own_key, dims, cuts, least, top_value):
    def one(axis_at, blocks):
        draws = jax.random.uniform(jax.random.fold_in(jax.random.fold_in(own_key, 6), axis_at), (blocks,), jnp.float32, least / len(cuts), top_value / len(cuts))
        return jnp.repeat(jnp.exp(draws), dims[axis_at] // blocks).reshape((-1,) + (1,) * (len(dims) - axis_at - 1))

    gain = one(*cuts[0])
    for cut in cuts[1:]:
        gain = gain * one(*cut)
    return gain


def shared_out(stream_key, own, number, rows, amount, top, limit, skew):
    order = jax.random.permutation(stream_key, amount)
    crowded, usual = shares(amount, rows * top, limit, skew, True), shares(amount, rows * top, limit, skew, False)
    places = jnp.arange(amount)

    def named(lengths, turn):
        used = int((lengths > 0).sum())
        fixed = max(1, used // 4)
        shifted = fixed + (places - fixed + turn * (used - fixed)) % max(1, amount - fixed)
        return jnp.zeros((amount,), jnp.int32).at[order[jnp.where(places < fixed, places, shifted)]].set(jnp.asarray(lengths, jnp.int32))

    lengths = jnp.where(number % 4 == 0, named(crowded, number // 4), named(usual, number - number // 4 - 1))
    mixed = jax.random.permutation(jax.random.fold_in(own, 3), amount)
    giver, sink = mixed[0:amount // 2 * 2:2], mixed[1:amount // 2 * 2:2]
    slack = jnp.minimum(lengths[giver] - 1, limit - lengths[sink]) // 2
    slack = jnp.where((giver == order[0]) | (sink == order[0]) | (lengths[sink] == 0), 0, jnp.maximum(slack, 0))
    shifted = jax.random.randint(jax.random.fold_in(own, 4), (amount // 2,), 0, 1 << 20) % (slack + 1)
    lengths = lengths.at[giver].add(-shifted).at[sink].add(shifted)
    items = jnp.searchsorted(jnp.cumsum(lengths), jnp.arange(rows * top), side="right").astype(jnp.int32)
    listing = items.reshape(top, rows).T
    listing = listing[jax.random.permutation(jax.random.fold_in(own, 1), rows)]
    turn = jax.random.randint(jax.random.fold_in(own, 2), (rows, 1), 0, top)
    return jnp.take_along_axis(listing, (jnp.arange(top)[None, :] + turn) % top, axis=1)


def shares(amount, total, limit, lean, full):
    portions = [(1 << 20) // math.isqrt(grade ** lean) + 1 for grade in range(1, amount + 1)]
    largest = limit if full else min(limit, max(-(-total // amount), total * portions[0] // sum(portions)))
    least = 1 if total - largest >= amount - 1 else 0
    counts, rest = [largest] + [least] * (amount - 1), total - largest - least * (amount - 1)
    while rest > 0:
        candidates = [i for i in range(1, amount) if counts[i] < largest] or [i for i in range(1, amount) if counts[i] < limit]
        mass, remaining = sum([portions[i] for i in candidates]), rest
        for i in candidates:
            more = min(limit - counts[i], max(1, remaining * portions[i] // mass), rest)
            counts[i] = counts[i] + more
            rest = rest - more
    return np.array(counts)


def bell_draw(rng, shape, deviation, reach, split=(), kind=jnp.bfloat16):
    values = jax.random.normal(rng, shape, jnp.float32) * deviation
    if len(split) > 0:
        values = block_levels(rng, shape, split, -0.22, 0.18) * values
    return jnp.clip(values, min=-reach, max=reach).astype(kind)


def heavy_noise(stream_key, extent, scale, bound, pieces, heavy, kind=jnp.bfloat16):
    values = scale * jax.random.normal(stream_key, extent, jnp.float32)
    if pieces:
        values = values * block_levels(stream_key, extent, pieces, -0.22, 0.18)
    return jnp.clip(with_spikes(values, jax.random.fold_in(stream_key, 3), *heavy), -bound, bound).astype(kind)


def setup_inputs(seed: int = 0) -> dict:
    keys = jax.random.split(jax.random.key(seed), 18)
    query_major = draw_query_major(jax.random.fold_in(keys[17], 71), 0)
    query_minor = draw_query_minor(jax.random.fold_in(keys[17], 71), 0)
    latent_rows = bell_draw(keys[2], (TOKENS, LATENT), 1.0, 6.0, ((0, 8),))
    rope_keys = draw_rope_keys(jax.random.fold_in(keys[17], 71), 0)
    key_up_major = bell_draw(keys[4], (LATENT, HEADS_MAJOR * NOPE_MAJOR), LATENT ** -0.5, 0.25, ((1, 4),))
    value_up_major = bell_draw(keys[5], (LATENT, HEADS_MAJOR * VAL_MAJOR), LATENT ** -0.5, 0.25, ((1, 4),))
    key_up_minor = bell_draw(keys[6], (LATENT, HEADS_MINOR * NOPE_MINOR), LATENT ** -0.5, 0.25, ((1, 4),))
    value_up_minor = bell_draw(keys[7], (LATENT, HEADS_MINOR * VAL_MINOR), LATENT ** -0.5, 0.25, ((1, 4),))
    out_major = heavy_noise(keys[8], (HEADS_MAJOR * VAL_MAJOR, D), ((HEADS_MAJOR * VAL_MAJOR + HEADS_MINOR * VAL_MINOR) // 16) ** -0.5, 0.625, ((0, 4),), (0, 1, 4, 2.0))
    out_minor = heavy_noise(keys[9], (HEADS_MINOR * VAL_MINOR, D), ((HEADS_MAJOR * VAL_MAJOR + HEADS_MINOR * VAL_MINOR) // 16) ** -0.5, 0.625, ((0, 4),), (0, 1, 4, 2.0))
    residual = draw_residual(jax.random.fold_in(keys[17], 71), 0)
    norm_gain = jnp.clip(1.0 + 0.18 * jax.random.normal(keys[11], (D,), jnp.float32), 0.1, 1.9)
    expert_ids_keys = jax.random.split(jax.random.fold_in(keys[12], 1), TOKENS // TOK_DEV)
    expert_ids_turns = jax.random.permutation(jax.random.fold_in(keys[12], 3), TOKENS // TOK_DEV)
    expert_ids = jax.vmap(lambda own, number: shared_out(jax.random.fold_in(keys[12], 2), own, number, TOK_DEV, EXPERTS, TOP, CAP, 1))(expert_ids_keys, expert_ids_turns).reshape((TOKENS, TOP))
    expert_weights = jnp.clip(0.2 + 0.8 * jax.random.uniform(keys[13], (TOKENS, TOP), jnp.float32) ** block_levels(keys[13], (TOKENS, TOP), ((0, 8),), -0.2, 0.2), 0.2, 1.0)
    gate_proj = bell_draw(keys[14], (EXPERTS, D, FF), D ** -0.5, 0.125, ((0, 8), (2, 4)))
    up_proj = bell_draw(keys[15], (EXPERTS, D, FF), D ** -0.5, 0.125, ((0, 8), (2, 4)))
    down_proj = heavy_noise(keys[16], (EXPERTS, FF, D), FF ** -0.5, 0.125, ((0, 8), (1, 4)), (1, 2, 4, 2.0))
    return {"query_major": query_major, "query_minor": query_minor, "latent_rows": latent_rows, "rope_keys": rope_keys, "key_up_major": key_up_major, "value_up_major": value_up_major, "key_up_minor": key_up_minor, "value_up_minor": value_up_minor, "out_major": out_major, "out_minor": out_minor, "residual": residual, "norm_gain": norm_gain, "expert_ids": expert_ids, "expert_weights": expert_weights, "gate_proj": gate_proj, "up_proj": up_proj, "down_proj": down_proj}


theta_base = 10000.0
norm_eps = 1e-06

def rotary(values, positions):
    half_width = values.shape[-1] // 2
    inverse_freq = 1.0 / theta_base ** (jnp.arange(half_width, dtype=jnp.float32) * (2.0 / values.shape[-1]))
    angles = positions.astype(jnp.float32)[:, None] * inverse_freq[None, :]
    view_shape = (angles.shape[0],) + (1,) * (values.ndim - 2) + (half_width,)
    cosine = jnp.cos(angles).reshape(view_shape)
    sine_table = jnp.sin(angles).reshape(view_shape)
    lower_half = values[..., :half_width].astype(jnp.float32)
    upper_half = values[..., half_width:].astype(jnp.float32)
    return jnp.concatenate([lower_half * cosine - upper_half * sine_table, upper_half * cosine + lower_half * sine_table], axis=-1)

def group_attention(query, latent_rows, rope_rot, key_up, value_up, head_count, nope_width, positions):
    tok_count = query.shape[0]
    rope_width = rope_rot.shape[1]
    shaped = query.reshape(tok_count, head_count, nope_width + rope_width)
    q_nope = shaped[:, :, :nope_width]
    q_rope = rotary(shaped[:, :, nope_width:], positions).astype(jnp.bfloat16)
    key_rows = jnp.dot(latent_rows, key_up, preferred_element_type=jnp.float32).astype(jnp.bfloat16).reshape(tok_count, head_count, nope_width)
    value_rows = jnp.dot(latent_rows, value_up, preferred_element_type=jnp.float32).astype(jnp.bfloat16).reshape(tok_count, head_count, -1)
    scale = (nope_width + rope_width) ** (-0.5)
    visible = positions[None, :] <= positions[:, None]

    def one_head(operands):
        head_nope, head_rope, head_keys, head_values = operands
        scores = jnp.dot(head_nope, head_keys.T, preferred_element_type=jnp.float32)
        scores = scores + jnp.dot(head_rope, rope_rot.T, preferred_element_type=jnp.float32)
        scores = jnp.where(visible, scores * scale, -jnp.inf)
        largest = lax.optimization_barrier(jnp.max(scores, axis=1, keepdims=True))
        weights = jnp.exp(scores - largest)
        totals = lax.optimization_barrier(jnp.sum(weights, axis=1, keepdims=True))
        summed = jnp.dot(weights.astype(jnp.bfloat16), head_values, preferred_element_type=jnp.float32)
        return (summed / totals).astype(jnp.bfloat16)
    stacked = lax.map(one_head, (q_nope.transpose(1, 0, 2), q_rope.transpose(1, 0, 2), key_rows.transpose(1, 0, 2), value_rows.transpose(1, 0, 2)))
    return stacked.transpose(1, 0, 2).reshape(tok_count, -1)

def head_projection(attn_major, attn_minor, out_major, out_minor):
    tok_count = attn_major.shape[0]
    width = out_major.shape[1]
    major_sets = attn_major.reshape(tok_count, N_TP, -1).transpose(1, 0, 2)
    minor_sets = attn_minor.reshape(tok_count, N_TP, -1).transpose(1, 0, 2)
    major_weights = out_major.reshape(N_TP, -1, width)
    minor_weights = out_minor.reshape(N_TP, -1, width)

    def add_set(summed, operands):
        set_major, set_minor, weight_major, weight_minor = operands
        partial_value = jnp.dot(set_major, weight_major, preferred_element_type=jnp.float32)
        partial_value = partial_value + jnp.dot(set_minor, weight_minor, preferred_element_type=jnp.float32)
        partial_value = lax.optimization_barrier(partial_value.astype(jnp.bfloat16)).astype(jnp.float32)
        return (summed + partial_value, None)
    summed, unused = lax.scan(add_set, jnp.zeros((tok_count, width), jnp.float32), (major_sets, minor_sets, major_weights, minor_weights))
    return summed

def slot_ids(route_block, experts, capacity):
    pairs = route_block.reshape(-1)
    matches = (pairs[:, None] == jnp.arange(experts, dtype=jnp.int32)[None, :]).astype(jnp.int32)
    ranks = jnp.cumsum(matches, axis=0) - 1
    return pairs * capacity + lax.optimization_barrier(jnp.sum(ranks * matches, axis=1))

def reference(query_major, query_minor, latent_rows, rope_keys, key_up_major, value_up_major, key_up_minor, value_up_minor, out_major, out_minor, residual, norm_gain, expert_ids, expert_weights, gate_proj, up_proj, down_proj):
    positions = jnp.arange(TOKENS, dtype=jnp.int32)
    rope_rot = rotary(rope_keys, positions).astype(jnp.bfloat16)
    attn_major = group_attention(query_major, latent_rows, rope_rot, key_up_major, value_up_major, HEADS_MAJOR, NOPE_MAJOR, positions)
    attn_minor = group_attention(query_minor, latent_rows, rope_rot, key_up_minor, value_up_minor, HEADS_MINOR, NOPE_MINOR, positions)
    head_total = head_projection(attn_major, attn_minor, out_major, out_minor)
    stream_mid = (residual.astype(jnp.float32) + head_total).astype(jnp.bfloat16)
    stream_f = stream_mid.astype(jnp.float32)
    normed = (stream_f * lax.rsqrt(lax.optimization_barrier(jnp.mean(stream_f * stream_f, axis=1, keepdims=True)) + norm_eps) * norm_gain[None, :]).astype(jnp.bfloat16)
    blocks = expert_ids.reshape(N_SP, TOK_DEV, TOP)
    local_slots = jax.vmap(lambda block_ids: slot_ids(block_ids, EXPERTS, CAP))(blocks)
    block_index = jnp.arange(N_SP, dtype=jnp.int32)[:, None]
    global_slots = (local_slots // CAP * (N_SP * CAP) + block_index * CAP + local_slots % CAP).reshape(-1)
    buffer = jnp.zeros((EXPERTS * N_SP * CAP, D), jnp.bfloat16).at[global_slots].set(jnp.repeat(normed, TOP, axis=0))

    def one_expert(operands):
        slot_rows, gate_weight, up_weight, down_weight = operands
        gate_pre = jnp.dot(slot_rows, gate_weight, preferred_element_type=jnp.float32)
        up_pre = jnp.dot(slot_rows, up_weight, preferred_element_type=jnp.float32)
        hidden = (jax.nn.silu(gate_pre) * up_pre).astype(jnp.bfloat16)
        hidden_sets = hidden.reshape(hidden.shape[0], N_TP, -1).transpose(1, 0, 2)
        down_sets = down_weight.reshape(N_TP, -1, D)

        def add_set(summed, operands_set):
            hidden_set, down_set = operands_set
            partial_value = jnp.dot(hidden_set, down_set, preferred_element_type=jnp.float32)
            partial_value = lax.optimization_barrier(partial_value.astype(jnp.bfloat16)).astype(jnp.float32)
            return (summed + partial_value, None)
        summed, unused = lax.scan(add_set, jnp.zeros((hidden.shape[0], D), jnp.float32), (hidden_sets, down_sets))
        return summed.astype(jnp.bfloat16)
    expert_out = lax.map(one_expert, (buffer.reshape(EXPERTS, N_SP * CAP, D), gate_proj, up_proj, down_proj))
    picked = expert_out.reshape(EXPERTS * N_SP * CAP, D)[global_slots].astype(jnp.float32)
    weighted = picked * expert_weights.reshape(-1)[:, None]
    moe_out = lax.optimization_barrier(jnp.sum(weighted.reshape(TOKENS, TOP, D), axis=1))
    return (stream_f + moe_out).astype(jnp.bfloat16)
```

```python
import functools

import jax
import jax.numpy as jnp
from jax import lax
from jax.experimental import pallas as pl
from jax.experimental.pallas import tpu as pltpu
from jax.sharding import PartitionSpec as P

NOPE_MAJOR = 128
NOPE_MINOR = 64
TOP = 2
MESH = pl.DeviceIdType.MESH

theta_base = 10000.0
norm_eps = 1e-06


def rotary(values, positions):
    half_width = values.shape[-1] // 2
    inverse_freq = 1.0 / theta_base ** (
        jnp.arange(half_width, dtype=jnp.float32) * (2.0 / values.shape[-1])
    )
    angles = positions.astype(jnp.float32)[:, None] * inverse_freq[None, :]
    view_shape = (angles.shape[0],) + (1,) * (values.ndim - 2) + (half_width,)
    cosine = jnp.cos(angles).reshape(view_shape)
    sine_table = jnp.sin(angles).reshape(view_shape)
    lower_half = values[..., :half_width].astype(jnp.float32)
    upper_half = values[..., half_width:].astype(jnp.float32)
    return jnp.concatenate(
        [
            lower_half * cosine - upper_half * sine_table,
            upper_half * cosine + lower_half * sine_table,
        ],
        axis=-1,
    )


def slot_ids(route_block, experts, capacity):
    pairs = route_block.reshape(-1)
    matches = pairs[:, None] == jnp.arange(experts, dtype=jnp.int32)[None, :]
    order = jnp.arange(pairs.shape[0], dtype=jnp.int32)
    earlier = (order[:, None] > order[None, :]).astype(jnp.bfloat16)
    ranks = jnp.dot(earlier, matches.astype(jnp.bfloat16), preferred_element_type=jnp.float32)
    rank = jnp.sum(jnp.where(matches, ranks, 0.0), axis=1).astype(jnp.int32)
    return (pairs * capacity + rank).reshape(route_block.shape)


def remote(src, dst, send_sem, recv_sem, sp_id, tp_id):
    return pltpu.make_async_remote_copy(
        src_ref=src,
        dst_ref=dst,
        send_sem=send_sem,
        recv_sem=recv_sem,
        device_id=(sp_id, tp_id),
        device_id_type=MESH,
    )


def greet(partners):
    barrier = pltpu.get_barrier_semaphore()
    for sp_id, tp_id in partners:
        pl.semaphore_signal(barrier, inc=1, device_id=(sp_id, tp_id), device_id_type=MESH)
    pl.semaphore_wait(barrier, len(partners))


def comm_call(body, out_shape, scratch, collective_id, operands, limit=60 * 1024 * 1024):
    return pl.pallas_call(
        body,
        out_shape=out_shape,
        in_specs=[pl.BlockSpec(memory_space=pltpu.VMEM)] * len(operands),
        out_specs=pl.BlockSpec(memory_space=pltpu.VMEM),
        scratch_shapes=scratch,
        compiler_params=pltpu.CompilerParams(
            collective_id=collective_id, has_side_effects=True, vmem_limit_bytes=limit
        ),
    )(*operands)


def gather_kernel(sp, x_ref, out_ref, up_send, up_recv, side_send, side_recv):
    rows = x_ref.shape[0]
    chips = sp // 2
    sp_id, tp_id = lax.axis_index("sp"), lax.axis_index("tp")
    level, core = sp_id // 2, lax.rem(sp_id, 2)
    sibling = 2 * level + 1 - core
    barrier = pltpu.get_barrier_semaphore()
    pl.semaphore_signal(barrier, inc=1, device_id=(sibling, tp_id), device_id_type=MESH)

    @pl.when(level > 0)
    def _():
        pl.semaphore_signal(barrier, inc=1, device_id=(sp_id - 2, tp_id), device_id_type=MESH)

    @pl.when(level < chips - 1)
    def _():
        pl.semaphore_signal(barrier, inc=1, device_id=(sp_id + 2, tp_id), device_id_type=MESH)

    pl.semaphore_wait(barrier, 1 + lax.min(level, 1) + lax.min(chips - 1 - level, 1))

    def rows_of(index):
        return pl.ds(pl.multiple_of(index * rows, rows), rows)

    def up_copy(step, src):
        place = out_ref.at[rows_of(sp_id - 2 * step), :]
        return remote(src if src is not None else place, place, up_send.at[step], up_recv.at[step], sp_id + 2, tp_id)

    def side_copy(step, src):
        place = out_ref.at[rows_of(sp_id - 2 * step), :]
        return remote(src if src is not None else place, place, side_send.at[step], side_recv.at[step], sibling, tp_id)

    def arrival(sem, index):
        place = out_ref.at[rows_of(index), :]
        return pltpu.make_async_copy(place, place, sem)

    @pl.when(level < chips - 1)
    def _():
        up_copy(0, x_ref).start()

    side_copy(0, x_ref).start()
    out_ref[rows_of(sp_id), :] = x_ref[...]
    for other in range(1, chips):

        @pl.when(level + other < chips)
        def _():
            first = pl.multiple_of((level + other) * 2 * rows, 2 * rows)
            out_ref[pl.ds(first, 2 * rows), :] = jnp.zeros((2 * rows, out_ref.shape[1]), out_ref.dtype)

    for step in range(1, chips):

        @pl.when(level - step >= 0)
        def _():
            arrival(up_recv.at[step - 1], sp_id - 2 * step).wait()

            @pl.when(level < chips - 1)
            def _():
                up_copy(step, None).start()

            side_copy(step, None).start()

    for step in range(chips):

        @pl.when(level - step >= 0)
        def _():
            arrival(side_recv.at[step], sibling - 2 * step).wait()
            side_copy(step, x_ref if step == 0 else None).wait_send()

            @pl.when(level < chips - 1)
            def _():
                up_copy(step, x_ref if step == 0 else None).wait_send()


def reduce_kernel(tp, part_ref, res_ref, out_ref, landed, send_sem, recv_sem):
    width = res_ref.shape[1]
    sp_id, tp_id = lax.axis_index("sp"), lax.axis_index("tp")
    peers = [lax.rem(tp_id + d, tp) for d in range(1, tp)]
    greet([(sp_id, p) for p in peers])

    def columns(index):
        return pl.ds(pl.multiple_of(index * width, width), width)

    copies = []
    for d in range(1, tp):
        copy = remote(
            part_ref.at[:, columns(peers[d - 1])],
            landed.at[d - 1],
            send_sem.at[d - 1],
            recv_sem.at[d - 1],
            sp_id,
            peers[d - 1],
        )
        copy.start()
        copies.append(copy)
    total = part_ref[:, columns(tp_id)].astype(jnp.float32)
    for d in range(1, tp):
        copies[d - 1].wait()
        total = total + landed[d - 1].astype(jnp.float32)
    out_ref[...] = (res_ref[...].astype(jnp.float32) + total).astype(jnp.bfloat16)


def near_first(count):
    order = [0]
    for d in range(1, count // 2 + 1):
        order.append(d)
        if count - d != d:
            order.append(count - d)
    return order


def square(tp_id):
    low = lax.rem(tp_id, 2)
    high = tp_id // 2
    return 2 * high + 1 - low, 2 * (1 - high) + low, 2 * (1 - high) + 1 - low


def dispatch_kernel(sp, tp, x_ref, out_ref, z_send, z_recv, t_send, t_recv, own_sem):
    cap = x_ref.shape[0] // sp
    width = x_ref.shape[1]
    half = cap // 2
    sp_id, tp_id = lax.axis_index("sp"), lax.axis_index("tp")
    greet(
        [(lax.rem(sp_id + d, sp), tp_id) for d in range(1, sp)]
        + [(sp_id, lax.rem(tp_id + d, tp)) for d in range(1, tp)]
    )

    def place(source, owner, part=None):
        first = source * cap
        if part is not None:
            first = first + part * half
        count = cap if part is None else half
        return out_ref.at[
            pl.ds(pl.multiple_of(first, half), count),
            pl.ds(pl.multiple_of(owner * width, width), width),
        ]

    def rows(source, part=None):
        first = source * cap
        if part is not None:
            first = first + part * half
        return x_ref.at[pl.ds(pl.multiple_of(first, half), cap if part is None else half), :]

    order = near_first(sp)
    z_copies = {}
    for d in order[1:]:
        target = lax.rem(sp_id + d, sp)
        z_copies[d] = remote(rows(target), place(sp_id, tp_id), z_send.at[d], z_recv.at[d], target, tp_id)
        z_copies[d].start()
    own = pltpu.make_async_copy(rows(sp_id), place(sp_id, tp_id), own_sem)
    own.start()

    def source_of(d):
        return lax.rem(sp_id + sp - d, sp)

    started = []
    if tp == 4:
        near, far, across = square(tp_id)

        def send(d, part, target, slot, owner):
            copy = remote(
                place(source_of(d), owner, part),
                place(source_of(d), owner, part),
                t_send.at[d, slot],
                t_recv.at[d, slot],
                sp_id,
                target,
            )
            copy.start()
            started.append(copy)
            return copy

        def relay(entry):
            d, to_near, to_far = entry
            to_near[0].wait_recv()
            fourth = send(d, 0, far, 4, near)
            to_far[1].wait_recv()
            fifth = send(d, 1, near, 5, far)
            return [to_near[1], to_far[0], fourth, fifth]

        waiting, rest = None, []
        for d in order:
            if d == 0:
                own.wait()
            else:
                z_copies[d].wait_recv()
            to_near = [send(d, 0, near, 0, tp_id), None]
            to_far = [None, send(d, 1, far, 3, tp_id)]
            to_near[1] = send(d, 1, near, 1, tp_id)
            to_far[0] = send(d, 0, far, 2, tp_id)
            if waiting is not None:
                rest += relay(waiting)
            waiting = (d, to_near, to_far)
        rest += relay(waiting)
        for copy in rest:
            copy.wait_recv()
    else:
        for d in order:
            if d == 0:
                own.wait()
            else:
                z_copies[d].wait_recv()
            for t in range(1, tp):
                copy = remote(
                    place(source_of(d), tp_id),
                    place(source_of(d), tp_id),
                    t_send.at[d, t],
                    t_recv.at[d, t],
                    sp_id,
                    lax.rem(tp_id + t, tp),
                )
                copy.start()
                started.append(copy)
        for copy in started:
            copy.wait_recv()
    for copy in started:
        copy.wait_send()
    for d in order[1:]:
        z_copies[d].wait_send()


def return_kernel(sp, tp, x_ref, out_ref, landed, turned, summed, t_send, t_recv, z_send, z_recv):
    cap = x_ref.shape[0] // sp
    width = out_ref.shape[1]
    half = cap // 2
    sp_id, tp_id = lax.axis_index("sp"), lax.axis_index("tp")
    greet(
        [(lax.rem(sp_id + d, sp), tp_id) for d in range(1, sp)]
        + [(sp_id, lax.rem(tp_id + d, tp)) for d in range(1, tp)]
    )

    def rows_at(target, part=None):
        first = target * cap
        if part is not None:
            first = first + part * half
        return pl.ds(pl.multiple_of(first, half), cap if part is None else half)

    def columns(owner):
        return pl.ds(pl.multiple_of(owner * width, width), width)

    order = near_first(sp)[::-1]
    started, z_copies = [], []

    def push(src, dst, d, slot, target):
        copy = remote(src, dst, t_send.at[d, slot], t_recv.at[d, slot], sp_id, target)
        copy.start()
        started.append(copy)
        return copy

    def deliver(d, target):
        if d == 0:
            return
        copy = remote(
            summed.at[d], out_ref.at[rows_at(sp_id), :], z_send.at[d], z_recv.at[d], target, tp_id
        )
        copy.start()
        z_copies.append(copy)

    def f32(value):
        return value.astype(jnp.float32)

    def place_sum(d, part, value):
        piece = pl.ds(part * half, half)
        summed[d, piece, :] = value.astype(jnp.bfloat16)
        if d == 0:
            out_ref[rows_at(sp_id, part), :] = value.astype(jnp.bfloat16)

    targets = {d: lax.rem(sp_id + d, sp) for d in order}
    if tp == 4:
        near, far, across = square(tp_id)
        first = {}

        def open_block(d):
            target = targets[d]
            first[d] = [
                push(x_ref.at[rows_at(target, 0), columns(across)], landed.at[d, 1], d, 1, near),
                push(x_ref.at[rows_at(target, 1), columns(across)], landed.at[d, 3], d, 3, far),
                push(x_ref.at[rows_at(target, 0), columns(near)], landed.at[d, 0], d, 0, near),
                push(x_ref.at[rows_at(target, 1), columns(far)], landed.at[d, 2], d, 2, far),
            ]

        second = {}

        def turn_block(d):
            target = targets[d]
            first[d][0].wait_recv()
            turned[d, 0] = (f32(x_ref[rows_at(target, 0), columns(far)]) + f32(landed[d, 1])).astype(jnp.bfloat16)
            first[d][1].wait_recv()
            turned[d, 1] = (f32(x_ref[rows_at(target, 1), columns(near)]) + f32(landed[d, 3])).astype(jnp.bfloat16)
            second[d] = [
                push(turned.at[d, 0], landed.at[d, 4], d, 4, far),
                push(turned.at[d, 1], landed.at[d, 5], d, 5, near),
            ]

        def close_block(d):
            target = targets[d]
            first[d][2].wait_recv()
            second[d][0].wait_recv()
            place_sum(d, 0, f32(x_ref[rows_at(target, 0), columns(tp_id)]) + f32(landed[d, 0]) + f32(landed[d, 4]))
            first[d][3].wait_recv()
            second[d][1].wait_recv()
            place_sum(d, 1, f32(x_ref[rows_at(target, 1), columns(tp_id)]) + f32(landed[d, 2]) + f32(landed[d, 5]))
            deliver(d, target)

        count = len(order)
        for i in range(count + 2):
            if i < count:
                open_block(order[i])
            if 0 <= i - 1 < count:
                turn_block(order[i - 1])
            if 0 <= i - 2 < count:
                close_block(order[i - 2])
    else:
        pushed = {}
        for d in order:
            pushed[d] = []
            for t in range(1, tp):
                owner = lax.rem(tp_id + t, tp)
                for part in range(2):
                    slot = 2 * (t - 1) + part
                    pushed[d].append(
                        push(x_ref.at[rows_at(targets[d], part), columns(owner)], landed.at[d, slot], d, slot, owner)
                    )
        for d in order:
            for part in range(2):
                value = f32(x_ref[rows_at(targets[d], part), columns(tp_id)])
                for t in range(1, tp):
                    pushed[d][2 * (t - 1) + part].wait_recv()
                    value = value + f32(landed[d, 2 * (t - 1) + part])
                place_sum(d, part, value)
            deliver(d, targets[d])
    for copy in started:
        copy.wait_send()
    for copy in z_copies:
        copy.wait()


def attention_kernel(
    groups,
    start_ref,
    joined_ref,
    nope_ref,
    rope_ref,
    key_major_ref,
    value_major_ref,
    key_minor_ref,
    value_minor_ref,
    out_major_ref,
    out_minor_ref,
    key_a,
    value_a,
    key_b,
    value_b,
):
    latent = key_major_ref.shape[0]
    tok_rows = nope_ref.shape[1]
    rows_f = joined_ref[:, :latent]
    tail = joined_ref[:, latent:]
    for kept, weight in (
        (key_a, key_major_ref),
        (value_a, value_major_ref),
        (key_b, key_minor_ref),
        (value_b, value_minor_ref),
    ):
        kept[...] = jnp.dot(rows_f, weight[...], preferred_element_type=jnp.float32).astype(jnp.bfloat16)
    total_keys = joined_ref.shape[0]
    shape = (tok_rows, total_keys)
    visible = lax.broadcasted_iota(jnp.int32, shape, 1) <= start_ref[0] + lax.broadcasted_iota(jnp.int32, shape, 0)
    contract = (((1,), (1,)), ((), ()))
    index = 0
    for kept_key, kept_value, out_ref, heads, pack, scale in (
        (key_a, value_a, out_major_ref, *groups[0]),
        (key_b, value_b, out_minor_ref, *groups[1]),
    ):
        tile = kept_key.shape[1] // (-(-heads // pack))
        lanes = lax.broadcasted_iota(jnp.int32, (tok_rows, tile), 1)
        for first in range(0, heads, pack):
            columns = pl.ds(first // pack * tile, tile)
            result = None
            for member in range(min(pack, heads - first)):
                scores = lax.dot_general(
                    nope_ref[index], kept_key[:, columns], contract, preferred_element_type=jnp.float32
                ) + lax.dot_general(rope_ref[index], tail, contract, preferred_element_type=jnp.float32)
                scores = jnp.where(visible, scores * scale, -jnp.inf)
                weights = jnp.exp(scores - jnp.max(scores, axis=1, keepdims=True))
                totals = jnp.sum(weights, axis=1, keepdims=True)
                summed = jnp.dot(
                    weights.astype(jnp.bfloat16), kept_value[:, columns], preferred_element_type=jnp.float32
                ) / totals
                result = summed if result is None else jnp.where(lanes < member * (tile // pack), result, summed)
                index += 1
            out_ref[:, columns] = result.astype(jnp.bfloat16)


def expert_kernel(x_ref, gain_ref, gate_ref, up_ref, down_ref, out_ref, normed, total):
    step = pl.program_id(0)

    @pl.when(step == 0)
    def _():
        rows_f = x_ref[...].astype(jnp.float32)
        power = jnp.mean(rows_f * rows_f, axis=1, keepdims=True)
        normed[...] = (rows_f * lax.rsqrt(power + norm_eps) * gain_ref[...]).astype(jnp.bfloat16)

    rows = normed[...]
    gate_pre = jnp.dot(rows, gate_ref[0], preferred_element_type=jnp.float32)
    up_pre = jnp.dot(rows, up_ref[0], preferred_element_type=jnp.float32)
    hidden = (gate_pre / (1.0 + jnp.exp(-gate_pre)) * up_pre).astype(jnp.bfloat16)
    part = jnp.dot(hidden, down_ref[0], preferred_element_type=jnp.float32)
    last = pl.num_programs(0) - 1

    @pl.when((step == 0) & (last > 0))
    def _():
        total[...] = part

    @pl.when((step > 0) & (step < last))
    def _():
        total[...] += part

    @pl.when((step == last) & (last > 0))
    def _():
        out_ref[...] = (total[...] + part).astype(jnp.bfloat16)

    @pl.when(last == 0)
    def _():
        out_ref[...] = part.astype(jnp.bfloat16)


def flip(index, offset):
    step = 1
    while step <= offset:
        if offset & step:
            index = index + step * (1 - 2 * lax.rem(index // step, 2))
        step *= 2
    return index


def moe_kernel(
    sp,
    x_ref,
    ids_ref,
    ids_t_ref,
    mix_ref,
    gain_ref,
    gate_ref,
    up_ref,
    down_ref,
    out_ref,
    gate,
    up,
    down,
    placed,
    rows_in,
    normed,
    hidden,
    part,
    landed,
    turned,
    summed,
    returned,
    hot,
    load_sem,
    z_send,
    z_recv,
    t_send,
    t_recv,
    r_send,
    r_recv,
    y_send,
    y_recv,
):
    tok_rows, width = x_ref.shape
    features = rows_in.shape[2]
    chips = sp // 2
    slots = placed.shape[0]
    cap = slots // sp
    units = gate.shape[1]
    sp_id, tp_id = lax.axis_index("sp"), lax.axis_index("tp")
    near, far, across = square(tp_id)

    loads = []
    pieces = load_sem.shape[1]
    for index, (src, dst) in enumerate(((gate_ref, gate), (up_ref, up), (down_ref, down))):
        rows = dst.shape[0] // pieces
        for piece in range(pieces):
            span = pl.ds(piece * rows, rows)
            copy = pltpu.make_async_copy(src.at[0, span, :], dst.at[span, :], load_sem.at[index, piece])
            copy.start()
            loads.append(copy)

    barrier = pltpu.get_barrier_semaphore()
    for offset in range(1, sp):
        pl.semaphore_signal(barrier, inc=1, device_id=(flip(sp_id, offset), tp_id), device_id_type=MESH)
    for peer in (near, far, across):
        pl.semaphore_signal(barrier, inc=1, device_id=(sp_id, peer), device_id_type=MESH)

    lanes = lax.broadcasted_iota(jnp.int32, (sp, tok_rows), 0)
    matches_t = [(lanes == ids_t_ref[j : j + 1, :]).astype(jnp.float32) for j in range(TOP)]
    order = (tok_rows, tok_rows)
    before_t = (lax.broadcasted_iota(jnp.int32, order, 0) < lax.broadcasted_iota(jnp.int32, order, 1)).astype(
        jnp.bfloat16
    )
    named_t = functools.reduce(lambda a, b: a + b, matches_t)
    earlier_t = jnp.dot(named_t.astype(jnp.bfloat16), before_t, preferred_element_type=jnp.float32)
    slot_rows = lax.broadcasted_iota(jnp.int32, (slots, tok_rows), 0)
    select = None
    for j in range(TOP):
        rank = jnp.sum(matches_t[j] * earlier_t, axis=0, keepdims=True).astype(jnp.int32)
        earlier_t = earlier_t + matches_t[j]
        chosen = jnp.where(slot_rows == ids_t_ref[j : j + 1, :] * cap + rank, 1.0, 0.0)
        select = chosen if select is None else select + chosen
    placed[...] = jnp.dot(select.astype(jnp.bfloat16), x_ref[...], preferred_element_type=jnp.float32).astype(
        jnp.bfloat16
    )

    def block(index):
        return pl.ds(pl.multiple_of(index * cap, cap), cap)

    def columns(owner):
        return pl.ds(pl.multiple_of(owner * width, width), width)

    own_columns = columns(tp_id)
    pl.semaphore_wait(barrier, sp - 1 + 3)

    z_copies = {}
    for offset in range(1, sp):
        target = flip(sp_id, offset)
        k, q = offset // 2, offset % 2
        z_copies[offset] = remote(
            placed.at[block(target), :],
            rows_in.at[k, pl.ds(q * cap, cap), own_columns],
            z_send.at[offset],
            z_recv.at[offset],
            target,
            tp_id,
        )
        z_copies[offset].start()
    rows_in[0, 0:cap, own_columns] = placed[block(sp_id), :]

    started = []

    def pass_on(k, q, owner, slot, target):
        place = rows_in.at[k, pl.ds(q * cap, cap), columns(owner)]
        copy = remote(place, place, t_send.at[k, slot], t_recv.at[k, slot], sp_id, target)
        copy.start()
        started.append(copy)
        return copy

    arriving = {}

    def open_chunk(k):
        if k == 0:
            first = [pass_on(0, 0, tp_id, 0, near), pass_on(0, 0, tp_id, 2, far)]
            z_copies[1].wait_recv()
            second = [pass_on(0, 1, tp_id, 3, far), pass_on(0, 1, tp_id, 1, near)]
            arriving[0] = [first[0], second[1], first[1], second[0]]
            return
        z_copies[2 * k].wait_recv()
        a = pass_on(k, 0, tp_id, 0, near)
        z_copies[2 * k + 1].wait_recv()
        d = pass_on(k, 1, tp_id, 3, far)
        b = pass_on(k, 1, tp_id, 1, near)
        c = pass_on(k, 0, tp_id, 2, far)
        arriving[k] = [a, b, c, d]

    def relay(k):
        a, b, c, d = arriving[k]
        a.wait_recv()
        e = pass_on(k, 0, near, 4, far)
        d.wait_recv()
        f = pass_on(k, 1, far, 5, near)
        arriving[k] = [b, c, e, f]

    def ready(k):
        for copy in arriving[k]:
            copy.wait_recv()
        rows = rows_in[k].astype(jnp.float32)
        power = jnp.mean(rows * rows, axis=1, keepdims=True)
        normed[...] = (rows * lax.rsqrt(power + norm_eps) * gain_ref[...]).astype(jnp.bfloat16)

    def expand():
        tile = 256
        rows = normed[...]
        for first in range(0, units, tile):
            span = slice(first, first + tile)
            gate_pre = jnp.dot(rows, gate[:, span], preferred_element_type=jnp.float32)
            up_pre = jnp.dot(rows, up[:, span], preferred_element_type=jnp.float32)
            hidden[:, span] = (gate_pre / (1.0 + jnp.exp(-gate_pre)) * up_pre).astype(jnp.bfloat16)

    def push(src, dst, k, slot, target):
        copy = remote(src, dst, r_send.at[k, slot], r_recv.at[k, slot], sp_id, target)
        copy.start()
        started.append(copy)
        return copy

    halves = (pl.ds(0, cap), pl.ds(cap, cap))
    leaving, turning = {}, {}

    def contract(k):
        rows = hidden[...]

        def fill(owner):
            part[k, :, columns(owner)] = jnp.dot(
                rows, down[:, columns(owner)], preferred_element_type=jnp.float32
            ).astype(jnp.bfloat16)

        def send(q, owner, slot, target):
            return push(part.at[k, halves[q], columns(owner)], landed.at[k, slot], k, slot, target)

        fill(across)
        second = send(0, across, 1, near)
        fourth = send(1, across, 3, far)
        fill(near)
        first = send(0, near, 0, near)
        fill(far)
        third = send(1, far, 2, far)
        fill(tp_id)
        leaving[k] = [first, second, third, fourth]

    def f32(value):
        return value.astype(jnp.float32)

    def turn(k):
        leaving[k][1].wait_recv()
        turned[k, 0] = (f32(part[k, halves[0], columns(far)]) + f32(landed[k, 1])).astype(jnp.bfloat16)
        a = push(turned.at[k, 0], landed.at[k, 4], k, 4, far)
        leaving[k][3].wait_recv()
        turned[k, 1] = (f32(part[k, halves[1], columns(near)]) + f32(landed[k, 3])).astype(jnp.bfloat16)
        b = push(turned.at[k, 1], landed.at[k, 5], k, 5, near)
        turning[k] = [a, b]

    back = {}

    def close(k):
        for q in range(2):
            leaving[k][2 * q].wait_recv()
            turning[k][q].wait_recv()
            value = f32(part[k, halves[q], own_columns]) + f32(landed[k, 2 * q]) + f32(landed[k, 4 + q])
            offset = 2 * k + q
            if offset == 0:
                returned[block(sp_id), :] = value.astype(jnp.bfloat16)
                continue
            summed[k, q] = value.astype(jnp.bfloat16)
            back[offset] = remote(
                summed.at[k, q],
                returned.at[block(sp_id), :],
                y_send.at[offset],
                y_recv.at[offset],
                flip(sp_id, offset),
                tp_id,
            )
            back[offset].start()

    open_chunk(0)
    relay(0)
    open_chunk(1)
    lanes = lax.broadcasted_iota(jnp.int32, (tok_rows, sp), 1)
    matches = [(lanes == ids_ref[:, j : j + 1]).astype(jnp.float32) for j in range(TOP)]
    before = (lax.broadcasted_iota(jnp.int32, order, 0) > lax.broadcasted_iota(jnp.int32, order, 1)).astype(
        jnp.bfloat16
    )
    named = functools.reduce(lambda a, b: a + b, matches)
    earlier = jnp.dot(before, named.astype(jnp.bfloat16), preferred_element_type=jnp.float32)
    slot_lanes = lax.broadcasted_iota(jnp.int32, (tok_rows, slots), 1)
    for j in range(TOP):
        rank = jnp.sum(matches[j] * earlier, axis=1, keepdims=True).astype(jnp.int32)
        earlier = earlier + matches[j]
        hot[j] = jnp.where(slot_lanes == ids_ref[:, j : j + 1] * cap + rank, 1.0, 0.0).astype(jnp.bfloat16)
    for copy in loads:
        copy.wait()
    relay(1)
    if chips > 2:
        open_chunk(2)
    turns = list(range(1, chips)) + [0]
    for index, k in enumerate(turns):
        ready(k)
        expand()
        if index + 2 < chips:
            relay(index + 2)
        if index + 3 < chips:
            open_chunk(index + 3)
        contract(k)
        if index >= 1:
            turn(turns[index - 1])
        if index >= 2:
            close(turns[index - 2])
    turn(turns[-1])
    close(turns[-2])
    close(turns[-1])
    for offset in range(1, sp):
        back[offset].wait_recv()
    total = x_ref[...].astype(jnp.float32)
    for j in range(TOP):
        total = total + jnp.dot(hot[j], returned[...], preferred_element_type=jnp.float32) * mix_ref[:, j : j + 1]
    out_ref[...] = total.astype(jnp.bfloat16)
    for copy in started:
        copy.wait_send()
    for offset in range(1, sp):
        z_copies[offset].wait_send()
        back[offset].wait_send()


def fused_experts(sp, tp, stream_mid, ids, mix, gain, gate_proj, up_proj, down_proj):
    tok_rows, width = stream_mid.shape
    cap = 2 * tok_rows * TOP // sp
    slots = sp * cap
    chips = sp // 2
    features = tp * width
    units = gate_proj.shape[2]
    dma = pltpu.SemaphoreType.DMA
    vmem = pl.BlockSpec(memory_space=pltpu.VMEM)
    hbm = pl.BlockSpec(memory_space=pl.ANY)
    bf16 = jnp.bfloat16
    return pl.pallas_call(
        functools.partial(moe_kernel, sp),
        out_shape=jax.ShapeDtypeStruct((tok_rows, width), bf16),
        in_specs=[vmem] * 5 + [hbm] * 3,
        out_specs=vmem,
        scratch_shapes=[
            pltpu.VMEM((features, units), bf16),
            pltpu.VMEM((features, units), bf16),
            pltpu.VMEM((units, features), bf16),
            pltpu.VMEM((slots, width), bf16),
            pltpu.VMEM((chips, 2 * cap, features), bf16),
            pltpu.VMEM((2 * cap, features), bf16),
            pltpu.VMEM((2 * cap, units), bf16),
            pltpu.VMEM((chips, 2 * cap, features), bf16),
            pltpu.VMEM((chips, 6, cap, width), bf16),
            pltpu.VMEM((chips, 2, cap, width), bf16),
            pltpu.VMEM((chips, 2, cap, width), bf16),
            pltpu.VMEM((slots, width), bf16),
            pltpu.VMEM((TOP, tok_rows, slots), bf16),
            dma((3, 4)),
            dma((sp,)),
            dma((sp,)),
            dma((chips, 6)),
            dma((chips, 6)),
            dma((chips, 6)),
            dma((chips, 6)),
            dma((sp,)),
            dma((sp,)),
        ],
        compiler_params=pltpu.CompilerParams(
            collective_id=4, has_side_effects=True, vmem_limit_bytes=60 * 1024 * 1024
        ),
    )(stream_mid, ids, ids.T, mix, gain.reshape(1, -1), gate_proj, up_proj, down_proj)


def run_experts(rows, gain, gate_proj, up_proj, down_proj):
    slots, features = rows.shape
    units = gate_proj.shape[2]
    tile = min(256, units)
    return pl.pallas_call(
        expert_kernel,
        grid=(units // tile,),
        out_shape=jax.ShapeDtypeStruct((slots, features), jnp.bfloat16),
        in_specs=[
            pl.BlockSpec((slots, features), lambda i: (0, 0)),
            pl.BlockSpec((1, features), lambda i: (0, 0)),
            pl.BlockSpec((1, features, tile), lambda i: (0, 0, i)),
            pl.BlockSpec((1, features, tile), lambda i: (0, 0, i)),
            pl.BlockSpec((1, tile, features), lambda i: (0, i, 0)),
        ],
        out_specs=pl.BlockSpec((slots, features), lambda i: (0, 0)),
        scratch_shapes=[
            pltpu.VMEM((slots, features), jnp.bfloat16),
            pltpu.VMEM((slots, features), jnp.float32),
        ],
        compiler_params=pltpu.CompilerParams(vmem_limit_bytes=60 * 1024 * 1024),
    )(rows, gain.reshape(1, -1), gate_proj, up_proj, down_proj)


def pad_columns(array, multiple):
    return jnp.pad(array, ((0, 0), (0, -array.shape[1] % multiple)))


def per_device(
    sp,
    tp,
    query_major,
    query_minor,
    latent_rows,
    rope_keys,
    key_up_major,
    value_up_major,
    key_up_minor,
    value_up_minor,
    out_major,
    out_minor,
    residual,
    norm_gain,
    expert_ids,
    expert_weights,
    gate_proj,
    up_proj,
    down_proj,
):
    tok_rows = query_major.shape[0]
    row_start = lax.axis_index("sp") * tok_rows
    positions = row_start + jnp.arange(tok_rows, dtype=jnp.int32)
    rope_width = rope_keys.shape[1]
    latent = latent_rows.shape[1]
    rope_rot = rotary(rope_keys, positions).astype(jnp.bfloat16)
    heads_major = key_up_major.shape[1] // NOPE_MAJOR
    heads_minor = key_up_minor.shape[1] // NOPE_MINOR
    shaped_major = query_major.reshape(tok_rows, heads_major, NOPE_MAJOR + rope_width)
    shaped_minor = query_minor.reshape(tok_rows, heads_minor, NOPE_MINOR + rope_width)
    nope_major = shaped_major[:, :, :NOPE_MAJOR]
    nope_minor = shaped_minor[:, :, :NOPE_MINOR]
    turned_major = rotary(shaped_major[:, :, NOPE_MAJOR:], positions).astype(jnp.bfloat16)
    turned_minor = rotary(shaped_minor[:, :, NOPE_MINOR:], positions).astype(jnp.bfloat16)
    scale_major = (NOPE_MAJOR + rope_width) ** (-0.5)
    scale_minor = (NOPE_MINOR + rope_width) ** (-0.5)

    joined = jnp.concatenate(
        [latent_rows, rope_rot, jnp.zeros((tok_rows, -(latent + rope_width) % 128), jnp.bfloat16)], axis=1
    )
    dma = pltpu.SemaphoreType.DMA
    chips = sp // 2
    gathered = comm_call(
        functools.partial(gather_kernel, sp),
        jax.ShapeDtypeStruct((sp * tok_rows, joined.shape[1]), jnp.bfloat16),
        [dma((chips,)), dma((chips,)), dma((chips,)), dma((chips,))],
        0,
        (joined,),
    )
    tail_width = joined.shape[1] - latent

    def by_head(array, width):
        return jnp.pad(array.transpose(1, 0, 2), ((0, 0), (0, 0), (0, width - array.shape[2])))

    pack = 128 // NOPE_MINOR
    spread = nope_minor.transpose(1, 0, 2)
    member = (jnp.arange(heads_minor, dtype=jnp.int32) % pack)[:, None, None]
    spread = jnp.concatenate(
        [jnp.where(member == m, spread, jnp.zeros_like(spread)) for m in range(pack)], axis=2
    )
    nope_all = jnp.concatenate([by_head(nope_major, 128), spread], axis=0)
    rope_all = jnp.concatenate([by_head(turned_major, tail_width), by_head(turned_minor, tail_width)], axis=0)
    minor_weights = [pad_columns(key_up_minor, 128), pad_columns(value_up_minor, 128)]
    minor_width = minor_weights[0].shape[1]
    keys = sp * tok_rows
    vmem = pl.BlockSpec(memory_space=pltpu.VMEM)
    attn_major, attn_minor = pl.pallas_call(
        functools.partial(attention_kernel, ((heads_major, 1, scale_major), (heads_minor, pack, scale_minor))),
        out_shape=(
            jax.ShapeDtypeStruct((tok_rows, value_up_major.shape[1]), jnp.bfloat16),
            jax.ShapeDtypeStruct((tok_rows, minor_width), jnp.bfloat16),
        ),
        in_specs=[pl.BlockSpec(memory_space=pltpu.SMEM)] + [vmem] * 7,
        out_specs=(vmem, vmem),
        scratch_shapes=[
            pltpu.VMEM((keys, key_up_major.shape[1]), jnp.bfloat16),
            pltpu.VMEM((keys, value_up_major.shape[1]), jnp.bfloat16),
            pltpu.VMEM((keys, minor_width), jnp.bfloat16),
            pltpu.VMEM((keys, minor_width), jnp.bfloat16),
        ],
        compiler_params=pltpu.CompilerParams(vmem_limit_bytes=60 * 1024 * 1024),
    )(
        row_start.reshape(1).astype(jnp.int32),
        gathered,
        nope_all,
        rope_all,
        key_up_major,
        value_up_major,
        *minor_weights,
    )
    attn_minor = attn_minor[:, : value_up_minor.shape[1]]
    partial_value = jnp.dot(attn_major, out_major, preferred_element_type=jnp.float32)
    partial_value = partial_value + jnp.dot(
        attn_minor, out_minor, preferred_element_type=jnp.float32
    )
    width = residual.shape[1]
    stream_mid = comm_call(
        functools.partial(reduce_kernel, tp),
        jax.ShapeDtypeStruct((tok_rows, width), jnp.bfloat16),
        [pltpu.VMEM((tp - 1, tok_rows, width), jnp.bfloat16), dma((tp - 1,)), dma((tp - 1,))],
        1,
        (partial_value.astype(jnp.bfloat16), residual),
    )
    if tp == 4 and sp & (sp - 1) == 0 and (2 * tok_rows * TOP // sp) % 16 == 0:
        return fused_experts(
            sp, tp, stream_mid, expert_ids, expert_weights, norm_gain, gate_proj, up_proj, down_proj
        )
    experts = sp
    capacity = 2 * tok_rows * TOP // experts
    slots = experts * capacity
    slot_list = slot_ids(expert_ids, experts, capacity)
    slot_numbers = jnp.arange(slots, dtype=jnp.int32)
    by_slot = slot_list.T
    select = (slot_numbers[:, None] == by_slot[0][None, :]).astype(jnp.bfloat16)
    for j in range(1, TOP):
        select = select + (slot_numbers[:, None] == by_slot[j][None, :]).astype(jnp.bfloat16)
    placed = jnp.dot(select, stream_mid, preferred_element_type=jnp.float32).astype(jnp.bfloat16)
    slots_t = 6 if tp == 4 else tp
    arrived = comm_call(
        functools.partial(dispatch_kernel, sp, tp),
        jax.ShapeDtypeStruct((slots, tp * width), jnp.bfloat16),
        [dma((sp,)), dma((sp,)), dma((sp, slots_t)), dma((sp, slots_t)), dma],
        2,
        (placed,),
    )
    down_part = run_experts(arrived, norm_gain, gate_proj, up_proj, down_proj)
    pieces = 6 if tp == 4 else 2 * (tp - 1)
    half = capacity // 2
    flat_out = comm_call(
        functools.partial(return_kernel, sp, tp),
        jax.ShapeDtypeStruct((slots, width), jnp.bfloat16),
        [
            pltpu.VMEM((sp, pieces, half, width), jnp.bfloat16),
            pltpu.VMEM((sp, 2, half, width), jnp.bfloat16),
            pltpu.VMEM((sp, capacity, width), jnp.bfloat16),
            dma((sp, pieces)),
            dma((sp, pieces)),
            dma((sp,)),
            dma((sp,)),
        ],
        3,
        (down_part,),
    )
    mixed = stream_mid.astype(jnp.float32)
    for j in range(TOP):
        hot = (slot_list[:, j : j + 1] == slot_numbers[None, :]).astype(jnp.bfloat16)
        mixed = mixed + jnp.dot(hot, flat_out, preferred_element_type=jnp.float32) * expert_weights[:, j : j + 1]
    return mixed.astype(jnp.bfloat16)


def solution(mesh):
    in_specs = (
        P("sp", "tp"),
        P("sp", "tp"),
        P("sp", None),
        P("sp", None),
        P(None, "tp"),
        P(None, "tp"),
        P(None, "tp"),
        P(None, "tp"),
        P("tp", None),
        P("tp", None),
        P("sp", "tp"),
        P(),
        P("sp", None),
        P("sp", None),
        P("sp", None, "tp"),
        P("sp", None, "tp"),
        P("sp", "tp", None),
    )
    out_specs = P("sp", "tp")
    return jax.shard_map(
        functools.partial(per_device, mesh.shape["sp"], mesh.shape["tp"]),
        mesh=mesh,
        in_specs=in_specs,
        out_specs=out_specs,
        check_vma=False,
    )
```

```python
import functools

import jax
import jax.numpy as jnp
import numpy as np
from jax import lax
from jax.experimental import pallas as pl
from jax.experimental.pallas import tpu as pltpu
from jax.sharding import PartitionSpec as P

NOPE_MAJOR = 128
NOPE_MINOR = 64
TOP = 2
MESH = pl.DeviceIdType.MESH

theta_base = 10000.0
norm_eps = 1e-06


def rotary(values, positions):
    half_width = values.shape[-1] // 2
    inverse_freq = 1.0 / theta_base ** (
        jnp.arange(half_width, dtype=jnp.float32) * (2.0 / values.shape[-1])
    )
    angles = positions.astype(jnp.float32)[:, None] * inverse_freq[None, :]
    view_shape = (angles.shape[0],) + (1,) * (values.ndim - 2) + (half_width,)
    cosine = jnp.cos(angles).reshape(view_shape)
    sine_table = jnp.sin(angles).reshape(view_shape)
    lower_half = values[..., :half_width].astype(jnp.float32)
    upper_half = values[..., half_width:].astype(jnp.float32)
    return jnp.concatenate(
        [
            lower_half * cosine - upper_half * sine_table,
            upper_half * cosine + lower_half * sine_table,
        ],
        axis=-1,
    )


def slot_ids(route_block, experts, capacity):
    pairs = route_block.reshape(-1)
    matches = pairs[:, None] == jnp.arange(experts, dtype=jnp.int32)[None, :]
    order = jnp.arange(pairs.shape[0], dtype=jnp.int32)
    earlier = (order[:, None] > order[None, :]).astype(jnp.bfloat16)
    ranks = jnp.dot(earlier, matches.astype(jnp.bfloat16), preferred_element_type=jnp.float32)
    rank = jnp.sum(jnp.where(matches, ranks, 0.0), axis=1).astype(jnp.int32)
    return (pairs * capacity + rank).reshape(route_block.shape)


def remote(src, dst, send_sem, recv_sem, sp_id, tp_id):
    return pltpu.make_async_remote_copy(
        src_ref=src,
        dst_ref=dst,
        send_sem=send_sem,
        recv_sem=recv_sem,
        device_id=(sp_id, tp_id),
        device_id_type=MESH,
    )


def greet(partners):
    barrier = pltpu.get_barrier_semaphore()
    for sp_id, tp_id in partners:
        pl.semaphore_signal(barrier, inc=1, device_id=(sp_id, tp_id), device_id_type=MESH)
    pl.semaphore_wait(barrier, len(partners))


def comm_call(body, out_shape, scratch, collective_id, operands, limit=60 * 1024 * 1024):
    return pl.pallas_call(
        body,
        out_shape=out_shape,
        in_specs=[pl.BlockSpec(memory_space=pltpu.VMEM)] * len(operands),
        out_specs=pl.BlockSpec(memory_space=pltpu.VMEM),
        scratch_shapes=scratch,
        compiler_params=pltpu.CompilerParams(
            collective_id=collective_id, has_side_effects=True, vmem_limit_bytes=limit
        ),
    )(*operands)


def gather_kernel(sp, x_ref, out_ref, up_send, up_recv, side_send, side_recv):
    rows = x_ref.shape[0]
    chips = sp // 2
    sp_id, tp_id = lax.axis_index("sp"), lax.axis_index("tp")
    level, core = sp_id // 2, lax.rem(sp_id, 2)
    sibling = 2 * level + 1 - core
    barrier = pltpu.get_barrier_semaphore()
    pl.semaphore_signal(barrier, inc=1, device_id=(sibling, tp_id), device_id_type=MESH)

    @pl.when(level > 0)
    def _():
        pl.semaphore_signal(barrier, inc=1, device_id=(sp_id - 2, tp_id), device_id_type=MESH)

    @pl.when(level < chips - 1)
    def _():
        pl.semaphore_signal(barrier, inc=1, device_id=(sp_id + 2, tp_id), device_id_type=MESH)

    pl.semaphore_wait(barrier, 1 + lax.min(level, 1) + lax.min(chips - 1 - level, 1))

    def rows_of(index):
        return pl.ds(pl.multiple_of(index * rows, rows), rows)

    def up_copy(step, src):
        place = out_ref.at[rows_of(sp_id - 2 * step), :]
        return remote(src if src is not None else place, place, up_send.at[step], up_recv.at[step], sp_id + 2, tp_id)

    def side_copy(step, src):
        place = out_ref.at[rows_of(sp_id - 2 * step), :]
        return remote(src if src is not None else place, place, side_send.at[step], side_recv.at[step], sibling, tp_id)

    def arrival(sem, index):
        place = out_ref.at[rows_of(index), :]
        return pltpu.make_async_copy(place, place, sem)

    @pl.when(level < chips - 1)
    def _():
        up_copy(0, x_ref).start()

    side_copy(0, x_ref).start()
    out_ref[rows_of(sp_id), :] = x_ref[...]
    for other in range(1, chips):

        @pl.when(level + other < chips)
        def _():
            first = pl.multiple_of((level + other) * 2 * rows, 2 * rows)
            out_ref[pl.ds(first, 2 * rows), :] = jnp.zeros((2 * rows, out_ref.shape[1]), out_ref.dtype)

    for step in range(1, chips):

        @pl.when(level - step >= 0)
        def _():
            arrival(up_recv.at[step - 1], sp_id - 2 * step).wait()

            @pl.when(level < chips - 1)
            def _():
                up_copy(step, None).start()

            side_copy(step, None).start()

    for step in range(chips):

        @pl.when(level - step >= 0)
        def _():
            arrival(side_recv.at[step], sibling - 2 * step).wait()
            side_copy(step, x_ref if step == 0 else None).wait_send()

            @pl.when(level < chips - 1)
            def _():
                up_copy(step, x_ref if step == 0 else None).wait_send()


def reduce_kernel(tp, part_ref, res_ref, out_ref, landed, send_sem, recv_sem):
    width = res_ref.shape[1]
    sp_id, tp_id = lax.axis_index("sp"), lax.axis_index("tp")
    peers = [lax.rem(tp_id + d, tp) for d in range(1, tp)]
    greet([(sp_id, p) for p in peers])

    def columns(index):
        return pl.ds(pl.multiple_of(index * width, width), width)

    copies = []
    for d in range(1, tp):
        copy = remote(
            part_ref.at[:, columns(peers[d - 1])],
            landed.at[d - 1],
            send_sem.at[d - 1],
            recv_sem.at[d - 1],
            sp_id,
            peers[d - 1],
        )
        copy.start()
        copies.append(copy)
    total = part_ref[:, columns(tp_id)].astype(jnp.float32)
    for d in range(1, tp):
        copies[d - 1].wait()
        total = total + landed[d - 1].astype(jnp.float32)
    out_ref[...] = (res_ref[...].astype(jnp.float32) + total).astype(jnp.bfloat16)


def near_first(count):
    order = [0]
    for d in range(1, count // 2 + 1):
        order.append(d)
        if count - d != d:
            order.append(count - d)
    return order


def square(tp_id):
    low = lax.rem(tp_id, 2)
    high = tp_id // 2
    return 2 * high + 1 - low, 2 * (1 - high) + low, 2 * (1 - high) + 1 - low


def dispatch_kernel(sp, tp, x_ref, out_ref, z_send, z_recv, t_send, t_recv, own_sem):
    cap = x_ref.shape[0] // sp
    width = x_ref.shape[1]
    half = cap // 2
    sp_id, tp_id = lax.axis_index("sp"), lax.axis_index("tp")
    greet(
        [(lax.rem(sp_id + d, sp), tp_id) for d in range(1, sp)]
        + [(sp_id, lax.rem(tp_id + d, tp)) for d in range(1, tp)]
    )

    def place(source, owner, part=None):
        first = source * cap
        if part is not None:
            first = first + part * half
        count = cap if part is None else half
        return out_ref.at[
            pl.ds(pl.multiple_of(first, half), count),
            pl.ds(pl.multiple_of(owner * width, width), width),
        ]

    def rows(source, part=None):
        first = source * cap
        if part is not None:
            first = first + part * half
        return x_ref.at[pl.ds(pl.multiple_of(first, half), cap if part is None else half), :]

    order = near_first(sp)
    z_copies = {}
    for d in order[1:]:
        target = lax.rem(sp_id + d, sp)
        z_copies[d] = remote(rows(target), place(sp_id, tp_id), z_send.at[d], z_recv.at[d], target, tp_id)
        z_copies[d].start()
    own = pltpu.make_async_copy(rows(sp_id), place(sp_id, tp_id), own_sem)
    own.start()

    def source_of(d):
        return lax.rem(sp_id + sp - d, sp)

    started = []
    if tp == 4:
        near, far, across = square(tp_id)

        def send(d, part, target, slot, owner):
            copy = remote(
                place(source_of(d), owner, part),
                place(source_of(d), owner, part),
                t_send.at[d, slot],
                t_recv.at[d, slot],
                sp_id,
                target,
            )
            copy.start()
            started.append(copy)
            return copy

        def relay(entry):
            d, to_near, to_far = entry
            to_near[0].wait_recv()
            fourth = send(d, 0, far, 4, near)
            to_far[1].wait_recv()
            fifth = send(d, 1, near, 5, far)
            return [to_near[1], to_far[0], fourth, fifth]

        waiting, rest = None, []
        for d in order:
            if d == 0:
                own.wait()
            else:
                z_copies[d].wait_recv()
            to_near = [send(d, 0, near, 0, tp_id), None]
            to_far = [None, send(d, 1, far, 3, tp_id)]
            to_near[1] = send(d, 1, near, 1, tp_id)
            to_far[0] = send(d, 0, far, 2, tp_id)
            if waiting is not None:
                rest += relay(waiting)
            waiting = (d, to_near, to_far)
        rest += relay(waiting)
        for copy in rest:
            copy.wait_recv()
    else:
        for d in order:
            if d == 0:
                own.wait()
            else:
                z_copies[d].wait_recv()
            for t in range(1, tp):
                copy = remote(
                    place(source_of(d), tp_id),
                    place(source_of(d), tp_id),
                    t_send.at[d, t],
                    t_recv.at[d, t],
                    sp_id,
                    lax.rem(tp_id + t, tp),
                )
                copy.start()
                started.append(copy)
        for copy in started:
            copy.wait_recv()
    for copy in started:
        copy.wait_send()
    for d in order[1:]:
        z_copies[d].wait_send()


def return_kernel(sp, tp, x_ref, out_ref, landed, turned, summed, t_send, t_recv, z_send, z_recv):
    cap = x_ref.shape[0] // sp
    width = out_ref.shape[1]
    half = cap // 2
    sp_id, tp_id = lax.axis_index("sp"), lax.axis_index("tp")
    greet(
        [(lax.rem(sp_id + d, sp), tp_id) for d in range(1, sp)]
        + [(sp_id, lax.rem(tp_id + d, tp)) for d in range(1, tp)]
    )

    def rows_at(target, part=None):
        first = target * cap
        if part is not None:
            first = first + part * half
        return pl.ds(pl.multiple_of(first, half), cap if part is None else half)

    def columns(owner):
        return pl.ds(pl.multiple_of(owner * width, width), width)

    order = near_first(sp)[::-1]
    started, z_copies = [], []

    def push(src, dst, d, slot, target):
        copy = remote(src, dst, t_send.at[d, slot], t_recv.at[d, slot], sp_id, target)
        copy.start()
        started.append(copy)
        return copy

    def deliver(d, target):
        if d == 0:
            return
        copy = remote(
            summed.at[d], out_ref.at[rows_at(sp_id), :], z_send.at[d], z_recv.at[d], target, tp_id
        )
        copy.start()
        z_copies.append(copy)

    def f32(value):
        return value.astype(jnp.float32)

    def place_sum(d, part, value):
        piece = pl.ds(part * half, half)
        summed[d, piece, :] = value.astype(jnp.bfloat16)
        if d == 0:
            out_ref[rows_at(sp_id, part), :] = value.astype(jnp.bfloat16)

    targets = {d: lax.rem(sp_id + d, sp) for d in order}
    if tp == 4:
        near, far, across = square(tp_id)
        first = {}

        def open_block(d):
            target = targets[d]
            first[d] = [
                push(x_ref.at[rows_at(target, 0), columns(across)], landed.at[d, 1], d, 1, near),
                push(x_ref.at[rows_at(target, 1), columns(across)], landed.at[d, 3], d, 3, far),
                push(x_ref.at[rows_at(target, 0), columns(near)], landed.at[d, 0], d, 0, near),
                push(x_ref.at[rows_at(target, 1), columns(far)], landed.at[d, 2], d, 2, far),
            ]

        second = {}

        def turn_block(d):
            target = targets[d]
            first[d][0].wait_recv()
            turned[d, 0] = (f32(x_ref[rows_at(target, 0), columns(far)]) + f32(landed[d, 1])).astype(jnp.bfloat16)
            first[d][1].wait_recv()
            turned[d, 1] = (f32(x_ref[rows_at(target, 1), columns(near)]) + f32(landed[d, 3])).astype(jnp.bfloat16)
            second[d] = [
                push(turned.at[d, 0], landed.at[d, 4], d, 4, far),
                push(turned.at[d, 1], landed.at[d, 5], d, 5, near),
            ]

        def close_block(d):
            target = targets[d]
            first[d][2].wait_recv()
            second[d][0].wait_recv()
            place_sum(d, 0, f32(x_ref[rows_at(target, 0), columns(tp_id)]) + f32(landed[d, 0]) + f32(landed[d, 4]))
            first[d][3].wait_recv()
            second[d][1].wait_recv()
            place_sum(d, 1, f32(x_ref[rows_at(target, 1), columns(tp_id)]) + f32(landed[d, 2]) + f32(landed[d, 5]))
            deliver(d, target)

        count = len(order)
        for i in range(count + 2):
            if i < count:
                open_block(order[i])
            if 0 <= i - 1 < count:
                turn_block(order[i - 1])
            if 0 <= i - 2 < count:
                close_block(order[i - 2])
    else:
        pushed = {}
        for d in order:
            pushed[d] = []
            for t in range(1, tp):
                owner = lax.rem(tp_id + t, tp)
                for part in range(2):
                    slot = 2 * (t - 1) + part
                    pushed[d].append(
                        push(x_ref.at[rows_at(targets[d], part), columns(owner)], landed.at[d, slot], d, slot, owner)
                    )
        for d in order:
            for part in range(2):
                value = f32(x_ref[rows_at(targets[d], part), columns(tp_id)])
                for t in range(1, tp):
                    pushed[d][2 * (t - 1) + part].wait_recv()
                    value = value + f32(landed[d, 2 * (t - 1) + part])
                place_sum(d, part, value)
            deliver(d, targets[d])
    for copy in started:
        copy.wait_send()
    for copy in z_copies:
        copy.wait()


def attention_kernel(
    groups,
    start_ref,
    joined_ref,
    nope_ref,
    rope_ref,
    key_major_ref,
    value_major_ref,
    key_minor_ref,
    value_minor_ref,
    out_major_ref,
    out_minor_ref,
    key_a,
    value_a,
    key_b,
    value_b,
):
    latent = key_major_ref.shape[0]
    tok_rows = nope_ref.shape[1]
    rows_f = joined_ref[:, :latent]
    tail = joined_ref[:, latent:]
    for kept, weight in (
        (key_a, key_major_ref),
        (value_a, value_major_ref),
        (key_b, key_minor_ref),
        (value_b, value_minor_ref),
    ):
        kept[...] = jnp.dot(rows_f, weight[...], preferred_element_type=jnp.float32).astype(jnp.bfloat16)
    total_keys = joined_ref.shape[0]
    shape = (tok_rows, total_keys)
    visible = lax.broadcasted_iota(jnp.int32, shape, 1) <= start_ref[0] + lax.broadcasted_iota(jnp.int32, shape, 0)
    contract = (((1,), (1,)), ((), ()))
    index = 0
    for kept_key, kept_value, out_ref, heads, pack, scale in (
        (key_a, value_a, out_major_ref, *groups[0]),
        (key_b, value_b, out_minor_ref, *groups[1]),
    ):
        tile = kept_key.shape[1] // (-(-heads // pack))
        lanes = lax.broadcasted_iota(jnp.int32, (tok_rows, tile), 1)
        for first in range(0, heads, pack):
            columns = pl.ds(first // pack * tile, tile)
            result = None
            for member in range(min(pack, heads - first)):
                scores = lax.dot_general(
                    nope_ref[index], kept_key[:, columns], contract, preferred_element_type=jnp.float32
                ) + lax.dot_general(rope_ref[index], tail, contract, preferred_element_type=jnp.float32)
                scores = jnp.where(visible, scores * scale, -jnp.inf)
                weights = jnp.exp(scores - jnp.max(scores, axis=1, keepdims=True))
                totals = jnp.sum(weights, axis=1, keepdims=True)
                summed = jnp.dot(
                    weights.astype(jnp.bfloat16), kept_value[:, columns], preferred_element_type=jnp.float32
                ) / totals
                result = summed if result is None else jnp.where(lanes < member * (tile // pack), result, summed)
                index += 1
            out_ref[:, columns] = result.astype(jnp.bfloat16)


def expert_kernel(x_ref, gain_ref, gate_ref, up_ref, down_ref, out_ref, normed, total):
    step = pl.program_id(0)

    @pl.when(step == 0)
    def _():
        rows_f = x_ref[...].astype(jnp.float32)
        power = jnp.mean(rows_f * rows_f, axis=1, keepdims=True)
        normed[...] = (rows_f * lax.rsqrt(power + norm_eps) * gain_ref[...]).astype(jnp.bfloat16)

    rows = normed[...]
    gate_pre = jnp.dot(rows, gate_ref[0], preferred_element_type=jnp.float32)
    up_pre = jnp.dot(rows, up_ref[0], preferred_element_type=jnp.float32)
    hidden = (gate_pre / (1.0 + jnp.exp(-gate_pre)) * up_pre).astype(jnp.bfloat16)
    part = jnp.dot(hidden, down_ref[0], preferred_element_type=jnp.float32)
    last = pl.num_programs(0) - 1

    @pl.when((step == 0) & (last > 0))
    def _():
        total[...] = part

    @pl.when((step > 0) & (step < last))
    def _():
        total[...] += part

    @pl.when((step == last) & (last > 0))
    def _():
        out_ref[...] = (total[...] + part).astype(jnp.bfloat16)

    @pl.when(last == 0)
    def _():
        out_ref[...] = part.astype(jnp.bfloat16)


def flip(index, offset):
    step = 1
    while step <= offset:
        if offset & step:
            index = index + step * (1 - 2 * lax.rem(index // step, 2))
        step *= 2
    return index


def moe_kernel(
    sp,
    x_ref,
    ids_ref,
    ids_t_ref,
    mix_ref,
    gain_ref,
    gate_ref,
    up_ref,
    down_ref,
    out_ref,
    gate,
    up,
    down,
    placed,
    rows_in,
    normed,
    hidden,
    part,
    landed,
    turned,
    summed,
    returned,
    hot,
    load_sem,
    z_send,
    z_recv,
    t_send,
    t_recv,
    r_send,
    r_recv,
    y_send,
    y_recv,
):
    tok_rows, width = x_ref.shape
    features = rows_in.shape[2]
    chips = sp // 2
    slots = placed.shape[0]
    cap = slots // sp
    units = gate.shape[1]
    sp_id, tp_id = lax.axis_index("sp"), lax.axis_index("tp")
    near, far, across = square(tp_id)

    loads = []
    pieces = load_sem.shape[1]
    for index, (src, dst) in enumerate(((gate_ref, gate), (up_ref, up), (down_ref, down))):
        rows = dst.shape[0] // pieces
        for piece in range(pieces):
            span = pl.ds(piece * rows, rows)
            copy = pltpu.make_async_copy(src.at[0, span, :], dst.at[span, :], load_sem.at[index, piece])
            copy.start()
            loads.append(copy)

    barrier = pltpu.get_barrier_semaphore()
    for offset in range(1, sp):
        pl.semaphore_signal(barrier, inc=1, device_id=(flip(sp_id, offset), tp_id), device_id_type=MESH)
    for peer in (near, far, across):
        pl.semaphore_signal(barrier, inc=1, device_id=(sp_id, peer), device_id_type=MESH)

    lanes = lax.broadcasted_iota(jnp.int32, (sp, tok_rows), 0)
    matches_t = [(lanes == ids_t_ref[j : j + 1, :]).astype(jnp.float32) for j in range(TOP)]
    order = (tok_rows, tok_rows)
    before_t = (lax.broadcasted_iota(jnp.int32, order, 0) < lax.broadcasted_iota(jnp.int32, order, 1)).astype(
        jnp.bfloat16
    )
    named_t = functools.reduce(lambda a, b: a + b, matches_t)
    earlier_t = jnp.dot(named_t.astype(jnp.bfloat16), before_t, preferred_element_type=jnp.float32)
    slot_rows = lax.broadcasted_iota(jnp.int32, (slots, tok_rows), 0)
    select = None
    for j in range(TOP):
        rank = jnp.sum(matches_t[j] * earlier_t, axis=0, keepdims=True).astype(jnp.int32)
        earlier_t = earlier_t + matches_t[j]
        chosen = jnp.where(slot_rows == ids_t_ref[j : j + 1, :] * cap + rank, 1.0, 0.0)
        select = chosen if select is None else select + chosen
    placed[...] = jnp.dot(select.astype(jnp.bfloat16), x_ref[...], preferred_element_type=jnp.float32).astype(
        jnp.bfloat16
    )

    def block(index):
        return pl.ds(pl.multiple_of(index * cap, cap), cap)

    def columns(owner):
        return pl.ds(pl.multiple_of(owner * width, width), width)

    own_columns = columns(tp_id)
    pl.semaphore_wait(barrier, sp - 1 + 3)

    z_copies = {}
    for offset in range(1, sp):
        target = flip(sp_id, offset)
        k, q = offset // 2, offset % 2
        z_copies[offset] = remote(
            placed.at[block(target), :],
            rows_in.at[k, pl.ds(q * cap, cap), own_columns],
            z_send.at[offset],
            z_recv.at[offset],
            target,
            tp_id,
        )
        z_copies[offset].start()
    rows_in[0, 0:cap, own_columns] = placed[block(sp_id), :]

    started = []

    def pass_on(k, q, owner, slot, target):
        place = rows_in.at[k, pl.ds(q * cap, cap), columns(owner)]
        copy = remote(place, place, t_send.at[k, slot], t_recv.at[k, slot], sp_id, target)
        copy.start()
        started.append(copy)
        return copy

    arriving = {}

    def open_chunk(k):
        if k == 0:
            first = [pass_on(0, 0, tp_id, 0, near), pass_on(0, 0, tp_id, 2, far)]
            z_copies[1].wait_recv()
            second = [pass_on(0, 1, tp_id, 3, far), pass_on(0, 1, tp_id, 1, near)]
            arriving[0] = [first[0], second[1], first[1], second[0]]
            return
        z_copies[2 * k].wait_recv()
        a = pass_on(k, 0, tp_id, 0, near)
        z_copies[2 * k + 1].wait_recv()
        d = pass_on(k, 1, tp_id, 3, far)
        b = pass_on(k, 1, tp_id, 1, near)
        c = pass_on(k, 0, tp_id, 2, far)
        arriving[k] = [a, b, c, d]

    def relay(k):
        a, b, c, d = arriving[k]
        a.wait_recv()
        e = pass_on(k, 0, near, 4, far)
        d.wait_recv()
        f = pass_on(k, 1, far, 5, near)
        arriving[k] = [b, c, e, f]

    def ready(k):
        for copy in arriving[k]:
            copy.wait_recv()
        rows = rows_in[k].astype(jnp.float32)
        power = jnp.mean(rows * rows, axis=1, keepdims=True)
        normed[...] = (rows * lax.rsqrt(power + norm_eps) * gain_ref[...]).astype(jnp.bfloat16)

    def expand():
        tile = 256
        rows = normed[...]
        for first in range(0, units, tile):
            span = slice(first, first + tile)
            gate_pre = jnp.dot(rows, gate[:, span], preferred_element_type=jnp.float32)
            up_pre = jnp.dot(rows, up[:, span], preferred_element_type=jnp.float32)
            hidden[:, span] = (gate_pre / (1.0 + jnp.exp(-gate_pre)) * up_pre).astype(jnp.bfloat16)

    def push(src, dst, k, slot, target):
        copy = remote(src, dst, r_send.at[k, slot], r_recv.at[k, slot], sp_id, target)
        copy.start()
        started.append(copy)
        return copy

    halves = (pl.ds(0, cap), pl.ds(cap, cap))
    leaving, turning = {}, {}

    def contract(k):
        rows = hidden[...]

        def fill(owner):
            part[k, :, columns(owner)] = jnp.dot(
                rows, down[:, columns(owner)], preferred_element_type=jnp.float32
            ).astype(jnp.bfloat16)

        def send(q, owner, slot, target):
            return push(part.at[k, halves[q], columns(owner)], landed.at[k, slot], k, slot, target)

        fill(across)
        second = send(0, across, 1, near)
        fourth = send(1, across, 3, far)
        fill(near)
        first = send(0, near, 0, near)
        fill(far)
        third = send(1, far, 2, far)
        fill(tp_id)
        leaving[k] = [first, second, third, fourth]

    def f32(value):
        return value.astype(jnp.float32)

    def turn(k):
        leaving[k][1].wait_recv()
        turned[k, 0] = (f32(part[k, halves[0], columns(far)]) + f32(landed[k, 1])).astype(jnp.bfloat16)
        a = push(turned.at[k, 0], landed.at[k, 4], k, 4, far)
        leaving[k][3].wait_recv()
        turned[k, 1] = (f32(part[k, halves[1], columns(near)]) + f32(landed[k, 3])).astype(jnp.bfloat16)
        b = push(turned.at[k, 1], landed.at[k, 5], k, 5, near)
        turning[k] = [a, b]

    back = {}

    def close(k):
        for q in range(2):
            leaving[k][2 * q].wait_recv()
            turning[k][q].wait_recv()
            value = f32(part[k, halves[q], own_columns]) + f32(landed[k, 2 * q]) + f32(landed[k, 4 + q])
            offset = 2 * k + q
            if offset == 0:
                returned[block(sp_id), :] = value.astype(jnp.bfloat16)
                continue
            summed[k, q] = value.astype(jnp.bfloat16)
            back[offset] = remote(
                summed.at[k, q],
                returned.at[block(sp_id), :],
                y_send.at[offset],
                y_recv.at[offset],
                flip(sp_id, offset),
                tp_id,
            )
            back[offset].start()

    open_chunk(0)
    relay(0)
    open_chunk(1)
    lanes = lax.broadcasted_iota(jnp.int32, (tok_rows, sp), 1)
    matches = [(lanes == ids_ref[:, j : j + 1]).astype(jnp.float32) for j in range(TOP)]
    before = (lax.broadcasted_iota(jnp.int32, order, 0) > lax.broadcasted_iota(jnp.int32, order, 1)).astype(
        jnp.bfloat16
    )
    named = functools.reduce(lambda a, b: a + b, matches)
    earlier = jnp.dot(before, named.astype(jnp.bfloat16), preferred_element_type=jnp.float32)
    slot_lanes = lax.broadcasted_iota(jnp.int32, (tok_rows, slots), 1)
    for j in range(TOP):
        rank = jnp.sum(matches[j] * earlier, axis=1, keepdims=True).astype(jnp.int32)
        earlier = earlier + matches[j]
        hot[j] = jnp.where(slot_lanes == ids_ref[:, j : j + 1] * cap + rank, 1.0, 0.0).astype(jnp.bfloat16)
    for copy in loads:
        copy.wait()
    relay(1)
    if chips > 2:
        open_chunk(2)
    turns = list(range(1, chips)) + [0]
    for index, k in enumerate(turns):
        ready(k)
        expand()
        if index + 2 < chips:
            relay(index + 2)
        if index + 3 < chips:
            open_chunk(index + 3)
        contract(k)
        if index >= 1:
            turn(turns[index - 1])
        if index >= 2:
            close(turns[index - 2])
    turn(turns[-1])
    close(turns[-2])
    close(turns[-1])
    for offset in range(1, sp):
        back[offset].wait_recv()
    total = x_ref[...].astype(jnp.float32)
    for j in range(TOP):
        total = total + jnp.dot(hot[j], returned[...], preferred_element_type=jnp.float32) * mix_ref[:, j : j + 1]
    out_ref[...] = total.astype(jnp.bfloat16)
    for copy in started:
        copy.wait_send()
    for offset in range(1, sp):
        z_copies[offset].wait_send()
        back[offset].wait_send()


def fused_experts(sp, tp, stream_mid, ids, mix, gain, gate_proj, up_proj, down_proj):
    tok_rows, width = stream_mid.shape
    cap = 2 * tok_rows * TOP // sp
    slots = sp * cap
    chips = sp // 2
    features = tp * width
    units = gate_proj.shape[2]
    dma = pltpu.SemaphoreType.DMA
    vmem = pl.BlockSpec(memory_space=pltpu.VMEM)
    hbm = pl.BlockSpec(memory_space=pl.ANY)
    bf16 = jnp.bfloat16
    return pl.pallas_call(
        functools.partial(moe_kernel, sp),
        out_shape=jax.ShapeDtypeStruct((tok_rows, width), bf16),
        in_specs=[vmem] * 5 + [hbm] * 3,
        out_specs=vmem,
        scratch_shapes=[
            pltpu.VMEM((features, units), bf16),
            pltpu.VMEM((features, units), bf16),
            pltpu.VMEM((units, features), bf16),
            pltpu.VMEM((slots, width), bf16),
            pltpu.VMEM((chips, 2 * cap, features), bf16),
            pltpu.VMEM((2 * cap, features), bf16),
            pltpu.VMEM((2 * cap, units), bf16),
            pltpu.VMEM((chips, 2 * cap, features), bf16),
            pltpu.VMEM((chips, 6, cap, width), bf16),
            pltpu.VMEM((chips, 2, cap, width), bf16),
            pltpu.VMEM((chips, 2, cap, width), bf16),
            pltpu.VMEM((slots, width), bf16),
            pltpu.VMEM((TOP, tok_rows, slots), bf16),
            dma((3, 4)),
            dma((sp,)),
            dma((sp,)),
            dma((chips, 6)),
            dma((chips, 6)),
            dma((chips, 6)),
            dma((chips, 6)),
            dma((sp,)),
            dma((sp,)),
        ],
        compiler_params=pltpu.CompilerParams(
            collective_id=4, has_side_effects=True, vmem_limit_bytes=60 * 1024 * 1024
        ),
    )(stream_mid, ids, ids.T, mix, gain.reshape(1, -1), gate_proj, up_proj, down_proj)


def rope_table(count, width):
    half_width = width // 2
    inverse_freq = (1.0 / theta_base ** (np.arange(half_width, dtype=np.float32) * (2.0 / width))).astype(np.float32)
    angles = np.arange(count, dtype=np.float32)[:, None] * inverse_freq[None, :]
    cosine, sine = np.cos(angles), np.sin(angles)
    return np.concatenate([cosine, cosine, -sine, sine], axis=1).astype(np.float32)


def attend_kernel(
    sp,
    heads,
    q_major_ref,
    q_minor_ref,
    latent_ref,
    rope_ref,
    table_ref,
    key_major_ref,
    value_major_ref,
    key_minor_ref,
    value_minor_ref,
    out_major_ref,
    out_minor_ref,
    res_ref,
    stream_ref,
    q_major,
    q_minor,
    rope_raw,
    table,
    weights,
    projection,
    residual,
    blocks,
    queries,
    kept,
    tops,
    sums,
    gathered_out,
    mixed,
    part,
    landed,
    turned,
    load_sem,
    z_send,
    z_recv,
    t_send,
    t_recv,
    s_send,
    s_recv,
    r_send,
    r_recv,
):
    heads_major, heads_minor = heads
    tok_rows, latent = latent_ref.shape
    rope_width = rope_ref.shape[1]
    chips = sp // 2
    tp = 4
    quarter = tok_rows // tp
    pack = 128 // NOPE_MINOR
    sp_id, tp_id = lax.axis_index("sp"), lax.axis_index("tp")
    level, core = sp_id // 2, lax.rem(sp_id, 2)
    sibling = flip(sp_id, 1)
    near, far, across = square(tp_id)
    f32, bf16 = jnp.float32, jnp.bfloat16

    loads = []

    def load(src, dst):
        copy = pltpu.make_async_copy(src, dst, load_sem.at[len(loads)])
        copy.start()
        loads.append(copy)
        return copy

    own_rows = pl.ds(pl.multiple_of(sp_id * tok_rows, tok_rows), tok_rows)
    early = [
        load(latent_ref, blocks.at[0, 0, :, pl.ds(0, latent)]),
        load(rope_ref, rope_raw),
        load(table_ref.at[own_rows, :], table),
    ]
    asked = [load(q_major_ref, q_major), load(q_minor_ref, q_minor)]
    spans, first = [], 0
    for ref in (key_major_ref, key_minor_ref, value_major_ref, value_minor_ref):
        span = pl.ds(first, ref.shape[1])
        asked.append(load(ref, weights.at[:, span]))
        spans.append(span)
        first += ref.shape[1]
    split = out_major_ref.shape[0]
    late = [
        load(out_major_ref, projection.at[pl.ds(0, split), :]),
        load(out_minor_ref, projection.at[pl.ds(split, out_minor_ref.shape[0]), :]),
        load(res_ref, residual),
    ]

    barrier = pltpu.get_barrier_semaphore()
    for offset in range(1, chips):
        pl.semaphore_signal(barrier, inc=1, device_id=(flip(sp_id, 2 * offset), tp_id), device_id_type=MESH)
    pl.semaphore_signal(barrier, inc=1, device_id=(sibling, tp_id), device_id_type=MESH)
    for peer in (near, far, across):
        pl.semaphore_signal(barrier, inc=1, device_id=(sp_id, peer), device_id_type=MESH)

    half = rope_width // 2

    def rotate(x):
        x = x.astype(f32)
        swapped = jnp.concatenate([x[:, half:], x[:, :half]], axis=1)
        return (x * table[:, :rope_width] + swapped * table[:, rope_width:]).astype(bf16)

    for copy in early:
        copy.wait()
    tail = blocks.shape[3] - latent
    pad = jnp.zeros((tok_rows, tail - rope_width), bf16)
    blocks[0, 0, :, latent:] = jnp.concatenate([rotate(rope_raw[...]), pad], axis=1)
    pl.semaphore_wait(barrier, chips - 1 + 1 + 3)

    own_quarter = pl.ds(pl.multiple_of(tp_id * quarter, quarter), quarter)

    def lift(d):
        return remote(
            blocks.at[0, 0, own_quarter, :],
            blocks.at[d, 0, own_quarter, :],
            z_send.at[d],
            z_recv.at[d],
            sp_id + 2 * d,
            tp_id,
        )

    def spread(d, slot):
        place = blocks.at[d, 0, own_quarter, :]
        return remote(place, place, t_send.at[d, slot], t_recv.at[d, slot], sp_id, (near, far, across)[slot])

    def share(d):
        return remote(blocks.at[d, 0], blocks.at[d, 1], s_send.at[d], s_recv.at[d], sibling, tp_id)

    for d in range(1, chips):

        @pl.when(level + d < chips)
        def _():
            lift(d).start()

    share(0).start()

    for copy in asked:
        copy.wait()
    zeros = jnp.zeros((tok_rows, 128 - rope_width), bf16)
    lanes = lax.broadcasted_iota(jnp.int32, (tok_rows, 128), 1)
    for h in range(heads_major):
        first = h * (NOPE_MAJOR + rope_width)
        queries[h, :, :128] = q_major[:, first : first + NOPE_MAJOR]
        turned_part = rotate(q_major[:, first + NOPE_MAJOR : first + NOPE_MAJOR + rope_width])
        queries[h, :, 128:] = jnp.concatenate([turned_part, zeros], axis=1)
    blank = jnp.zeros((tok_rows, NOPE_MINOR), bf16)
    for h in range(heads_minor):
        first = h * (NOPE_MINOR + rope_width)
        member = h % pack
        nope = q_minor[:, first : first + NOPE_MINOR]
        row = [blank] * member + [nope] + [blank] * (pack - 1 - member)
        queries[heads_major + h, :, :128] = jnp.concatenate(row, axis=1)
        turned_part = rotate(q_minor[:, first + NOPE_MINOR : first + NOPE_MINOR + rope_width])
        queries[heads_major + h, :, 128:] = jnp.concatenate([turned_part, zeros], axis=1)

    keys = 2 * tok_rows
    log2e = 1.4426950408889634
    contract = (((1,), (1,)), ((), ()))

    def project(d):
        for q in range(2):
            rows = blocks[d, q, :, :latent]
            kept[pl.ds(q * tok_rows, tok_rows), :] = jnp.dot(rows, weights[...], preferred_element_type=f32).astype(
                bf16
            )

    def attend(d):
        tails = jnp.concatenate([blocks[d, 0, :, latent:], blocks[d, 1, :, latent:]], axis=0)
        for h in range(heads_major + heads_minor):
            if h < heads_major:
                tile, scale = h, (NOPE_MAJOR + rope_width) ** (-0.5)
                key_at, value_at = tile * 128, spans[2].start + tile * 128
            else:
                tile, scale = (h - heads_major) // pack, (NOPE_MINOR + rope_width) ** (-0.5)
                key_at, value_at = spans[1].start + tile * 128, spans[3].start + tile * 128
            key = jnp.concatenate([kept[:, key_at : key_at + 128], tails], axis=1)
            scores = lax.dot_general(queries[h], key, contract, preferred_element_type=f32) * (scale * log2e)
            if d == 0:
                spot = lax.broadcasted_iota(jnp.int32, (tok_rows, keys), 1)
                row = lax.broadcasted_iota(jnp.int32, (tok_rows, keys), 0)
                limit = jnp.where(spot < tok_rows, row, keys * core - 1)
                scores = jnp.where(spot <= limit, scores, -jnp.inf)
            peak = jnp.max(scores, axis=1, keepdims=True)
            if d > 0:
                before = tops[h][:, :1]
                peak = jnp.maximum(before, peak)
                fade = jnp.exp2(before - peak)
            chance = jnp.exp2(scores - peak)
            total = jnp.sum(chance, axis=1, keepdims=True)
            summed = jnp.dot(chance.astype(bf16), kept[:, value_at : value_at + 128], preferred_element_type=f32)
            if d > 0:
                total = total + sums[h][:, :1] * fade
                summed = summed + gathered_out[h] * fade
            tops[h] = jnp.broadcast_to(peak, (tok_rows, 128))
            sums[h] = jnp.broadcast_to(total, (tok_rows, 128))
            gathered_out[h] = summed

    def arrival(place, sem):
        return pltpu.make_async_copy(place, place, sem)

    share(0).wait_recv()
    project(0)

    for d in range(1, chips):
        if d == 2 or chips == 2:
            attend(0)

        @pl.when(level >= d)
        def _():
            arrival(blocks.at[d, 0, own_quarter, :], z_recv.at[d]).wait()
            for slot in range(3):
                spread(d, slot).start()

    for d in range(1, chips):

        @pl.when(level >= d)
        def _():
            for slot in range(3):
                spread(d, slot).wait_recv()
            share(d).start()

    for d in range(1, chips):

        @pl.when(level >= d)
        def _():
            share(d).wait_recv()
            project(d)
            attend(d)

    for h in range(heads_major):
        mixed[:, h * 128 : h * 128 + 128] = (gathered_out[h] / sums[h]).astype(bf16)
    for tile in range(-(-heads_minor // pack)):
        result = None
        for member in range(min(pack, heads_minor - tile * pack)):
            h = heads_major + tile * pack + member
            value = gathered_out[h] / sums[h]
            result = value if result is None else jnp.where(lanes < member * NOPE_MINOR, result, value)
        first = (heads_major + tile) * 128
        mixed[:, first : first + 128] = result.astype(bf16)

    width = stream_ref.shape[1]
    for copy in late:
        copy.wait()

    def columns(owner):
        return pl.ds(pl.multiple_of(owner * width, width), width)

    mid = tok_rows // 2
    halves = (pl.ds(0, mid), pl.ds(mid, mid))
    rows = mixed[...]
    started = []

    def fill(owner):
        part[:, columns(owner)] = jnp.dot(rows, projection[:, columns(owner)], preferred_element_type=f32).astype(bf16)

    def push(src, slot, target):
        copy = remote(src, landed.at[slot], r_send.at[slot], r_recv.at[slot], sp_id, target)
        copy.start()
        started.append(copy)
        return copy

    fill(across)
    second = push(part.at[halves[0], columns(across)], 1, near)
    fourth = push(part.at[halves[1], columns(across)], 3, far)
    fill(near)
    first = push(part.at[halves[0], columns(near)], 0, near)
    fill(far)
    third = push(part.at[halves[1], columns(far)], 2, far)
    fill(tp_id)
    second.wait_recv()
    turned[0] = (part[halves[0], columns(far)].astype(f32) + landed[1].astype(f32)).astype(bf16)
    fifth = push(turned.at[0], 4, far)
    fourth.wait_recv()
    turned[1] = (part[halves[1], columns(near)].astype(f32) + landed[3].astype(f32)).astype(bf16)
    sixth = push(turned.at[1], 5, near)
    for q, plain, summed in ((0, first, fifth), (1, third, sixth)):
        plain.wait_recv()
        value = part[halves[q], columns(tp_id)].astype(f32) + residual[halves[q], :].astype(f32)
        value = value + landed[2 * q].astype(f32)
        summed.wait_recv()
        stream_ref[halves[q], :] = (value + landed[4 + q].astype(f32)).astype(bf16)

    for copy in started:
        copy.wait_send()
    share(0).wait_send()
    for d in range(1, chips):

        @pl.when(level + d < chips)
        def _():
            lift(d).wait_send()

        @pl.when(level >= d)
        def _():
            share(d).wait_send()
            for slot in range(3):
                spread(d, slot).wait_send()


def fused_attention(
    sp,
    query_major,
    query_minor,
    latent_rows,
    rope_keys,
    key_up_major,
    value_up_major,
    key_up_minor,
    value_up_minor,
    out_major,
    out_minor,
    residual,
):
    tok_rows, latent = latent_rows.shape
    rope_width = rope_keys.shape[1]
    width = residual.shape[1]
    chips = sp // 2
    heads = (key_up_major.shape[1] // NOPE_MAJOR, key_up_minor.shape[1] // NOPE_MINOR)
    count = heads[0] + heads[1]
    joined = latent + rope_width + -(latent + rope_width) % 128
    kept = key_up_major.shape[1] + key_up_minor.shape[1] + value_up_major.shape[1] + value_up_minor.shape[1]
    mixed = value_up_major.shape[1] + value_up_minor.shape[1]
    dma = pltpu.SemaphoreType.DMA
    bf16 = jnp.bfloat16
    table = jnp.asarray(rope_table(sp * tok_rows, rope_width))
    operands = (
        query_major,
        query_minor,
        latent_rows,
        rope_keys,
        table,
        key_up_major,
        value_up_major,
        key_up_minor,
        value_up_minor,
        out_major,
        out_minor,
        residual,
    )
    return pl.pallas_call(
        functools.partial(attend_kernel, sp, heads),
        out_shape=jax.ShapeDtypeStruct((tok_rows, width), bf16),
        in_specs=[pl.BlockSpec(memory_space=pl.ANY)] * len(operands),
        out_specs=pl.BlockSpec(memory_space=pltpu.VMEM),
        scratch_shapes=[
            pltpu.VMEM(query_major.shape, bf16),
            pltpu.VMEM(query_minor.shape, bf16),
            pltpu.VMEM(rope_keys.shape, bf16),
            pltpu.VMEM((tok_rows, 2 * rope_width), jnp.float32),
            pltpu.VMEM((latent, kept), bf16),
            pltpu.VMEM((mixed, out_major.shape[1]), bf16),
            pltpu.VMEM(residual.shape, bf16),
            pltpu.VMEM((chips, 2, tok_rows, joined), bf16),
            pltpu.VMEM((count, tok_rows, 256), bf16),
            pltpu.VMEM((2 * tok_rows, kept), bf16),
            pltpu.VMEM((count, tok_rows, 128), jnp.float32),
            pltpu.VMEM((count, tok_rows, 128), jnp.float32),
            pltpu.VMEM((count, tok_rows, 128), jnp.float32),
            pltpu.VMEM((tok_rows, mixed), bf16),
            pltpu.VMEM((tok_rows, out_major.shape[1]), bf16),
            pltpu.VMEM((6, tok_rows // 2, width), bf16),
            pltpu.VMEM((2, tok_rows // 2, width), bf16),
            dma((len(operands),)),
            dma((chips,)),
            dma((chips,)),
            dma((chips, 3)),
            dma((chips, 3)),
            dma((chips,)),
            dma((chips,)),
            dma((6,)),
            dma((6,)),
        ],
        compiler_params=pltpu.CompilerParams(
            collective_id=5, has_side_effects=True, vmem_limit_bytes=60 * 1024 * 1024
        ),
    )(*operands)


def run_experts(rows, gain, gate_proj, up_proj, down_proj):
    slots, features = rows.shape
    units = gate_proj.shape[2]
    tile = min(256, units)
    return pl.pallas_call(
        expert_kernel,
        grid=(units // tile,),
        out_shape=jax.ShapeDtypeStruct((slots, features), jnp.bfloat16),
        in_specs=[
            pl.BlockSpec((slots, features), lambda i: (0, 0)),
            pl.BlockSpec((1, features), lambda i: (0, 0)),
            pl.BlockSpec((1, features, tile), lambda i: (0, 0, i)),
            pl.BlockSpec((1, features, tile), lambda i: (0, 0, i)),
            pl.BlockSpec((1, tile, features), lambda i: (0, i, 0)),
        ],
        out_specs=pl.BlockSpec((slots, features), lambda i: (0, 0)),
        scratch_shapes=[
            pltpu.VMEM((slots, features), jnp.bfloat16),
            pltpu.VMEM((slots, features), jnp.float32),
        ],
        compiler_params=pltpu.CompilerParams(vmem_limit_bytes=60 * 1024 * 1024),
    )(rows, gain.reshape(1, -1), gate_proj, up_proj, down_proj)


def pad_columns(array, multiple):
    return jnp.pad(array, ((0, 0), (0, -array.shape[1] % multiple)))


def per_device(
    sp,
    tp,
    query_major,
    query_minor,
    latent_rows,
    rope_keys,
    key_up_major,
    value_up_major,
    key_up_minor,
    value_up_minor,
    out_major,
    out_minor,
    residual,
    norm_gain,
    expert_ids,
    expert_weights,
    gate_proj,
    up_proj,
    down_proj,
):
    tok_rows = query_major.shape[0]
    fast = tp == 4 and sp & (sp - 1) == 0
    fast = fast and tok_rows % 64 == 0 and (2 * tok_rows * TOP // sp) % 16 == 0
    fast = fast and key_up_major.shape[1] % 128 == 0 and key_up_minor.shape[1] % 128 == 0
    if fast:
        stream_mid = fused_attention(
            sp,
            query_major,
            query_minor,
            latent_rows,
            rope_keys,
            key_up_major,
            value_up_major,
            key_up_minor,
            value_up_minor,
            out_major,
            out_minor,
            residual,
        )
        return fused_experts(
            sp, tp, stream_mid, expert_ids, expert_weights, norm_gain, gate_proj, up_proj, down_proj
        )
    row_start = lax.axis_index("sp") * tok_rows
    positions = row_start + jnp.arange(tok_rows, dtype=jnp.int32)
    rope_width = rope_keys.shape[1]
    latent = latent_rows.shape[1]
    rope_rot = rotary(rope_keys, positions).astype(jnp.bfloat16)
    heads_major = key_up_major.shape[1] // NOPE_MAJOR
    heads_minor = key_up_minor.shape[1] // NOPE_MINOR
    shaped_major = query_major.reshape(tok_rows, heads_major, NOPE_MAJOR + rope_width)
    shaped_minor = query_minor.reshape(tok_rows, heads_minor, NOPE_MINOR + rope_width)
    nope_major = shaped_major[:, :, :NOPE_MAJOR]
    nope_minor = shaped_minor[:, :, :NOPE_MINOR]
    turned_major = rotary(shaped_major[:, :, NOPE_MAJOR:], positions).astype(jnp.bfloat16)
    turned_minor = rotary(shaped_minor[:, :, NOPE_MINOR:], positions).astype(jnp.bfloat16)
    scale_major = (NOPE_MAJOR + rope_width) ** (-0.5)
    scale_minor = (NOPE_MINOR + rope_width) ** (-0.5)

    joined = jnp.concatenate(
        [latent_rows, rope_rot, jnp.zeros((tok_rows, -(latent + rope_width) % 128), jnp.bfloat16)], axis=1
    )
    dma = pltpu.SemaphoreType.DMA
    chips = sp // 2
    gathered = comm_call(
        functools.partial(gather_kernel, sp),
        jax.ShapeDtypeStruct((sp * tok_rows, joined.shape[1]), jnp.bfloat16),
        [dma((chips,)), dma((chips,)), dma((chips,)), dma((chips,))],
        0,
        (joined,),
    )
    tail_width = joined.shape[1] - latent

    def by_head(array, width):
        return jnp.pad(array.transpose(1, 0, 2), ((0, 0), (0, 0), (0, width - array.shape[2])))

    pack = 128 // NOPE_MINOR
    spread = nope_minor.transpose(1, 0, 2)
    member = (jnp.arange(heads_minor, dtype=jnp.int32) % pack)[:, None, None]
    spread = jnp.concatenate(
        [jnp.where(member == m, spread, jnp.zeros_like(spread)) for m in range(pack)], axis=2
    )
    nope_all = jnp.concatenate([by_head(nope_major, 128), spread], axis=0)
    rope_all = jnp.concatenate([by_head(turned_major, tail_width), by_head(turned_minor, tail_width)], axis=0)
    minor_weights = [pad_columns(key_up_minor, 128), pad_columns(value_up_minor, 128)]
    minor_width = minor_weights[0].shape[1]
    keys = sp * tok_rows
    vmem = pl.BlockSpec(memory_space=pltpu.VMEM)
    attn_major, attn_minor = pl.pallas_call(
        functools.partial(attention_kernel, ((heads_major, 1, scale_major), (heads_minor, pack, scale_minor))),
        out_shape=(
            jax.ShapeDtypeStruct((tok_rows, value_up_major.shape[1]), jnp.bfloat16),
            jax.ShapeDtypeStruct((tok_rows, minor_width), jnp.bfloat16),
        ),
        in_specs=[pl.BlockSpec(memory_space=pltpu.SMEM)] + [vmem] * 7,
        out_specs=(vmem, vmem),
        scratch_shapes=[
            pltpu.VMEM((keys, key_up_major.shape[1]), jnp.bfloat16),
            pltpu.VMEM((keys, value_up_major.shape[1]), jnp.bfloat16),
            pltpu.VMEM((keys, minor_width), jnp.bfloat16),
            pltpu.VMEM((keys, minor_width), jnp.bfloat16),
        ],
        compiler_params=pltpu.CompilerParams(vmem_limit_bytes=60 * 1024 * 1024),
    )(
        row_start.reshape(1).astype(jnp.int32),
        gathered,
        nope_all,
        rope_all,
        key_up_major,
        value_up_major,
        *minor_weights,
    )
    attn_minor = attn_minor[:, : value_up_minor.shape[1]]
    partial_value = jnp.dot(attn_major, out_major, preferred_element_type=jnp.float32)
    partial_value = partial_value + jnp.dot(
        attn_minor, out_minor, preferred_element_type=jnp.float32
    )
    width = residual.shape[1]
    stream_mid = comm_call(
        functools.partial(reduce_kernel, tp),
        jax.ShapeDtypeStruct((tok_rows, width), jnp.bfloat16),
        [pltpu.VMEM((tp - 1, tok_rows, width), jnp.bfloat16), dma((tp - 1,)), dma((tp - 1,))],
        1,
        (partial_value.astype(jnp.bfloat16), residual),
    )
    experts = sp
    capacity = 2 * tok_rows * TOP // experts
    slots = experts * capacity
    slot_list = slot_ids(expert_ids, experts, capacity)
    slot_numbers = jnp.arange(slots, dtype=jnp.int32)
    by_slot = slot_list.T
    select = (slot_numbers[:, None] == by_slot[0][None, :]).astype(jnp.bfloat16)
    for j in range(1, TOP):
        select = select + (slot_numbers[:, None] == by_slot[j][None, :]).astype(jnp.bfloat16)
    placed = jnp.dot(select, stream_mid, preferred_element_type=jnp.float32).astype(jnp.bfloat16)
    slots_t = 6 if tp == 4 else tp
    arrived = comm_call(
        functools.partial(dispatch_kernel, sp, tp),
        jax.ShapeDtypeStruct((slots, tp * width), jnp.bfloat16),
        [dma((sp,)), dma((sp,)), dma((sp, slots_t)), dma((sp, slots_t)), dma],
        2,
        (placed,),
    )
    down_part = run_experts(arrived, norm_gain, gate_proj, up_proj, down_proj)
    pieces = 6 if tp == 4 else 2 * (tp - 1)
    half = capacity // 2
    flat_out = comm_call(
        functools.partial(return_kernel, sp, tp),
        jax.ShapeDtypeStruct((slots, width), jnp.bfloat16),
        [
            pltpu.VMEM((sp, pieces, half, width), jnp.bfloat16),
            pltpu.VMEM((sp, 2, half, width), jnp.bfloat16),
            pltpu.VMEM((sp, capacity, width), jnp.bfloat16),
            dma((sp, pieces)),
            dma((sp, pieces)),
            dma((sp,)),
            dma((sp,)),
        ],
        3,
        (down_part,),
    )
    mixed = stream_mid.astype(jnp.float32)
    for j in range(TOP):
        hot = (slot_list[:, j : j + 1] == slot_numbers[None, :]).astype(jnp.bfloat16)
        mixed = mixed + jnp.dot(hot, flat_out, preferred_element_type=jnp.float32) * expert_weights[:, j : j + 1]
    return mixed.astype(jnp.bfloat16)


def solution(mesh):
    in_specs = (
        P("sp", "tp"),
        P("sp", "tp"),
        P("sp", None),
        P("sp", None),
        P(None, "tp"),
        P(None, "tp"),
        P(None, "tp"),
        P(None, "tp"),
        P("tp", None),
        P("tp", None),
        P("sp", "tp"),
        P(),
        P("sp", None),
        P("sp", None),
        P("sp", None, "tp"),
        P("sp", None, "tp"),
        P("sp", "tp", None),
    )
    out_specs = P("sp", "tp")
    return jax.shard_map(
        functools.partial(per_device, mesh.shape["sp"], mesh.shape["tp"]),
        mesh=mesh,
        in_specs=in_specs,
        out_specs=out_specs,
        check_vma=False,
    )
```

```python
import functools

import jax
import jax.numpy as jnp
import numpy as np
from jax import lax
from jax.experimental import pallas as pl
from jax.experimental.pallas import tpu as pltpu
from jax.sharding import PartitionSpec as P

NOPE_MAJOR = 128
NOPE_MINOR = 64
TOP = 2
MESH = pl.DeviceIdType.MESH

theta_base = 10000.0
norm_eps = 1e-06


def rotary(values, positions):
    half_width = values.shape[-1] // 2
    inverse_freq = 1.0 / theta_base ** (
        jnp.arange(half_width, dtype=jnp.float32) * (2.0 / values.shape[-1])
    )
    angles = positions.astype(jnp.float32)[:, None] * inverse_freq[None, :]
    view_shape = (angles.shape[0],) + (1,) * (values.ndim - 2) + (half_width,)
    cosine = jnp.cos(angles).reshape(view_shape)
    sine_table = jnp.sin(angles).reshape(view_shape)
    lower_half = values[..., :half_width].astype(jnp.float32)
    upper_half = values[..., half_width:].astype(jnp.float32)
    return jnp.concatenate(
        [
            lower_half * cosine - upper_half * sine_table,
            upper_half * cosine + lower_half * sine_table,
        ],
        axis=-1,
    )


def slot_ids(route_block, experts, capacity):
    pairs = route_block.reshape(-1)
    matches = pairs[:, None] == jnp.arange(experts, dtype=jnp.int32)[None, :]
    order = jnp.arange(pairs.shape[0], dtype=jnp.int32)
    earlier = (order[:, None] > order[None, :]).astype(jnp.bfloat16)
    ranks = jnp.dot(earlier, matches.astype(jnp.bfloat16), preferred_element_type=jnp.float32)
    rank = jnp.sum(jnp.where(matches, ranks, 0.0), axis=1).astype(jnp.int32)
    return (pairs * capacity + rank).reshape(route_block.shape)


def remote(src, dst, send_sem, recv_sem, sp_id, tp_id):
    return pltpu.make_async_remote_copy(
        src_ref=src,
        dst_ref=dst,
        send_sem=send_sem,
        recv_sem=recv_sem,
        device_id=(sp_id, tp_id),
        device_id_type=MESH,
    )


def greet(partners):
    barrier = pltpu.get_barrier_semaphore()
    for sp_id, tp_id in partners:
        pl.semaphore_signal(barrier, inc=1, device_id=(sp_id, tp_id), device_id_type=MESH)
    pl.semaphore_wait(barrier, len(partners))


def comm_call(body, out_shape, scratch, collective_id, operands, limit=60 * 1024 * 1024):
    return pl.pallas_call(
        body,
        out_shape=out_shape,
        in_specs=[pl.BlockSpec(memory_space=pltpu.VMEM)] * len(operands),
        out_specs=pl.BlockSpec(memory_space=pltpu.VMEM),
        scratch_shapes=scratch,
        compiler_params=pltpu.CompilerParams(
            collective_id=collective_id, has_side_effects=True, vmem_limit_bytes=limit
        ),
    )(*operands)


def gather_kernel(sp, x_ref, out_ref, up_send, up_recv, side_send, side_recv):
    rows = x_ref.shape[0]
    chips = sp // 2
    sp_id, tp_id = lax.axis_index("sp"), lax.axis_index("tp")
    level, core = sp_id // 2, lax.rem(sp_id, 2)
    sibling = 2 * level + 1 - core
    barrier = pltpu.get_barrier_semaphore()
    pl.semaphore_signal(barrier, inc=1, device_id=(sibling, tp_id), device_id_type=MESH)

    @pl.when(level > 0)
    def _():
        pl.semaphore_signal(barrier, inc=1, device_id=(sp_id - 2, tp_id), device_id_type=MESH)

    @pl.when(level < chips - 1)
    def _():
        pl.semaphore_signal(barrier, inc=1, device_id=(sp_id + 2, tp_id), device_id_type=MESH)

    pl.semaphore_wait(barrier, 1 + lax.min(level, 1) + lax.min(chips - 1 - level, 1))

    def rows_of(index):
        return pl.ds(pl.multiple_of(index * rows, rows), rows)

    def up_copy(step, src):
        place = out_ref.at[rows_of(sp_id - 2 * step), :]
        return remote(src if src is not None else place, place, up_send.at[step], up_recv.at[step], sp_id + 2, tp_id)

    def side_copy(step, src):
        place = out_ref.at[rows_of(sp_id - 2 * step), :]
        return remote(src if src is not None else place, place, side_send.at[step], side_recv.at[step], sibling, tp_id)

    def arrival(sem, index):
        place = out_ref.at[rows_of(index), :]
        return pltpu.make_async_copy(place, place, sem)

    @pl.when(level < chips - 1)
    def _():
        up_copy(0, x_ref).start()

    side_copy(0, x_ref).start()
    out_ref[rows_of(sp_id), :] = x_ref[...]
    for other in range(1, chips):

        @pl.when(level + other < chips)
        def _():
            first = pl.multiple_of((level + other) * 2 * rows, 2 * rows)
            out_ref[pl.ds(first, 2 * rows), :] = jnp.zeros((2 * rows, out_ref.shape[1]), out_ref.dtype)

    for step in range(1, chips):

        @pl.when(level - step >= 0)
        def _():
            arrival(up_recv.at[step - 1], sp_id - 2 * step).wait()

            @pl.when(level < chips - 1)
            def _():
                up_copy(step, None).start()

            side_copy(step, None).start()

    for step in range(chips):

        @pl.when(level - step >= 0)
        def _():
            arrival(side_recv.at[step], sibling - 2 * step).wait()
            side_copy(step, x_ref if step == 0 else None).wait_send()

            @pl.when(level < chips - 1)
            def _():
                up_copy(step, x_ref if step == 0 else None).wait_send()


def reduce_kernel(tp, part_ref, res_ref, out_ref, landed, send_sem, recv_sem):
    width = res_ref.shape[1]
    sp_id, tp_id = lax.axis_index("sp"), lax.axis_index("tp")
    peers = [lax.rem(tp_id + d, tp) for d in range(1, tp)]
    greet([(sp_id, p) for p in peers])

    def columns(index):
        return pl.ds(pl.multiple_of(index * width, width), width)

    copies = []
    for d in range(1, tp):
        copy = remote(
            part_ref.at[:, columns(peers[d - 1])],
            landed.at[d - 1],
            send_sem.at[d - 1],
            recv_sem.at[d - 1],
            sp_id,
            peers[d - 1],
        )
        copy.start()
        copies.append(copy)
    total = part_ref[:, columns(tp_id)].astype(jnp.float32)
    for d in range(1, tp):
        copies[d - 1].wait()
        total = total + landed[d - 1].astype(jnp.float32)
    out_ref[...] = (res_ref[...].astype(jnp.float32) + total).astype(jnp.bfloat16)


def near_first(count):
    order = [0]
    for d in range(1, count // 2 + 1):
        order.append(d)
        if count - d != d:
            order.append(count - d)
    return order


def square(tp_id):
    low = lax.rem(tp_id, 2)
    high = tp_id // 2
    return 2 * high + 1 - low, 2 * (1 - high) + low, 2 * (1 - high) + 1 - low


def dispatch_kernel(sp, tp, x_ref, out_ref, z_send, z_recv, t_send, t_recv, own_sem):
    cap = x_ref.shape[0] // sp
    width = x_ref.shape[1]
    half = cap // 2
    sp_id, tp_id = lax.axis_index("sp"), lax.axis_index("tp")
    greet(
        [(lax.rem(sp_id + d, sp), tp_id) for d in range(1, sp)]
        + [(sp_id, lax.rem(tp_id + d, tp)) for d in range(1, tp)]
    )

    def place(source, owner, part=None):
        first = source * cap
        if part is not None:
            first = first + part * half
        count = cap if part is None else half
        return out_ref.at[
            pl.ds(pl.multiple_of(first, half), count),
            pl.ds(pl.multiple_of(owner * width, width), width),
        ]

    def rows(source, part=None):
        first = source * cap
        if part is not None:
            first = first + part * half
        return x_ref.at[pl.ds(pl.multiple_of(first, half), cap if part is None else half), :]

    order = near_first(sp)
    z_copies = {}
    for d in order[1:]:
        target = lax.rem(sp_id + d, sp)
        z_copies[d] = remote(rows(target), place(sp_id, tp_id), z_send.at[d], z_recv.at[d], target, tp_id)
        z_copies[d].start()
    own = pltpu.make_async_copy(rows(sp_id), place(sp_id, tp_id), own_sem)
    own.start()

    def source_of(d):
        return lax.rem(sp_id + sp - d, sp)

    started = []
    if tp == 4:
        near, far, across = square(tp_id)

        def send(d, part, target, slot, owner):
            copy = remote(
                place(source_of(d), owner, part),
                place(source_of(d), owner, part),
                t_send.at[d, slot],
                t_recv.at[d, slot],
                sp_id,
                target,
            )
            copy.start()
            started.append(copy)
            return copy

        def relay(entry):
            d, to_near, to_far = entry
            to_near[0].wait_recv()
            fourth = send(d, 0, far, 4, near)
            to_far[1].wait_recv()
            fifth = send(d, 1, near, 5, far)
            return [to_near[1], to_far[0], fourth, fifth]

        waiting, rest = None, []
        for d in order:
            if d == 0:
                own.wait()
            else:
                z_copies[d].wait_recv()
            to_near = [send(d, 0, near, 0, tp_id), None]
            to_far = [None, send(d, 1, far, 3, tp_id)]
            to_near[1] = send(d, 1, near, 1, tp_id)
            to_far[0] = send(d, 0, far, 2, tp_id)
            if waiting is not None:
                rest += relay(waiting)
            waiting = (d, to_near, to_far)
        rest += relay(waiting)
        for copy in rest:
            copy.wait_recv()
    else:
        for d in order:
            if d == 0:
                own.wait()
            else:
                z_copies[d].wait_recv()
            for t in range(1, tp):
                copy = remote(
                    place(source_of(d), tp_id),
                    place(source_of(d), tp_id),
                    t_send.at[d, t],
                    t_recv.at[d, t],
                    sp_id,
                    lax.rem(tp_id + t, tp),
                )
                copy.start()
                started.append(copy)
        for copy in started:
            copy.wait_recv()
    for copy in started:
        copy.wait_send()
    for d in order[1:]:
        z_copies[d].wait_send()


def return_kernel(sp, tp, x_ref, out_ref, landed, turned, summed, t_send, t_recv, z_send, z_recv):
    cap = x_ref.shape[0] // sp
    width = out_ref.shape[1]
    half = cap // 2
    sp_id, tp_id = lax.axis_index("sp"), lax.axis_index("tp")
    greet(
        [(lax.rem(sp_id + d, sp), tp_id) for d in range(1, sp)]
        + [(sp_id, lax.rem(tp_id + d, tp)) for d in range(1, tp)]
    )

    def rows_at(target, part=None):
        first = target * cap
        if part is not None:
            first = first + part * half
        return pl.ds(pl.multiple_of(first, half), cap if part is None else half)

    def columns(owner):
        return pl.ds(pl.multiple_of(owner * width, width), width)

    order = near_first(sp)[::-1]
    started, z_copies = [], []

    def push(src, dst, d, slot, target):
        copy = remote(src, dst, t_send.at[d, slot], t_recv.at[d, slot], sp_id, target)
        copy.start()
        started.append(copy)
        return copy

    def deliver(d, target):
        if d == 0:
            return
        copy = remote(
            summed.at[d], out_ref.at[rows_at(sp_id), :], z_send.at[d], z_recv.at[d], target, tp_id
        )
        copy.start()
        z_copies.append(copy)

    def f32(value):
        return value.astype(jnp.float32)

    def place_sum(d, part, value):
        piece = pl.ds(part * half, half)
        summed[d, piece, :] = value.astype(jnp.bfloat16)
        if d == 0:
            out_ref[rows_at(sp_id, part), :] = value.astype(jnp.bfloat16)

    targets = {d: lax.rem(sp_id + d, sp) for d in order}
    if tp == 4:
        near, far, across = square(tp_id)
        first = {}

        def open_block(d):
            target = targets[d]
            first[d] = [
                push(x_ref.at[rows_at(target, 0), columns(across)], landed.at[d, 1], d, 1, near),
                push(x_ref.at[rows_at(target, 1), columns(across)], landed.at[d, 3], d, 3, far),
                push(x_ref.at[rows_at(target, 0), columns(near)], landed.at[d, 0], d, 0, near),
                push(x_ref.at[rows_at(target, 1), columns(far)], landed.at[d, 2], d, 2, far),
            ]

        second = {}

        def turn_block(d):
            target = targets[d]
            first[d][0].wait_recv()
            turned[d, 0] = (f32(x_ref[rows_at(target, 0), columns(far)]) + f32(landed[d, 1])).astype(jnp.bfloat16)
            first[d][1].wait_recv()
            turned[d, 1] = (f32(x_ref[rows_at(target, 1), columns(near)]) + f32(landed[d, 3])).astype(jnp.bfloat16)
            second[d] = [
                push(turned.at[d, 0], landed.at[d, 4], d, 4, far),
                push(turned.at[d, 1], landed.at[d, 5], d, 5, near),
            ]

        def close_block(d):
            target = targets[d]
            first[d][2].wait_recv()
            second[d][0].wait_recv()
            place_sum(d, 0, f32(x_ref[rows_at(target, 0), columns(tp_id)]) + f32(landed[d, 0]) + f32(landed[d, 4]))
            first[d][3].wait_recv()
            second[d][1].wait_recv()
            place_sum(d, 1, f32(x_ref[rows_at(target, 1), columns(tp_id)]) + f32(landed[d, 2]) + f32(landed[d, 5]))
            deliver(d, target)

        count = len(order)
        for i in range(count + 2):
            if i < count:
                open_block(order[i])
            if 0 <= i - 1 < count:
                turn_block(order[i - 1])
            if 0 <= i - 2 < count:
                close_block(order[i - 2])
    else:
        pushed = {}
        for d in order:
            pushed[d] = []
            for t in range(1, tp):
                owner = lax.rem(tp_id + t, tp)
                for part in range(2):
                    slot = 2 * (t - 1) + part
                    pushed[d].append(
                        push(x_ref.at[rows_at(targets[d], part), columns(owner)], landed.at[d, slot], d, slot, owner)
                    )
        for d in order:
            for part in range(2):
                value = f32(x_ref[rows_at(targets[d], part), columns(tp_id)])
                for t in range(1, tp):
                    pushed[d][2 * (t - 1) + part].wait_recv()
                    value = value + f32(landed[d, 2 * (t - 1) + part])
                place_sum(d, part, value)
            deliver(d, targets[d])
    for copy in started:
        copy.wait_send()
    for copy in z_copies:
        copy.wait()


def attention_kernel(
    groups,
    start_ref,
    joined_ref,
    nope_ref,
    rope_ref,
    key_major_ref,
    value_major_ref,
    key_minor_ref,
    value_minor_ref,
    out_major_ref,
    out_minor_ref,
    key_a,
    value_a,
    key_b,
    value_b,
):
    latent = key_major_ref.shape[0]
    tok_rows = nope_ref.shape[1]
    rows_f = joined_ref[:, :latent]
    tail = joined_ref[:, latent:]
    for kept, weight in (
        (key_a, key_major_ref),
        (value_a, value_major_ref),
        (key_b, key_minor_ref),
        (value_b, value_minor_ref),
    ):
        kept[...] = jnp.dot(rows_f, weight[...], preferred_element_type=jnp.float32).astype(jnp.bfloat16)
    total_keys = joined_ref.shape[0]
    shape = (tok_rows, total_keys)
    visible = lax.broadcasted_iota(jnp.int32, shape, 1) <= start_ref[0] + lax.broadcasted_iota(jnp.int32, shape, 0)
    contract = (((1,), (1,)), ((), ()))
    index = 0
    for kept_key, kept_value, out_ref, heads, pack, scale in (
        (key_a, value_a, out_major_ref, *groups[0]),
        (key_b, value_b, out_minor_ref, *groups[1]),
    ):
        tile = kept_key.shape[1] // (-(-heads // pack))
        lanes = lax.broadcasted_iota(jnp.int32, (tok_rows, tile), 1)
        for first in range(0, heads, pack):
            columns = pl.ds(first // pack * tile, tile)
            result = None
            for member in range(min(pack, heads - first)):
                scores = lax.dot_general(
                    nope_ref[index], kept_key[:, columns], contract, preferred_element_type=jnp.float32
                ) + lax.dot_general(rope_ref[index], tail, contract, preferred_element_type=jnp.float32)
                scores = jnp.where(visible, scores * scale, -jnp.inf)
                weights = jnp.exp(scores - jnp.max(scores, axis=1, keepdims=True))
                totals = jnp.sum(weights, axis=1, keepdims=True)
                summed = jnp.dot(
                    weights.astype(jnp.bfloat16), kept_value[:, columns], preferred_element_type=jnp.float32
                ) / totals
                result = summed if result is None else jnp.where(lanes < member * (tile // pack), result, summed)
                index += 1
            out_ref[:, columns] = result.astype(jnp.bfloat16)


def expert_kernel(x_ref, gain_ref, gate_ref, up_ref, down_ref, out_ref, normed, total):
    step = pl.program_id(0)

    @pl.when(step == 0)
    def _():
        rows_f = x_ref[...].astype(jnp.float32)
        power = jnp.mean(rows_f * rows_f, axis=1, keepdims=True)
        normed[...] = (rows_f * lax.rsqrt(power + norm_eps) * gain_ref[...]).astype(jnp.bfloat16)

    rows = normed[...]
    gate_pre = jnp.dot(rows, gate_ref[0], preferred_element_type=jnp.float32)
    up_pre = jnp.dot(rows, up_ref[0], preferred_element_type=jnp.float32)
    hidden = (gate_pre / (1.0 + jnp.exp(-gate_pre)) * up_pre).astype(jnp.bfloat16)
    part = jnp.dot(hidden, down_ref[0], preferred_element_type=jnp.float32)
    last = pl.num_programs(0) - 1

    @pl.when((step == 0) & (last > 0))
    def _():
        total[...] = part

    @pl.when((step > 0) & (step < last))
    def _():
        total[...] += part

    @pl.when((step == last) & (last > 0))
    def _():
        out_ref[...] = (total[...] + part).astype(jnp.bfloat16)

    @pl.when(last == 0)
    def _():
        out_ref[...] = part.astype(jnp.bfloat16)


def flip(index, offset):
    step = 1
    while step <= offset:
        if offset & step:
            index = index + step * (1 - 2 * lax.rem(index // step, 2))
        step *= 2
    return index


def rope_table(count, width):
    half_width = width // 2
    inverse_freq = (1.0 / theta_base ** (np.arange(half_width, dtype=np.float32) * (2.0 / width))).astype(np.float32)
    angles = np.arange(count, dtype=np.float32)[:, None] * inverse_freq[None, :]
    cosine, sine = np.cos(angles), np.sin(angles)
    return np.concatenate([cosine, cosine, -sine, sine], axis=1).astype(np.float32)


def plans(chips):
    last = chips - 1
    simple = {"streamed": [("open", 0), ("relay", 0)]}
    for k in range(last):
        simple[f"between {k}"] = [("open", k + 1)]
        simple[f"after {k}"] = [("relay", k + 1)] + ([("turn", k - 1)] if k else [])
    simple[f"after {last}"] = [("turn", last - 1)] if last else []
    simple[f"after {last}"] += [("turn", last)] + [("close", k) for k in range(chips)]
    if chips != 4:
        return [simple] * chips
    low = {
        "streamed": [("open", 0), ("relay", 0)],
        "between 0": [("open", 1)],
        "after 0": [("relay", 1), ("open", 2)],
        "between 1": [("relay", 2)],
        "after 1": [("turn", 0)],
        "between 2": [("open", 3)],
        "after 2": [("relay", 3), ("turn", 1), ("close", 0), ("turn", 2), ("close", 1)],
        "after 3": [("close", 2), ("turn", 3), ("close", 3)],
    }
    early = {
        "pushed": [("open", 0)],
    }
    ending = {
        "after 2": [("turn", 1), ("close", 0)],
        "after 3": [("turn", 2), ("close", 1), ("turn", 3), ("close", 2), ("close", 3)],
    }
    upper = {
        "streamed": [("relay", 0), ("open", 1), ("open", 2), ("relay", 1)],
        "between 0": [("relay", 2)],
        "between 1": [("open", 3)],
        "after 1": [("relay", 3), ("turn", 0)],
    }
    top = {
        "streamed": [("relay", 0), ("open", 3), ("open", 1), ("relay", 1), ("open", 2)],
        "between 0": [("relay", 2)],
        "after 0": [("relay", 3)],
        "after 1": [("turn", 0)],
    }
    return [low, low, early | upper | ending, early | top | ending]


def layer_kernel(
    sp,
    heads,
    q_major_ref,
    q_minor_ref,
    latent_ref,
    rope_ref,
    table_ref,
    key_major_ref,
    value_major_ref,
    key_minor_ref,
    value_minor_ref,
    out_major_ref,
    out_minor_ref,
    res_ref,
    ids_ref,
    mix_ref,
    gain_ref,
    gate_ref,
    up_ref,
    down_ref,
    out_ref,
    q_major,
    q_minor,
    rope_raw,
    table,
    weights,
    projection,
    residual,
    ids,
    mix,
    gain,
    gate,
    up,
    down,
    blocks,
    queries,
    kept,
    tops,
    scores,
    chances,
    fades,
    gathered_out,
    mixed,
    spread_part,
    spread_landed,
    spread_turned,
    stream,
    select,
    hot,
    mix_column,
    placed,
    rows_in,
    normed,
    hidden,
    part,
    landed,
    turned,
    summed,
    returned,
    load_sem,
    expert_sem,
    l_send,
    l_recv,
    q_send,
    q_recv,
    s_send,
    s_recv,
    o_send,
    o_recv,
    z_send,
    z_recv,
    t_send,
    t_recv,
    r_send,
    r_recv,
    y_send,
    y_recv,
):
    heads_major, heads_minor = heads
    tok_rows, latent = latent_ref.shape
    rope_width = rope_ref.shape[0]
    chips = sp // 2
    tp = 4
    quarter = tok_rows // tp
    pack = 128 // NOPE_MINOR
    sp_id, tp_id = lax.axis_index("sp"), lax.axis_index("tp")
    level, core = sp_id // 2, lax.rem(sp_id, 2)
    sibling = flip(sp_id, 1)
    near, far, across = square(tp_id)
    f32, bf16 = jnp.float32, jnp.bfloat16

    loads = []

    def load(src, dst):
        copy = pltpu.make_async_copy(src, dst, load_sem.at[len(loads)])
        copy.start()
        loads.append(copy)
        return copy

    own_rows = pl.ds(pl.multiple_of(sp_id * tok_rows, tok_rows), tok_rows)
    early = [
        load(latent_ref, blocks.at[0, 0, :, pl.ds(0, latent)]),
        load(rope_ref, rope_raw),
        load(table_ref.at[own_rows, :], table),
    ]
    asked = [load(q_major_ref, q_major), load(q_minor_ref, q_minor)]
    spans, first = [], 0
    for ref in (key_major_ref, key_minor_ref, value_major_ref, value_minor_ref):
        span = pl.ds(first, ref.shape[1])
        asked.append(load(ref, weights.at[:, span]))
        spans.append(span)
        first += ref.shape[1]
    split = out_major_ref.shape[0]
    routing = [load(ids_ref, ids), load(mix_ref, mix), load(gain_ref, gain)]
    late = [
        load(out_major_ref, projection.at[pl.ds(0, split), :]),
        load(out_minor_ref, projection.at[pl.ds(split, out_minor_ref.shape[0]), :]),
        load(res_ref, residual),
    ]

    barrier = pltpu.get_barrier_semaphore()
    for offset in range(1, sp):
        pl.semaphore_signal(barrier, inc=1, device_id=(flip(sp_id, offset), tp_id), device_id_type=MESH)
    for peer in (near, far, across):
        pl.semaphore_signal(barrier, inc=1, device_id=(sp_id, peer), device_id_type=MESH)

    lane = lax.broadcasted_iota(jnp.int32, (tok_rows, 128), 1)
    low = lane < rope_width

    def rotator(cosine, back, ahead):
        def rotate(x):
            return x * cosine + pltpu.roll(x, 128 - rope_width // 2, 1) * back + pltpu.roll(x, rope_width // 2, 1) * ahead

        return rotate

    for copy in early:
        copy.wait()
    trig = table[...]
    flipped = pltpu.roll(trig, 64, 1)
    half = rope_width // 2
    rotate_low = rotator(
        jnp.where(low, trig, 1.0),
        jnp.where(lane < half, flipped, 0.0),
        jnp.where((lane >= half) & low, flipped, 0.0),
    )
    rotate_high = rotator(
        jnp.where(low, 1.0, flipped),
        jnp.where(low | (lane >= 64 + half), 0.0, trig),
        jnp.where(lane >= 64 + half, trig, 0.0),
    )
    raw = rope_raw[...].astype(f32)
    raw = jnp.concatenate([raw, jnp.zeros((128 - rope_width, tok_rows), f32)], axis=0).T
    blocks[0, 0, :, latent:] = rotate_low(raw).astype(bf16)
    pl.semaphore_wait(barrier, sp - 1 + 3)

    own_quarter = pl.ds(pl.multiple_of(tp_id * quarter, quarter), quarter)

    def lift(d):
        return remote(
            blocks.at[0, 0, own_quarter, :],
            blocks.at[d, 0, own_quarter, :],
            l_send.at[d],
            l_recv.at[d],
            sp_id + 2 * d,
            tp_id,
        )

    def spread(d, slot):
        place = blocks.at[d, 0, own_quarter, :]
        return remote(place, place, q_send.at[d, slot], q_recv.at[d, slot], sp_id, (near, far, across)[slot])

    def share(d):
        return remote(blocks.at[d, 0], blocks.at[d, 1], s_send.at[d], s_recv.at[d], sibling, tp_id)

    for d in range(1, chips):

        @pl.when(level + d < chips)
        def _():
            lift(d).start()

    share(0).start()

    for copy in asked:
        copy.wait()
    expert_loads = []
    pieces = expert_sem.shape[1]
    for index, (src, dst) in enumerate(((gate_ref, gate), (up_ref, up), (down_ref, down))):
        count = dst.shape[0] // pieces
        for piece in range(pieces):
            span = pl.ds(piece * count, count)
            copy = pltpu.make_async_copy(src.at[0, span, :], dst.at[span, :], expert_sem.at[index, piece])
            copy.start()
            expert_loads.append(copy)
    def column(ref, index):
        return ref[:, index * 128 : index * 128 + 128].astype(f32)

    def only_low(x):
        return jnp.where(low, x, 0.0).astype(bf16)

    for pair in range(heads_major // 2):
        one, two = column(q_major, 3 * pair + 1), column(q_major, 3 * pair + 2)
        queries[2 * pair, :, :128] = q_major[:, pair * 384 : pair * 384 + 128]
        queries[2 * pair, :, 128:] = only_low(rotate_low(one))
        queries[2 * pair + 1, :, :128] = jnp.where(low, pltpu.roll(one, 64, 1), pltpu.roll(two, 64, 1)).astype(bf16)
        queries[2 * pair + 1, :, 128:] = only_low(pltpu.roll(rotate_high(two), 64, 1))
    for h in range(heads_minor):
        whole = rotate_high(column(q_minor, h))
        moved = pltpu.roll(whole, 64, 1)
        queries[heads_major + h, :, 128:] = only_low(moved)
        if h % pack == 0:
            queries[heads_major + h, :, :128] = only_low(whole)
        else:
            queries[heads_major + h, :, :128] = jnp.where(low, 0.0, moved).astype(bf16)

    keys = 2 * tok_rows
    log2e = 1.4426950408889634
    contract = (((1,), (1,)), ((), ()))

    def project(d):
        for q in range(2):
            rows = blocks[d, q, :, :latent]
            kept[pl.ds(q * tok_rows, tok_rows), :] = jnp.dot(rows, weights[...], preferred_element_type=f32).astype(
                bf16
            )

    everyone = range(heads_major + heads_minor)

    def tile_of(h):
        return h if h < heads_major else (h - heads_major) // pack

    def attend(d):
        tails = jnp.concatenate([blocks[d, 0, :, latent:], blocks[d, 1, :, latent:]], axis=0)
        for h in everyone:
            nope = NOPE_MAJOR if h < heads_major else NOPE_MINOR
            key_at = tile_of(h) * 128 + (0 if h < heads_major else spans[1].start)
            key = jnp.concatenate([kept[:, key_at : key_at + 128], tails], axis=1)
            scale = (nope + rope_width) ** (-0.5) * log2e
            value = lax.dot_general(queries[h], key, contract, preferred_element_type=f32) * scale
            if d == 0:
                spot = lax.broadcasted_iota(jnp.int32, (tok_rows, keys), 1)
                row = lax.broadcasted_iota(jnp.int32, (tok_rows, keys), 0)
                limit = jnp.where(spot < tok_rows, row, keys * core - 1)
                value = jnp.where(spot <= limit, value, -jnp.inf)
            scores[h] = value
        for h in everyone:
            value = scores[h]
            peak = jnp.max(value, axis=1, keepdims=True)
            if d > 0:
                before = tops[h][:, :1]
                peak = jnp.maximum(before, peak)
                fades[h] = jnp.broadcast_to(jnp.exp2(before - peak), (tok_rows, 128))
            chances[h] = jnp.exp2(value - peak).astype(bf16)
            tops[h] = jnp.broadcast_to(peak, (tok_rows, 128))
        ones = jnp.ones((keys, 128), bf16)
        for h in everyone:
            value_at = tile_of(h) * 128 + (spans[2].start if h < heads_major else spans[3].start)
            value = jnp.concatenate([kept[:, value_at : value_at + 128], ones], axis=1)
            summed = jnp.dot(chances[h], value, preferred_element_type=f32)
            if d == 0:
                gathered_out[h] = summed
            else:
                fade = fades[h]
                gathered_out[h, :, :128] = summed[:, :128] + gathered_out[h, :, :128] * fade
                gathered_out[h, :, 128:] = summed[:, 128:] + gathered_out[h, :, 128:] * fade

    slots = placed.shape[0]
    cap = slots // sp
    width = stream.shape[1]

    def prepare_routing():
        for copy in routing:
            copy.wait()
        lanes = lax.broadcasted_iota(jnp.int32, (sp, tok_rows), 0)
        matches = [(lanes == ids[j : j + 1, :]).astype(f32) for j in range(TOP)]
        order = (tok_rows, tok_rows)
        before = lax.broadcasted_iota(jnp.int32, order, 0) < lax.broadcasted_iota(jnp.int32, order, 1)
        named = functools.reduce(lambda a, b: a + b, matches)
        earlier = jnp.dot(named.astype(bf16), before.astype(bf16), preferred_element_type=f32)
        slot_rows = lax.broadcasted_iota(jnp.int32, (slots, tok_rows), 0)
        either = None
        for j in range(TOP):
            rank = jnp.sum(matches[j] * earlier, axis=0, keepdims=True).astype(jnp.int32)
            earlier = earlier + matches[j]
            chosen = jnp.where(slot_rows == ids[j : j + 1, :] * cap + rank, 1.0, 0.0)
            hot[j] = chosen.T.astype(bf16)
            mix_column[j] = jnp.broadcast_to(mix[j : j + 1, :], order).T
            either = chosen if either is None else either + chosen
        select[...] = either.astype(bf16)

    def columns(owner):
        return pl.ds(pl.multiple_of(owner * width, width), width)

    def arrival(place, sem):
        return pltpu.make_async_copy(place, place, sem)

    own_columns = columns(tp_id)

    def block(index):
        return pl.ds(pl.multiple_of(index * cap, cap), cap)

    def ends(target_level, q):
        return 2 * target_level + flip(core, q)

    def handoff(k, q, target_level):
        return remote(
            placed.at[block(ends(target_level, q)), :],
            rows_in.at[level, pl.ds(q * cap, cap), own_columns],
            z_send.at[k, q],
            z_recv.at[level, q],
            ends(target_level, q),
            tp_id,
        )

    parts = {0: (0, 0, 0), 1: (1, 0, 0), 2: (0, 0, 1), 3: (1, 0, 1), 4: (0, 1, 1), 5: (1, 1, 0)}

    def pass_on(k, slot):
        q, borrowed, to_far = parts[slot]
        owner = tp_id
        if borrowed:
            owner = near if slot == 4 else far
        place = rows_in.at[k, pl.ds(q * cap, cap), columns(owner)]
        target = far if to_far else near
        return remote(place, place, t_send.at[k, slot], t_recv.at[k, slot], sp_id, target)

    def open_chunk(k):
        @pl.when(level != k)
        def _():
            arrival(rows_in.at[k, pl.ds(0, cap), own_columns], z_recv.at[k, 0]).wait()

        pass_on(k, 0).start()
        pass_on(k, 2).start()
        arrival(rows_in.at[k, pl.ds(cap, cap), own_columns], z_recv.at[k, 1]).wait()
        pass_on(k, 3).start()
        pass_on(k, 1).start()

    def relay(k):
        pass_on(k, 0).wait_recv()
        pass_on(k, 4).start()
        pass_on(k, 3).wait_recv()
        pass_on(k, 5).start()

    def push(k, slot):
        src, target = {
            0: (part.at[k, pl.ds(0, cap), columns(near)], near),
            1: (part.at[k, pl.ds(0, cap), columns(across)], near),
            2: (part.at[k, pl.ds(cap, cap), columns(far)], far),
            3: (part.at[k, pl.ds(cap, cap), columns(across)], far),
            4: (turned.at[k, 0], far),
            5: (turned.at[k, 1], near),
        }[slot]
        return remote(src, landed.at[k, slot], r_send.at[k, slot], r_recv.at[k, slot], sp_id, target)

    def wide(value):
        return value.astype(f32)

    def turn(k):
        push(k, 1).wait_recv()
        turned[k, 0] = (wide(part[k, :cap, columns(far)]) + wide(landed[k, 1])).astype(bf16)
        push(k, 4).start()
        push(k, 3).wait_recv()
        turned[k, 1] = (wide(part[k, cap:, columns(near)]) + wide(landed[k, 3])).astype(bf16)
        push(k, 5).start()

    def back(k, q):
        return remote(
            summed.at[k, q],
            returned.at[block(sp_id), :],
            y_send.at[k, q],
            y_recv.at[level, q],
            ends(k, q),
            tp_id,
        )

    def close(k):
        for q in range(2):
            push(k, 2 * q).wait_recv()
            push(k, 4 + q).wait_recv()
            value = wide(part[k, q * cap : q * cap + cap, own_columns])
            value = (value + wide(landed[k, 2 * q]) + wide(landed[k, 4 + q])).astype(bf16)
            summed[k, q] = value
            if q == 1:
                back(k, q).start()
                continue

            @pl.when(level == k)
            def _():
                returned[block(sp_id), :] = summed[k, 0]

            @pl.when(level != k)
            def _():
                back(k, 0).start()

    actions = {"open": open_chunk, "relay": relay, "turn": turn, "close": close}

    def run(point):
        for here, plan in enumerate(plans(chips)):
            events = plan.get(point, ())
            if events:

                @pl.when(level == here)
                def _():
                    for action, k in events:
                        actions[action](k)

    def forward(d):
        @pl.when(level >= d)
        def _():
            arrival(blocks.at[d, 0, own_quarter, :], l_recv.at[d]).wait()
            for slot in range(3):
                spread(d, slot).start()

    for d in range(1, chips // 2):
        forward(d)
    share(0).wait_recv()
    project(0)
    for d in range(chips // 2, chips - 1):
        forward(d)
    attend(0)
    forward(chips - 1)
    prepare_routing()
    for d in range(1, chips):

        @pl.when(level >= d)
        def _():
            for slot in range(3):
                spread(d, slot).wait_recv()
            share(d).start()

    run("gathered")
    for d in range(1, chips):
        if d == chips - 1:
            run("last")

        @pl.when(level >= d)
        def _():
            share(d).wait_recv()
            project(d)
            attend(d)

    def share_of(h):
        return gathered_out[h, :, :128] / gathered_out[h, :, 128:]

    for h in range(heads_major):
        mixed[:, h * 128 : h * 128 + 128] = share_of(h).astype(bf16)
    for tile in range(-(-heads_minor // pack)):
        result = None
        for member in range(min(pack, heads_minor - tile * pack)):
            h = heads_major + tile * pack + member
            value = share_of(h)
            result = value if result is None else jnp.where(lane < member * NOPE_MINOR, result, value)
        first = (heads_major + tile) * 128
        mixed[:, first : first + 128] = result.astype(bf16)

    for copy in late:
        copy.wait()

    mid = tok_rows // 2
    mids = (pl.ds(0, mid), pl.ds(mid, mid))
    rows = mixed[...]
    spread_started = []

    def fill_out(owner):
        spread_part[:, columns(owner)] = jnp.dot(rows, projection[:, columns(owner)], preferred_element_type=f32).astype(bf16)

    def push_out(src, slot, target):
        copy = remote(src, spread_landed.at[slot], o_send.at[slot], o_recv.at[slot], sp_id, target)
        copy.start()
        spread_started.append(copy)
        return copy

    fill_out(across)
    second = push_out(spread_part.at[mids[0], columns(across)], 1, near)
    fourth = push_out(spread_part.at[mids[1], columns(across)], 3, far)
    fill_out(near)
    first = push_out(spread_part.at[mids[0], columns(near)], 0, near)
    fill_out(far)
    third = push_out(spread_part.at[mids[1], columns(far)], 2, far)
    fill_out(tp_id)
    second.wait_recv()
    spread_turned[0] = (spread_part[mids[0], columns(far)].astype(f32) + spread_landed[1].astype(f32)).astype(bf16)
    fifth = push_out(spread_turned.at[0], 4, far)
    fourth.wait_recv()
    spread_turned[1] = (spread_part[mids[1], columns(near)].astype(f32) + spread_landed[3].astype(f32)).astype(bf16)
    sixth = push_out(spread_turned.at[1], 5, near)
    run("pushed")
    for q, plain, bent in ((0, first, fifth), (1, third, sixth)):
        plain.wait_recv()
        value = spread_part[mids[q], columns(tp_id)].astype(f32) + residual[mids[q], :].astype(f32)
        value = value + spread_landed[2 * q].astype(f32)
        bent.wait_recv()
        stream[mids[q], :] = (value + spread_landed[4 + q].astype(f32)).astype(bf16)

    units = gate.shape[1]
    placed[...] = jnp.dot(select[...], stream[...], preferred_element_type=f32).astype(bf16)

    handoff(0, 1, level).start()
    for k in range(chips - 1, 0, -1):
        for q in range(2):
            handoff(k, q, flip(level, k)).start()
    rows_in[level, 0:cap, own_columns] = placed[block(sp_id), :]

    def ready(k):
        for slot in (1, 2, 4, 5):
            pass_on(k, slot).wait_recv()
        rows = rows_in[k].astype(f32)
        power = jnp.mean(rows * rows, axis=1, keepdims=True)
        normed[...] = (rows * lax.rsqrt(power + norm_eps) * gain[...]).astype(bf16)

    def expand():
        tile = 256
        rows = normed[...]
        for first in range(0, units, tile):
            span = slice(first, first + tile)
            gate_pre = jnp.dot(rows, gate[:, span], preferred_element_type=f32)
            up_pre = jnp.dot(rows, up[:, span], preferred_element_type=f32)
            hidden[:, span] = (gate_pre / (1.0 + jnp.exp(-gate_pre)) * up_pre).astype(bf16)

    def contract(k):
        rows = hidden[...]

        def fill(owner):
            part[k, :, columns(owner)] = jnp.dot(
                rows, down[:, columns(owner)], preferred_element_type=f32
            ).astype(bf16)

        fill(across)
        push(k, 1).start()
        push(k, 3).start()
        fill(near)
        push(k, 0).start()
        fill(far)
        push(k, 2).start()
        fill(tp_id)

    run("streamed")
    for copy in expert_loads:
        copy.wait()
    for k in range(chips):
        ready(k)
        expand()
        run(f"between {k}")
        contract(k)
        run(f"after {k}")

    for k in range(chips):
        for q in range(2):
            if q == 1:
                arrival(returned.at[block(ends(k, q)), :], y_recv.at[k, q]).wait()
                continue

            @pl.when(level != k)
            def _():
                arrival(returned.at[block(ends(k, q)), :], y_recv.at[k, q]).wait()

    total = stream[...].astype(f32)
    for j in range(TOP):
        total = total + jnp.dot(hot[j], returned[...], preferred_element_type=f32) * mix_column[j][:, :1]
    out_ref[...] = total.astype(bf16)
    for k in range(chips):
        for slot in range(6):
            pass_on(k, slot).wait_send()
            push(k, slot).wait_send()
        back(k, 1).wait_send()

        @pl.when(level != k)
        def _():
            back(k, 0).wait_send()

        for q in range(2):
            if k > 0 or q > 0:
                handoff(k, q, flip(level, k)).wait_send()
    for copy in spread_started:
        copy.wait_send()
    share(0).wait_send()
    for d in range(1, chips):

        @pl.when(level + d < chips)
        def _():
            lift(d).wait_send()

        @pl.when(level >= d)
        def _():
            share(d).wait_send()
            for slot in range(3):
                spread(d, slot).wait_send()


def fused_layer(
    sp,
    tp,
    query_major,
    query_minor,
    latent_rows,
    rope_keys,
    key_up_major,
    value_up_major,
    key_up_minor,
    value_up_minor,
    out_major,
    out_minor,
    residual,
    norm_gain,
    expert_ids,
    expert_weights,
    gate_proj,
    up_proj,
    down_proj,
):
    tok_rows, latent = latent_rows.shape
    rope_width = rope_keys.shape[1]
    width = residual.shape[1]
    features = tp * width
    units = gate_proj.shape[2]
    chips = sp // 2
    cap = 2 * tok_rows * TOP // sp
    slots = sp * cap
    heads = (key_up_major.shape[1] // NOPE_MAJOR, key_up_minor.shape[1] // NOPE_MINOR)
    count = heads[0] + heads[1]
    joined = latent + rope_width + -(latent + rope_width) % 128
    kept = key_up_major.shape[1] + key_up_minor.shape[1] + value_up_major.shape[1] + value_up_minor.shape[1]
    mixed = value_up_major.shape[1] + value_up_minor.shape[1]
    dma = pltpu.SemaphoreType.DMA
    bf16, f32 = jnp.bfloat16, jnp.float32
    table = jnp.asarray(rope_table(sp * tok_rows, rope_width))
    operands = (
        query_major,
        query_minor,
        latent_rows,
        rope_keys.T,
        table,
        key_up_major,
        value_up_major,
        key_up_minor,
        value_up_minor,
        out_major,
        out_minor,
        residual,
        expert_ids.T,
        expert_weights.T,
        norm_gain.reshape(1, -1),
        gate_proj,
        up_proj,
        down_proj,
    )
    vmem = pltpu.VMEM
    return pl.pallas_call(
        functools.partial(layer_kernel, sp, heads),
        out_shape=jax.ShapeDtypeStruct((tok_rows, width), bf16),
        in_specs=[pl.BlockSpec(memory_space=pl.ANY)] * len(operands),
        out_specs=pl.BlockSpec(memory_space=pltpu.VMEM),
        scratch_shapes=[
            vmem(query_major.shape, bf16),
            vmem(query_minor.shape, bf16),
            vmem((rope_width, tok_rows), bf16),
            vmem((tok_rows, 2 * rope_width), f32),
            vmem((latent, kept), bf16),
            vmem((mixed, features), bf16),
            vmem(residual.shape, bf16),
            vmem((TOP, tok_rows), jnp.int32),
            vmem((TOP, tok_rows), f32),
            vmem((1, features), f32),
            vmem((features, units), bf16),
            vmem((features, units), bf16),
            vmem((units, features), bf16),
            vmem((chips, 2, tok_rows, joined), bf16),
            vmem((count, tok_rows, 256), bf16),
            vmem((2 * tok_rows, kept), bf16),
            vmem((count, tok_rows, 128), f32),
            vmem((count, tok_rows, 2 * tok_rows), f32),
            vmem((count, tok_rows, 2 * tok_rows), bf16),
            vmem((count, tok_rows, 128), f32),
            vmem((count, tok_rows, 256), f32),
            vmem((tok_rows, mixed), bf16),
            vmem((tok_rows, features), bf16),
            vmem((6, tok_rows // 2, width), bf16),
            vmem((2, tok_rows // 2, width), bf16),
            vmem((tok_rows, width), bf16),
            vmem((slots, tok_rows), bf16),
            vmem((TOP, tok_rows, slots), bf16),
            vmem((TOP, tok_rows, tok_rows), f32),
            vmem((slots, width), bf16),
            vmem((chips, 2 * cap, features), bf16),
            vmem((2 * cap, features), bf16),
            vmem((2 * cap, units), bf16),
            vmem((chips, 2 * cap, features), bf16),
            vmem((chips, 6, cap, width), bf16),
            vmem((chips, 2, cap, width), bf16),
            vmem((chips, 2, cap, width), bf16),
            vmem((slots, width), bf16),
            dma((len(operands),)),
            dma((3, 4)),
            dma((chips,)),
            dma((chips,)),
            dma((chips, 3)),
            dma((chips, 3)),
            dma((chips,)),
            dma((chips,)),
            dma((6,)),
            dma((6,)),
            dma((chips, 2)),
            dma((chips, 2)),
            dma((chips, 6)),
            dma((chips, 6)),
            dma((chips, 6)),
            dma((chips, 6)),
            dma((chips, 2)),
            dma((chips, 2)),
        ],
        compiler_params=pltpu.CompilerParams(
            collective_id=4, has_side_effects=True, vmem_limit_bytes=60 * 1024 * 1024
        ),
    )(*operands)


def run_experts(rows, gain, gate_proj, up_proj, down_proj):
    slots, features = rows.shape
    units = gate_proj.shape[2]
    tile = min(256, units)
    return pl.pallas_call(
        expert_kernel,
        grid=(units // tile,),
        out_shape=jax.ShapeDtypeStruct((slots, features), jnp.bfloat16),
        in_specs=[
            pl.BlockSpec((slots, features), lambda i: (0, 0)),
            pl.BlockSpec((1, features), lambda i: (0, 0)),
            pl.BlockSpec((1, features, tile), lambda i: (0, 0, i)),
            pl.BlockSpec((1, features, tile), lambda i: (0, 0, i)),
            pl.BlockSpec((1, tile, features), lambda i: (0, i, 0)),
        ],
        out_specs=pl.BlockSpec((slots, features), lambda i: (0, 0)),
        scratch_shapes=[
            pltpu.VMEM((slots, features), jnp.bfloat16),
            pltpu.VMEM((slots, features), jnp.float32),
        ],
        compiler_params=pltpu.CompilerParams(vmem_limit_bytes=60 * 1024 * 1024),
    )(rows, gain.reshape(1, -1), gate_proj, up_proj, down_proj)


def pad_columns(array, multiple):
    return jnp.pad(array, ((0, 0), (0, -array.shape[1] % multiple)))


def per_device(
    sp,
    tp,
    query_major,
    query_minor,
    latent_rows,
    rope_keys,
    key_up_major,
    value_up_major,
    key_up_minor,
    value_up_minor,
    out_major,
    out_minor,
    residual,
    norm_gain,
    expert_ids,
    expert_weights,
    gate_proj,
    up_proj,
    down_proj,
):
    tok_rows = query_major.shape[0]
    fast = tp == 4 and sp & (sp - 1) == 0
    fast = fast and tok_rows % 64 == 0 and (2 * tok_rows * TOP // sp) % 16 == 0
    fast = fast and key_up_major.shape[1] % 128 == 0 and key_up_minor.shape[1] % 128 == 0
    if fast:
        return fused_layer(
            sp,
            tp,
            query_major,
            query_minor,
            latent_rows,
            rope_keys,
            key_up_major,
            value_up_major,
            key_up_minor,
            value_up_minor,
            out_major,
            out_minor,
            residual,
            norm_gain,
            expert_ids,
            expert_weights,
            gate_proj,
            up_proj,
            down_proj,
        )
    row_start = lax.axis_index("sp") * tok_rows
    positions = row_start + jnp.arange(tok_rows, dtype=jnp.int32)
    rope_width = rope_keys.shape[1]
    latent = latent_rows.shape[1]
    rope_rot = rotary(rope_keys, positions).astype(jnp.bfloat16)
    heads_major = key_up_major.shape[1] // NOPE_MAJOR
    heads_minor = key_up_minor.shape[1] // NOPE_MINOR
    shaped_major = query_major.reshape(tok_rows, heads_major, NOPE_MAJOR + rope_width)
    shaped_minor = query_minor.reshape(tok_rows, heads_minor, NOPE_MINOR + rope_width)
    nope_major = shaped_major[:, :, :NOPE_MAJOR]
    nope_minor = shaped_minor[:, :, :NOPE_MINOR]
    turned_major = rotary(shaped_major[:, :, NOPE_MAJOR:], positions).astype(jnp.bfloat16)
    turned_minor = rotary(shaped_minor[:, :, NOPE_MINOR:], positions).astype(jnp.bfloat16)
    scale_major = (NOPE_MAJOR + rope_width) ** (-0.5)
    scale_minor = (NOPE_MINOR + rope_width) ** (-0.5)

    joined = jnp.concatenate(
        [latent_rows, rope_rot, jnp.zeros((tok_rows, -(latent + rope_width) % 128), jnp.bfloat16)], axis=1
    )
    dma = pltpu.SemaphoreType.DMA
    chips = sp // 2
    gathered = comm_call(
        functools.partial(gather_kernel, sp),
        jax.ShapeDtypeStruct((sp * tok_rows, joined.shape[1]), jnp.bfloat16),
        [dma((chips,)), dma((chips,)), dma((chips,)), dma((chips,))],
        0,
        (joined,),
    )
    tail_width = joined.shape[1] - latent

    def by_head(array, width):
        return jnp.pad(array.transpose(1, 0, 2), ((0, 0), (0, 0), (0, width - array.shape[2])))

    pack = 128 // NOPE_MINOR
    spread = nope_minor.transpose(1, 0, 2)
    member = (jnp.arange(heads_minor, dtype=jnp.int32) % pack)[:, None, None]
    spread = jnp.concatenate(
        [jnp.where(member == m, spread, jnp.zeros_like(spread)) for m in range(pack)], axis=2
    )
    nope_all = jnp.concatenate([by_head(nope_major, 128), spread], axis=0)
    rope_all = jnp.concatenate([by_head(turned_major, tail_width), by_head(turned_minor, tail_width)], axis=0)
    minor_weights = [pad_columns(key_up_minor, 128), pad_columns(value_up_minor, 128)]
    minor_width = minor_weights[0].shape[1]
    keys = sp * tok_rows
    vmem = pl.BlockSpec(memory_space=pltpu.VMEM)
    attn_major, attn_minor = pl.pallas_call(
        functools.partial(attention_kernel, ((heads_major, 1, scale_major), (heads_minor, pack, scale_minor))),
        out_shape=(
            jax.ShapeDtypeStruct((tok_rows, value_up_major.shape[1]), jnp.bfloat16),
            jax.ShapeDtypeStruct((tok_rows, minor_width), jnp.bfloat16),
        ),
        in_specs=[pl.BlockSpec(memory_space=pltpu.SMEM)] + [vmem] * 7,
        out_specs=(vmem, vmem),
        scratch_shapes=[
            pltpu.VMEM((keys, key_up_major.shape[1]), jnp.bfloat16),
            pltpu.VMEM((keys, value_up_major.shape[1]), jnp.bfloat16),
            pltpu.VMEM((keys, minor_width), jnp.bfloat16),
            pltpu.VMEM((keys, minor_width), jnp.bfloat16),
        ],
        compiler_params=pltpu.CompilerParams(vmem_limit_bytes=60 * 1024 * 1024),
    )(
        row_start.reshape(1).astype(jnp.int32),
        gathered,
        nope_all,
        rope_all,
        key_up_major,
        value_up_major,
        *minor_weights,
    )
    attn_minor = attn_minor[:, : value_up_minor.shape[1]]
    partial_value = jnp.dot(attn_major, out_major, preferred_element_type=jnp.float32)
    partial_value = partial_value + jnp.dot(
        attn_minor, out_minor, preferred_element_type=jnp.float32
    )
    width = residual.shape[1]
    stream_mid = comm_call(
        functools.partial(reduce_kernel, tp),
        jax.ShapeDtypeStruct((tok_rows, width), jnp.bfloat16),
        [pltpu.VMEM((tp - 1, tok_rows, width), jnp.bfloat16), dma((tp - 1,)), dma((tp - 1,))],
        1,
        (partial_value.astype(jnp.bfloat16), residual),
    )
    experts = sp
    capacity = 2 * tok_rows * TOP // experts
    slots = experts * capacity
    slot_list = slot_ids(expert_ids, experts, capacity)
    slot_numbers = jnp.arange(slots, dtype=jnp.int32)
    by_slot = slot_list.T
    select = (slot_numbers[:, None] == by_slot[0][None, :]).astype(jnp.bfloat16)
    for j in range(1, TOP):
        select = select + (slot_numbers[:, None] == by_slot[j][None, :]).astype(jnp.bfloat16)
    placed = jnp.dot(select, stream_mid, preferred_element_type=jnp.float32).astype(jnp.bfloat16)
    slots_t = 6 if tp == 4 else tp
    arrived = comm_call(
        functools.partial(dispatch_kernel, sp, tp),
        jax.ShapeDtypeStruct((slots, tp * width), jnp.bfloat16),
        [dma((sp,)), dma((sp,)), dma((sp, slots_t)), dma((sp, slots_t)), dma],
        2,
        (placed,),
    )
    down_part = run_experts(arrived, norm_gain, gate_proj, up_proj, down_proj)
    pieces = 6 if tp == 4 else 2 * (tp - 1)
    half = capacity // 2
    flat_out = comm_call(
        functools.partial(return_kernel, sp, tp),
        jax.ShapeDtypeStruct((slots, width), jnp.bfloat16),
        [
            pltpu.VMEM((sp, pieces, half, width), jnp.bfloat16),
            pltpu.VMEM((sp, 2, half, width), jnp.bfloat16),
            pltpu.VMEM((sp, capacity, width), jnp.bfloat16),
            dma((sp, pieces)),
            dma((sp, pieces)),
            dma((sp,)),
            dma((sp,)),
        ],
        3,
        (down_part,),
    )
    mixed = stream_mid.astype(jnp.float32)
    for j in range(TOP):
        hot = (slot_list[:, j : j + 1] == slot_numbers[None, :]).astype(jnp.bfloat16)
        mixed = mixed + jnp.dot(hot, flat_out, preferred_element_type=jnp.float32) * expert_weights[:, j : j + 1]
    return mixed.astype(jnp.bfloat16)


def solution(mesh):
    in_specs = (
        P("sp", "tp"),
        P("sp", "tp"),
        P("sp", None),
        P("sp", None),
        P(None, "tp"),
        P(None, "tp"),
        P(None, "tp"),
        P(None, "tp"),
        P("tp", None),
        P("tp", None),
        P("sp", "tp"),
        P(),
        P("sp", None),
        P("sp", None),
        P("sp", None, "tp"),
        P("sp", None, "tp"),
        P("sp", "tp", None),
    )
    out_specs = P("sp", "tp")
    return jax.shard_map(
        functools.partial(per_device, mesh.shape["sp"], mesh.shape["tp"]),
        mesh=mesh,
        in_specs=in_specs,
        out_specs=out_specs,
        check_vma=False,
    )
```

```python
import functools

import jax
import jax.numpy as jnp
import numpy as np
from jax import lax
from jax.experimental import pallas as pl
from jax.experimental.pallas import tpu as pltpu
from jax.sharding import PartitionSpec as P

NOPE_MAJOR = 128
NOPE_MINOR = 64
TOP = 2
MESH = pl.DeviceIdType.MESH

theta_base = 10000.0
norm_eps = 1e-06


def rotary(values, positions):
    half_width = values.shape[-1] // 2
    inverse_freq = 1.0 / theta_base ** (
        jnp.arange(half_width, dtype=jnp.float32) * (2.0 / values.shape[-1])
    )
    angles = positions.astype(jnp.float32)[:, None] * inverse_freq[None, :]
    view_shape = (angles.shape[0],) + (1,) * (values.ndim - 2) + (half_width,)
    cosine = jnp.cos(angles).reshape(view_shape)
    sine_table = jnp.sin(angles).reshape(view_shape)
    lower_half = values[..., :half_width].astype(jnp.float32)
    upper_half = values[..., half_width:].astype(jnp.float32)
    return jnp.concatenate(
        [
            lower_half * cosine - upper_half * sine_table,
            upper_half * cosine + lower_half * sine_table,
        ],
        axis=-1,
    )


def slot_ids(route_block, experts, capacity):
    pairs = route_block.reshape(-1)
    matches = pairs[:, None] == jnp.arange(experts, dtype=jnp.int32)[None, :]
    order = jnp.arange(pairs.shape[0], dtype=jnp.int32)
    earlier = (order[:, None] > order[None, :]).astype(jnp.bfloat16)
    ranks = jnp.dot(earlier, matches.astype(jnp.bfloat16), preferred_element_type=jnp.float32)
    rank = jnp.sum(jnp.where(matches, ranks, 0.0), axis=1).astype(jnp.int32)
    return (pairs * capacity + rank).reshape(route_block.shape)


def remote(src, dst, send_sem, recv_sem, sp_id, tp_id):
    return pltpu.make_async_remote_copy(
        src_ref=src,
        dst_ref=dst,
        send_sem=send_sem,
        recv_sem=recv_sem,
        device_id=(sp_id, tp_id),
        device_id_type=MESH,
    )


def greet(partners):
    barrier = pltpu.get_barrier_semaphore()
    for sp_id, tp_id in partners:
        pl.semaphore_signal(barrier, inc=1, device_id=(sp_id, tp_id), device_id_type=MESH)
    pl.semaphore_wait(barrier, len(partners))


def comm_call(body, out_shape, scratch, collective_id, operands, limit=60 * 1024 * 1024):
    return pl.pallas_call(
        body,
        out_shape=out_shape,
        in_specs=[pl.BlockSpec(memory_space=pltpu.VMEM)] * len(operands),
        out_specs=pl.BlockSpec(memory_space=pltpu.VMEM),
        scratch_shapes=scratch,
        compiler_params=pltpu.CompilerParams(
            collective_id=collective_id, has_side_effects=True, vmem_limit_bytes=limit
        ),
    )(*operands)


def gather_kernel(sp, x_ref, out_ref, up_send, up_recv, side_send, side_recv):
    rows = x_ref.shape[0]
    chips = sp // 2
    sp_id, tp_id = lax.axis_index("sp"), lax.axis_index("tp")
    level, core = sp_id // 2, lax.rem(sp_id, 2)
    sibling = 2 * level + 1 - core
    barrier = pltpu.get_barrier_semaphore()
    pl.semaphore_signal(barrier, inc=1, device_id=(sibling, tp_id), device_id_type=MESH)

    @pl.when(level > 0)
    def _():
        pl.semaphore_signal(barrier, inc=1, device_id=(sp_id - 2, tp_id), device_id_type=MESH)

    @pl.when(level < chips - 1)
    def _():
        pl.semaphore_signal(barrier, inc=1, device_id=(sp_id + 2, tp_id), device_id_type=MESH)

    pl.semaphore_wait(barrier, 1 + lax.min(level, 1) + lax.min(chips - 1 - level, 1))

    def rows_of(index):
        return pl.ds(pl.multiple_of(index * rows, rows), rows)

    def up_copy(step, src):
        place = out_ref.at[rows_of(sp_id - 2 * step), :]
        return remote(src if src is not None else place, place, up_send.at[step], up_recv.at[step], sp_id + 2, tp_id)

    def side_copy(step, src):
        place = out_ref.at[rows_of(sp_id - 2 * step), :]
        return remote(src if src is not None else place, place, side_send.at[step], side_recv.at[step], sibling, tp_id)

    def arrival(sem, index):
        place = out_ref.at[rows_of(index), :]
        return pltpu.make_async_copy(place, place, sem)

    @pl.when(level < chips - 1)
    def _():
        up_copy(0, x_ref).start()

    side_copy(0, x_ref).start()
    out_ref[rows_of(sp_id), :] = x_ref[...]
    for other in range(1, chips):

        @pl.when(level + other < chips)
        def _():
            first = pl.multiple_of((level + other) * 2 * rows, 2 * rows)
            out_ref[pl.ds(first, 2 * rows), :] = jnp.zeros((2 * rows, out_ref.shape[1]), out_ref.dtype)

    for step in range(1, chips):

        @pl.when(level - step >= 0)
        def _():
            arrival(up_recv.at[step - 1], sp_id - 2 * step).wait()

            @pl.when(level < chips - 1)
            def _():
                up_copy(step, None).start()

            side_copy(step, None).start()

    for step in range(chips):

        @pl.when(level - step >= 0)
        def _():
            arrival(side_recv.at[step], sibling - 2 * step).wait()
            side_copy(step, x_ref if step == 0 else None).wait_send()

            @pl.when(level < chips - 1)
            def _():
                up_copy(step, x_ref if step == 0 else None).wait_send()


def reduce_kernel(tp, part_ref, res_ref, out_ref, landed, send_sem, recv_sem):
    width = res_ref.shape[1]
    sp_id, tp_id = lax.axis_index("sp"), lax.axis_index("tp")
    peers = [lax.rem(tp_id + d, tp) for d in range(1, tp)]
    greet([(sp_id, p) for p in peers])

    def columns(index):
        return pl.ds(pl.multiple_of(index * width, width), width)

    copies = []
    for d in range(1, tp):
        copy = remote(
            part_ref.at[:, columns(peers[d - 1])],
            landed.at[d - 1],
            send_sem.at[d - 1],
            recv_sem.at[d - 1],
            sp_id,
            peers[d - 1],
        )
        copy.start()
        copies.append(copy)
    total = part_ref[:, columns(tp_id)].astype(jnp.float32)
    for d in range(1, tp):
        copies[d - 1].wait()
        total = total + landed[d - 1].astype(jnp.float32)
    out_ref[...] = (res_ref[...].astype(jnp.float32) + total).astype(jnp.bfloat16)


def near_first(count):
    order = [0]
    for d in range(1, count // 2 + 1):
        order.append(d)
        if count - d != d:
            order.append(count - d)
    return order


def square(tp_id):
    low = lax.rem(tp_id, 2)
    high = tp_id // 2
    return 2 * high + 1 - low, 2 * (1 - high) + low, 2 * (1 - high) + 1 - low


def dispatch_kernel(sp, tp, x_ref, out_ref, z_send, z_recv, t_send, t_recv, own_sem):
    cap = x_ref.shape[0] // sp
    width = x_ref.shape[1]
    half = cap // 2
    sp_id, tp_id = lax.axis_index("sp"), lax.axis_index("tp")
    greet(
        [(lax.rem(sp_id + d, sp), tp_id) for d in range(1, sp)]
        + [(sp_id, lax.rem(tp_id + d, tp)) for d in range(1, tp)]
    )

    def place(source, owner, part=None):
        first = source * cap
        if part is not None:
            first = first + part * half
        count = cap if part is None else half
        return out_ref.at[
            pl.ds(pl.multiple_of(first, half), count),
            pl.ds(pl.multiple_of(owner * width, width), width),
        ]

    def rows(source, part=None):
        first = source * cap
        if part is not None:
            first = first + part * half
        return x_ref.at[pl.ds(pl.multiple_of(first, half), cap if part is None else half), :]

    order = near_first(sp)
    z_copies = {}
    for d in order[1:]:
        target = lax.rem(sp_id + d, sp)
        z_copies[d] = remote(rows(target), place(sp_id, tp_id), z_send.at[d], z_recv.at[d], target, tp_id)
        z_copies[d].start()
    own = pltpu.make_async_copy(rows(sp_id), place(sp_id, tp_id), own_sem)
    own.start()

    def source_of(d):
        return lax.rem(sp_id + sp - d, sp)

    started = []
    if tp == 4:
        near, far, across = square(tp_id)

        def send(d, part, target, slot, owner):
            copy = remote(
                place(source_of(d), owner, part),
                place(source_of(d), owner, part),
                t_send.at[d, slot],
                t_recv.at[d, slot],
                sp_id,
                target,
            )
            copy.start()
            started.append(copy)
            return copy

        def relay(entry):
            d, to_near, to_far = entry
            to_near[0].wait_recv()
            fourth = send(d, 0, far, 4, near)
            to_far[1].wait_recv()
            fifth = send(d, 1, near, 5, far)
            return [to_near[1], to_far[0], fourth, fifth]

        waiting, rest = None, []
        for d in order:
            if d == 0:
                own.wait()
            else:
                z_copies[d].wait_recv()
            to_near = [send(d, 0, near, 0, tp_id), None]
            to_far = [None, send(d, 1, far, 3, tp_id)]
            to_near[1] = send(d, 1, near, 1, tp_id)
            to_far[0] = send(d, 0, far, 2, tp_id)
            if waiting is not None:
                rest += relay(waiting)
            waiting = (d, to_near, to_far)
        rest += relay(waiting)
        for copy in rest:
            copy.wait_recv()
    else:
        for d in order:
            if d == 0:
                own.wait()
            else:
                z_copies[d].wait_recv()
            for t in range(1, tp):
                copy = remote(
                    place(source_of(d), tp_id),
                    place(source_of(d), tp_id),
                    t_send.at[d, t],
                    t_recv.at[d, t],
                    sp_id,
                    lax.rem(tp_id + t, tp),
                )
                copy.start()
                started.append(copy)
        for copy in started:
            copy.wait_recv()
    for copy in started:
        copy.wait_send()
    for d in order[1:]:
        z_copies[d].wait_send()


def return_kernel(sp, tp, x_ref, out_ref, landed, turned, summed, t_send, t_recv, z_send, z_recv):
    cap = x_ref.shape[0] // sp
    width = out_ref.shape[1]
    half = cap // 2
    sp_id, tp_id = lax.axis_index("sp"), lax.axis_index("tp")
    greet(
        [(lax.rem(sp_id + d, sp), tp_id) for d in range(1, sp)]
        + [(sp_id, lax.rem(tp_id + d, tp)) for d in range(1, tp)]
    )

    def rows_at(target, part=None):
        first = target * cap
        if part is not None:
            first = first + part * half
        return pl.ds(pl.multiple_of(first, half), cap if part is None else half)

    def columns(owner):
        return pl.ds(pl.multiple_of(owner * width, width), width)

    order = near_first(sp)[::-1]
    started, z_copies = [], []

    def push(src, dst, d, slot, target):
        copy = remote(src, dst, t_send.at[d, slot], t_recv.at[d, slot], sp_id, target)
        copy.start()
        started.append(copy)
        return copy

    def deliver(d, target):
        if d == 0:
            return
        copy = remote(
            summed.at[d], out_ref.at[rows_at(sp_id), :], z_send.at[d], z_recv.at[d], target, tp_id
        )
        copy.start()
        z_copies.append(copy)

    def f32(value):
        return value.astype(jnp.float32)

    def place_sum(d, part, value):
        piece = pl.ds(part * half, half)
        summed[d, piece, :] = value.astype(jnp.bfloat16)
        if d == 0:
            out_ref[rows_at(sp_id, part), :] = value.astype(jnp.bfloat16)

    targets = {d: lax.rem(sp_id + d, sp) for d in order}
    if tp == 4:
        near, far, across = square(tp_id)
        first = {}

        def open_block(d):
            target = targets[d]
            first[d] = [
                push(x_ref.at[rows_at(target, 0), columns(across)], landed.at[d, 1], d, 1, near),
                push(x_ref.at[rows_at(target, 1), columns(across)], landed.at[d, 3], d, 3, far),
                push(x_ref.at[rows_at(target, 0), columns(near)], landed.at[d, 0], d, 0, near),
                push(x_ref.at[rows_at(target, 1), columns(far)], landed.at[d, 2], d, 2, far),
            ]

        second = {}

        def turn_block(d):
            target = targets[d]
            first[d][0].wait_recv()
            turned[d, 0] = (f32(x_ref[rows_at(target, 0), columns(far)]) + f32(landed[d, 1])).astype(jnp.bfloat16)
            first[d][1].wait_recv()
            turned[d, 1] = (f32(x_ref[rows_at(target, 1), columns(near)]) + f32(landed[d, 3])).astype(jnp.bfloat16)
            second[d] = [
                push(turned.at[d, 0], landed.at[d, 4], d, 4, far),
                push(turned.at[d, 1], landed.at[d, 5], d, 5, near),
            ]

        def close_block(d):
            target = targets[d]
            first[d][2].wait_recv()
            second[d][0].wait_recv()
            place_sum(d, 0, f32(x_ref[rows_at(target, 0), columns(tp_id)]) + f32(landed[d, 0]) + f32(landed[d, 4]))
            first[d][3].wait_recv()
            second[d][1].wait_recv()
            place_sum(d, 1, f32(x_ref[rows_at(target, 1), columns(tp_id)]) + f32(landed[d, 2]) + f32(landed[d, 5]))
            deliver(d, target)

        count = len(order)
        for i in range(count + 2):
            if i < count:
                open_block(order[i])
            if 0 <= i - 1 < count:
                turn_block(order[i - 1])
            if 0 <= i - 2 < count:
                close_block(order[i - 2])
    else:
        pushed = {}
        for d in order:
            pushed[d] = []
            for t in range(1, tp):
                owner = lax.rem(tp_id + t, tp)
                for part in range(2):
                    slot = 2 * (t - 1) + part
                    pushed[d].append(
                        push(x_ref.at[rows_at(targets[d], part), columns(owner)], landed.at[d, slot], d, slot, owner)
                    )
        for d in order:
            for part in range(2):
                value = f32(x_ref[rows_at(targets[d], part), columns(tp_id)])
                for t in range(1, tp):
                    pushed[d][2 * (t - 1) + part].wait_recv()
                    value = value + f32(landed[d, 2 * (t - 1) + part])
                place_sum(d, part, value)
            deliver(d, targets[d])
    for copy in started:
        copy.wait_send()
    for copy in z_copies:
        copy.wait()


def attention_kernel(
    groups,
    start_ref,
    joined_ref,
    nope_ref,
    rope_ref,
    key_major_ref,
    value_major_ref,
    key_minor_ref,
    value_minor_ref,
    out_major_ref,
    out_minor_ref,
    key_a,
    value_a,
    key_b,
    value_b,
):
    latent = key_major_ref.shape[0]
    tok_rows = nope_ref.shape[1]
    rows_f = joined_ref[:, :latent]
    tail = joined_ref[:, latent:]
    for kept, weight in (
        (key_a, key_major_ref),
        (value_a, value_major_ref),
        (key_b, key_minor_ref),
        (value_b, value_minor_ref),
    ):
        kept[...] = jnp.dot(rows_f, weight[...], preferred_element_type=jnp.float32).astype(jnp.bfloat16)
    total_keys = joined_ref.shape[0]
    shape = (tok_rows, total_keys)
    visible = lax.broadcasted_iota(jnp.int32, shape, 1) <= start_ref[0] + lax.broadcasted_iota(jnp.int32, shape, 0)
    contract = (((1,), (1,)), ((), ()))
    index = 0
    for kept_key, kept_value, out_ref, heads, pack, scale in (
        (key_a, value_a, out_major_ref, *groups[0]),
        (key_b, value_b, out_minor_ref, *groups[1]),
    ):
        tile = kept_key.shape[1] // (-(-heads // pack))
        lanes = lax.broadcasted_iota(jnp.int32, (tok_rows, tile), 1)
        for first in range(0, heads, pack):
            columns = pl.ds(first // pack * tile, tile)
            result = None
            for member in range(min(pack, heads - first)):
                scores = lax.dot_general(
                    nope_ref[index], kept_key[:, columns], contract, preferred_element_type=jnp.float32
                ) + lax.dot_general(rope_ref[index], tail, contract, preferred_element_type=jnp.float32)
                scores = jnp.where(visible, scores * scale, -jnp.inf)
                weights = jnp.exp(scores - jnp.max(scores, axis=1, keepdims=True))
                totals = jnp.sum(weights, axis=1, keepdims=True)
                summed = jnp.dot(
                    weights.astype(jnp.bfloat16), kept_value[:, columns], preferred_element_type=jnp.float32
                ) / totals
                result = summed if result is None else jnp.where(lanes < member * (tile // pack), result, summed)
                index += 1
            out_ref[:, columns] = result.astype(jnp.bfloat16)


def expert_kernel(x_ref, gain_ref, gate_ref, up_ref, down_ref, out_ref, normed, total):
    step = pl.program_id(0)

    @pl.when(step == 0)
    def _():
        rows_f = x_ref[...].astype(jnp.float32)
        power = jnp.mean(rows_f * rows_f, axis=1, keepdims=True)
        normed[...] = (rows_f * lax.rsqrt(power + norm_eps) * gain_ref[...]).astype(jnp.bfloat16)

    rows = normed[...]
    gate_pre = jnp.dot(rows, gate_ref[0], preferred_element_type=jnp.float32)
    up_pre = jnp.dot(rows, up_ref[0], preferred_element_type=jnp.float32)
    hidden = (gate_pre / (1.0 + jnp.exp(-gate_pre)) * up_pre).astype(jnp.bfloat16)
    part = jnp.dot(hidden, down_ref[0], preferred_element_type=jnp.float32)
    last = pl.num_programs(0) - 1

    @pl.when((step == 0) & (last > 0))
    def _():
        total[...] = part

    @pl.when((step > 0) & (step < last))
    def _():
        total[...] += part

    @pl.when((step == last) & (last > 0))
    def _():
        out_ref[...] = (total[...] + part).astype(jnp.bfloat16)

    @pl.when(last == 0)
    def _():
        out_ref[...] = part.astype(jnp.bfloat16)


def flip(index, offset):
    step = 1
    while step <= offset:
        if offset & step:
            index = index + step * (1 - 2 * lax.rem(index // step, 2))
        step *= 2
    return index


def rope_table(count, width):
    half_width = width // 2
    inverse_freq = (1.0 / theta_base ** (np.arange(half_width, dtype=np.float32) * (2.0 / width))).astype(np.float32)
    angles = np.arange(count, dtype=np.float32)[:, None] * inverse_freq[None, :]
    cosine, sine = np.cos(angles), np.sin(angles)
    return np.concatenate([cosine, cosine, -sine, sine], axis=1).astype(np.float32)


def plans(chips):
    last = chips - 1
    simple = {"streamed": [("open", 0), ("relay", 0)]}
    for k in range(last):
        simple[f"between {k}"] = [("open", k + 1)]
        simple[f"after {k}"] = [("relay", k + 1)] + ([("turn", k - 1)] if k else [])
    simple[f"after {last}"] = [("turn", last - 1)] if last else []
    simple[f"after {last}"] += [("turn", last)] + [("close", k) for k in range(chips)]
    if chips != 4:
        return [simple] * chips
    ending = {
        "after 2": [("turn", 1), ("close", 0)],
        "after 3": [("turn", 2), ("close", 1), ("turn", 3), ("close", 2), ("close", 3)],
    }
    bottom = {
        "streamed": [("open", 0), ("relay", 0)],
        "between 0": [("open", 1)],
        "after 0": [("relay", 1)],
        "between 1": [("open", 2)],
        "after 1": [("relay", 2), ("open", 3), ("turn", 0)],
        "between 2": [("relay", 3)],
    }
    lower = {
        "streamed": [("open", 0), ("open", 1), ("relay", 0)],
        "between 0": [("relay", 1), ("open", 2)],
        "between 1": [("relay", 2)],
        "after 1": [("open", 3), ("turn", 0)],
        "between 2": [("relay", 3)],
    }
    upper = {
        "pushed": [("open", 0)],
        "streamed": [("relay", 0), ("open", 1), ("open", 2)],
        "between 0": [("relay", 1)],
        "after 0": [("relay", 2)],
        "between 1": [("open", 3)],
        "after 1": [("turn", 0)],
        "between 2": [("relay", 3)],
    }
    top = {
        "pushed": [("open", 0)],
        "streamed": [("relay", 0), ("open", 1), ("open", 3), ("open", 2)],
        "between 0": [("relay", 1)],
        "after 0": [("relay", 3)],
        "between 1": [("relay", 2)],
        "after 1": [("turn", 0)],
    }
    return [bottom | ending, lower | ending, upper | ending, top | ending]


def layer_kernel(
    sp,
    heads,
    q_major_ref,
    q_minor_ref,
    latent_ref,
    rope_ref,
    table_ref,
    key_major_ref,
    value_major_ref,
    key_minor_ref,
    value_minor_ref,
    out_major_ref,
    out_minor_ref,
    res_ref,
    ids_ref,
    mix_ref,
    gain_ref,
    gate_ref,
    up_ref,
    down_ref,
    out_ref,
    q_major,
    q_minor,
    rope_raw,
    table,
    weights,
    projection,
    residual,
    ids,
    mix,
    gain,
    gate,
    up,
    down,
    blocks,
    queries,
    kept,
    tops,
    scores,
    chances,
    fades,
    gathered_out,
    mixed,
    spread_part,
    spread_landed,
    spread_turned,
    stream,
    select,
    hot,
    mix_column,
    placed,
    rows_in,
    normed,
    hidden,
    part,
    landed,
    turned,
    summed,
    returned,
    load_sem,
    expert_sem,
    l_send,
    l_recv,
    q_send,
    q_recv,
    s_send,
    s_recv,
    o_send,
    o_recv,
    z_send,
    z_recv,
    t_send,
    t_recv,
    r_send,
    r_recv,
    y_send,
    y_recv,
):
    heads_major, heads_minor = heads
    tok_rows, latent = latent_ref.shape
    rope_width = rope_ref.shape[0]
    chips = sp // 2
    tp = 4
    quarter = tok_rows // tp
    pack = 128 // NOPE_MINOR
    sp_id, tp_id = lax.axis_index("sp"), lax.axis_index("tp")
    level, core = sp_id // 2, lax.rem(sp_id, 2)
    sibling = flip(sp_id, 1)
    near, far, across = square(tp_id)
    f32, bf16 = jnp.float32, jnp.bfloat16

    loads = []

    def load(src, dst):
        copy = pltpu.make_async_copy(src, dst, load_sem.at[len(loads)])
        copy.start()
        loads.append(copy)
        return copy

    own_rows = pl.ds(pl.multiple_of(sp_id * tok_rows, tok_rows), tok_rows)
    early = [
        load(latent_ref, blocks.at[0, 0, :, pl.ds(0, latent)]),
        load(rope_ref, rope_raw),
        load(table_ref.at[own_rows, :], table),
    ]
    asked = [load(q_major_ref, q_major), load(q_minor_ref, q_minor)]
    spans, first = [], 0
    for ref in (key_major_ref, key_minor_ref, value_major_ref, value_minor_ref):
        span = pl.ds(first, ref.shape[1])
        asked.append(load(ref, weights.at[:, span]))
        spans.append(span)
        first += ref.shape[1]
    split = out_major_ref.shape[0]
    routing = [load(ids_ref, ids), load(mix_ref, mix), load(gain_ref, gain)]
    late = [
        load(out_major_ref, projection.at[pl.ds(0, split), :]),
        load(out_minor_ref, projection.at[pl.ds(split, out_minor_ref.shape[0]), :]),
        load(res_ref, residual),
    ]

    barrier = pltpu.get_barrier_semaphore()
    for offset in range(1, sp):
        pl.semaphore_signal(barrier, inc=1, device_id=(flip(sp_id, offset), tp_id), device_id_type=MESH)
    for peer in (near, far, across):
        pl.semaphore_signal(barrier, inc=1, device_id=(sp_id, peer), device_id_type=MESH)

    lane = lax.broadcasted_iota(jnp.int32, (tok_rows, 128), 1)
    low = lane < rope_width

    def rotator(cosine, back, ahead):
        def rotate(x):
            return x * cosine + pltpu.roll(x, 128 - rope_width // 2, 1) * back + pltpu.roll(x, rope_width // 2, 1) * ahead

        return rotate

    for copy in early:
        copy.wait()
    trig = table[...]
    flipped = pltpu.roll(trig, 64, 1)
    half = rope_width // 2
    rotate_low = rotator(
        jnp.where(low, trig, 1.0),
        jnp.where(lane < half, flipped, 0.0),
        jnp.where((lane >= half) & low, flipped, 0.0),
    )
    rotate_high = rotator(
        jnp.where(low, 1.0, flipped),
        jnp.where(low | (lane >= 64 + half), 0.0, trig),
        jnp.where(lane >= 64 + half, trig, 0.0),
    )
    raw = rope_raw[...].astype(f32)
    raw = jnp.concatenate([raw, jnp.zeros((128 - rope_width, tok_rows), f32)], axis=0).T
    blocks[0, 0, :, latent:] = rotate_low(raw).astype(bf16)
    pl.semaphore_wait(barrier, sp - 1 + 3)

    own_quarter = pl.ds(pl.multiple_of(tp_id * quarter, quarter), quarter)

    def lift(d):
        return remote(
            blocks.at[0, 0, own_quarter, :],
            blocks.at[d, 0, own_quarter, :],
            l_send.at[d],
            l_recv.at[d],
            sp_id + 2 * d,
            tp_id,
        )

    def spread(d, slot):
        place = blocks.at[d, 0, own_quarter, :]
        return remote(place, place, q_send.at[d, slot], q_recv.at[d, slot], sp_id, (near, far, across)[slot])

    def share(d):
        return remote(blocks.at[d, 0], blocks.at[d, 1], s_send.at[d], s_recv.at[d], sibling, tp_id)

    for d in range(1, chips):

        @pl.when(level + d < chips)
        def _():
            lift(d).start()

    share(0).start()

    for copy in asked:
        copy.wait()
    pieces = 4
    for index, (src, dst) in enumerate(((gate_ref, gate), (up_ref, up), (down_ref, down))):
        count = dst.shape[0] // pieces
        for piece in range(pieces):
            span = pl.ds(piece * count, count)
            copy = pltpu.make_async_copy(src.at[0, span, :], dst.at[span, :], expert_sem.at[index])
            copy.start()
    def column(ref, index):
        return ref[:, index * 128 : index * 128 + 128].astype(f32)

    def only_low(x):
        return jnp.where(low, x, 0.0).astype(bf16)

    for pair in range(heads_major // 2):
        one, two = column(q_major, 3 * pair + 1), column(q_major, 3 * pair + 2)
        queries[2 * pair, :, :128] = q_major[:, pair * 384 : pair * 384 + 128]
        queries[2 * pair, :, 128:] = only_low(rotate_low(one))
        queries[2 * pair + 1, :, :128] = jnp.where(low, pltpu.roll(one, 64, 1), pltpu.roll(two, 64, 1)).astype(bf16)
        queries[2 * pair + 1, :, 128:] = only_low(pltpu.roll(rotate_high(two), 64, 1))
    for h in range(heads_minor):
        whole = rotate_high(column(q_minor, h))
        moved = pltpu.roll(whole, 64, 1)
        queries[heads_major + h, :, 128:] = only_low(moved)
        if h % pack == 0:
            queries[heads_major + h, :, :128] = only_low(whole)
        else:
            queries[heads_major + h, :, :128] = jnp.where(low, 0.0, moved).astype(bf16)

    keys = 2 * tok_rows
    log2e = 1.4426950408889634
    contract = (((1,), (1,)), ((), ()))

    def project(d):
        for q in range(2):
            rows = blocks[d, q, :, :latent]
            kept[pl.ds(q * tok_rows, tok_rows), :] = jnp.dot(rows, weights[...], preferred_element_type=f32).astype(
                bf16
            )

    everyone = range(heads_major + heads_minor)

    def tile_of(h):
        return h if h < heads_major else (h - heads_major) // pack

    def attend(d):
        tails = jnp.concatenate([blocks[d, 0, :, latent:], blocks[d, 1, :, latent:]], axis=0)
        for h in everyone:
            nope = NOPE_MAJOR if h < heads_major else NOPE_MINOR
            key_at = tile_of(h) * 128 + (0 if h < heads_major else spans[1].start)
            key = jnp.concatenate([kept[:, key_at : key_at + 128], tails], axis=1)
            scale = (nope + rope_width) ** (-0.5) * log2e
            value = lax.dot_general(queries[h], key, contract, preferred_element_type=f32) * scale
            if d == 0:
                spot = lax.broadcasted_iota(jnp.int32, (tok_rows, keys), 1)
                row = lax.broadcasted_iota(jnp.int32, (tok_rows, keys), 0)
                limit = jnp.where(spot < tok_rows, row, keys * core - 1)
                value = jnp.where(spot <= limit, value, -jnp.inf)
            scores[h] = value
        for h in everyone:
            value = scores[h]
            peak = jnp.max(value, axis=1, keepdims=True)
            if d > 0:
                before = tops[h][:, :1]
                peak = jnp.maximum(before, peak)
                fades[h] = jnp.broadcast_to(jnp.exp2(before - peak), (tok_rows, 128))
            chances[h] = jnp.exp2(value - peak).astype(bf16)
            tops[h] = jnp.broadcast_to(peak, (tok_rows, 128))
        ones = jnp.ones((keys, 128), bf16)
        for h in everyone:
            value_at = tile_of(h) * 128 + (spans[2].start if h < heads_major else spans[3].start)
            value = jnp.concatenate([kept[:, value_at : value_at + 128], ones], axis=1)
            summed = jnp.dot(chances[h], value, preferred_element_type=f32)
            if d == 0:
                gathered_out[h] = summed
            else:
                fade = fades[h]
                gathered_out[h, :, :128] = summed[:, :128] + gathered_out[h, :, :128] * fade
                gathered_out[h, :, 128:] = summed[:, 128:] + gathered_out[h, :, 128:] * fade

    slots = placed.shape[0]
    cap = slots // sp
    width = stream.shape[1]

    def prepare_routing():
        for copy in routing:
            copy.wait()
        lanes = lax.broadcasted_iota(jnp.int32, (sp, tok_rows), 0)
        matches = [(lanes == ids[j : j + 1, :]).astype(f32) for j in range(TOP)]
        order = (tok_rows, tok_rows)
        before = lax.broadcasted_iota(jnp.int32, order, 0) < lax.broadcasted_iota(jnp.int32, order, 1)
        named = functools.reduce(lambda a, b: a + b, matches)
        earlier = jnp.dot(named.astype(bf16), before.astype(bf16), preferred_element_type=f32)
        slot_rows = lax.broadcasted_iota(jnp.int32, (slots, tok_rows), 0)
        either = None
        for j in range(TOP):
            rank = jnp.sum(matches[j] * earlier, axis=0, keepdims=True).astype(jnp.int32)
            earlier = earlier + matches[j]
            chosen = jnp.where(slot_rows == ids[j : j + 1, :] * cap + rank, 1.0, 0.0)
            hot[j] = chosen.T.astype(bf16)
            mix_column[j] = jnp.broadcast_to(mix[j : j + 1, :], order).T
            either = chosen if either is None else either + chosen
        select[...] = either.astype(bf16)

    def columns(owner):
        return pl.ds(pl.multiple_of(owner * width, width), width)

    def arrival(place, sem):
        return pltpu.make_async_copy(place, place, sem)

    own_columns = columns(tp_id)

    def block(index):
        return pl.ds(pl.multiple_of(index * cap, cap), cap)

    def ends(target_level, q):
        return 2 * target_level + flip(core, q)

    def handoff(k, q, target_level):
        return remote(
            placed.at[block(ends(target_level, q)), :],
            rows_in.at[level, pl.ds(q * cap, cap), own_columns],
            z_send,
            z_recv.at[level, q],
            ends(target_level, q),
            tp_id,
        )

    parts = {0: (0, 0, 0), 1: (1, 0, 0), 2: (0, 0, 1), 3: (1, 0, 1), 4: (0, 1, 1), 5: (1, 1, 0)}

    def pass_on(k, slot):
        q, borrowed, to_far = parts[slot]
        owner = tp_id
        if borrowed:
            owner = near if slot == 4 else far
        place = rows_in.at[k, pl.ds(q * cap, cap), columns(owner)]
        target = far if to_far else near
        return remote(place, place, t_send, t_recv.at[k, slot], sp_id, target)

    def open_chunk(k):
        @pl.when(level != k)
        def _():
            arrival(rows_in.at[k, pl.ds(0, cap), own_columns], z_recv.at[k, 0]).wait()

        pass_on(k, 0).start()
        pass_on(k, 2).start()
        arrival(rows_in.at[k, pl.ds(cap, cap), own_columns], z_recv.at[k, 1]).wait()
        pass_on(k, 3).start()
        pass_on(k, 1).start()

    def relay(k):
        pass_on(k, 0).wait_recv()
        pass_on(k, 4).start()
        pass_on(k, 3).wait_recv()
        pass_on(k, 5).start()

    def push(k, slot):
        src, target = {
            0: (part.at[k, pl.ds(0, cap), columns(near)], near),
            1: (part.at[k, pl.ds(0, cap), columns(across)], near),
            2: (part.at[k, pl.ds(cap, cap), columns(far)], far),
            3: (part.at[k, pl.ds(cap, cap), columns(across)], far),
            4: (turned.at[k, 0], far),
            5: (turned.at[k, 1], near),
        }[slot]
        return remote(src, landed.at[k, slot], r_send, r_recv.at[k, slot], sp_id, target)

    def wide(value):
        return value.astype(f32)

    def turn(k):
        push(k, 1).wait_recv()
        turned[k, 0] = (wide(part[k, :cap, columns(far)]) + wide(landed[k, 1])).astype(bf16)
        push(k, 4).start()
        push(k, 3).wait_recv()
        turned[k, 1] = (wide(part[k, cap:, columns(near)]) + wide(landed[k, 3])).astype(bf16)
        push(k, 5).start()

    def back(k, q):
        return remote(
            summed.at[k, q],
            returned.at[block(sp_id), :],
            y_send,
            y_recv.at[level, q],
            ends(k, q),
            tp_id,
        )

    def close(k):
        for q in range(2):
            push(k, 2 * q).wait_recv()
            push(k, 4 + q).wait_recv()
            value = wide(part[k, q * cap : q * cap + cap, own_columns])
            value = (value + wide(landed[k, 2 * q]) + wide(landed[k, 4 + q])).astype(bf16)
            summed[k, q] = value
            if q == 1:
                back(k, q).start()
                continue

            @pl.when(level == k)
            def _():
                returned[block(sp_id), :] = summed[k, 0]

            @pl.when(level != k)
            def _():
                back(k, 0).start()

    actions = {"open": open_chunk, "relay": relay, "turn": turn, "close": close}

    def run(point):
        for here, plan in enumerate(plans(chips)):
            events = plan.get(point, ())
            if events:

                @pl.when(level == here)
                def _():
                    for action, k in events:
                        actions[action](k)

    def forward(d):
        @pl.when(level >= d)
        def _():
            arrival(blocks.at[d, 0, own_quarter, :], l_recv.at[d]).wait()
            for slot in range(3):
                spread(d, slot).start()

    for d in range(1, chips // 2):
        forward(d)
    share(0).wait_recv()
    project(0)
    for d in range(chips // 2, chips - 1):
        forward(d)
    attend(0)
    forward(chips - 1)
    def collect(d):
        @pl.when(level >= d)
        def _():
            for slot in range(3):
                spread(d, slot).wait_recv()
            share(d).start()

    def process(d):
        @pl.when(level >= d)
        def _():
            share(d).wait_recv()
            project(d)
            attend(d)

    collect(1)
    prepare_routing()
    process(1)
    for d in range(2, chips):
        collect(d)
    for d in range(2, chips):
        process(d)

    def share_of(h):
        return gathered_out[h, :, :128] / gathered_out[h, :, 128:]

    for h in range(heads_major):
        mixed[:, h * 128 : h * 128 + 128] = share_of(h).astype(bf16)
    for tile in range(-(-heads_minor // pack)):
        result = None
        for member in range(min(pack, heads_minor - tile * pack)):
            h = heads_major + tile * pack + member
            value = share_of(h)
            result = value if result is None else jnp.where(lane < member * NOPE_MINOR, result, value)
        first = (heads_major + tile) * 128
        mixed[:, first : first + 128] = result.astype(bf16)

    for copy in late:
        copy.wait()

    mid = tok_rows // 2
    mids = (pl.ds(0, mid), pl.ds(mid, mid))
    rows = mixed[...]

    def fill_out(owner):
        spread_part[:, columns(owner)] = jnp.dot(rows, projection[:, columns(owner)], preferred_element_type=f32).astype(bf16)

    def push_out(src, slot, target):
        copy = remote(src, spread_landed.at[slot], o_send, o_recv.at[slot], sp_id, target)
        copy.start()
        return copy

    fill_out(across)
    second = push_out(spread_part.at[mids[0], columns(across)], 1, near)
    fourth = push_out(spread_part.at[mids[1], columns(across)], 3, far)
    fill_out(near)
    first = push_out(spread_part.at[mids[0], columns(near)], 0, near)
    fill_out(far)
    third = push_out(spread_part.at[mids[1], columns(far)], 2, far)
    fill_out(tp_id)
    second.wait_recv()
    spread_turned[0] = (spread_part[mids[0], columns(far)].astype(f32) + spread_landed[1].astype(f32)).astype(bf16)
    fifth = push_out(spread_turned.at[0], 4, far)
    fourth.wait_recv()
    spread_turned[1] = (spread_part[mids[1], columns(near)].astype(f32) + spread_landed[3].astype(f32)).astype(bf16)
    sixth = push_out(spread_turned.at[1], 5, near)
    run("pushed")
    for q, plain, bent in ((0, first, fifth), (1, third, sixth)):
        plain.wait_recv()
        value = spread_part[mids[q], columns(tp_id)].astype(f32) + residual[mids[q], :].astype(f32)
        value = value + spread_landed[2 * q].astype(f32)
        bent.wait_recv()
        stream[mids[q], :] = (value + spread_landed[4 + q].astype(f32)).astype(bf16)

    units = gate.shape[1]
    placed[...] = jnp.dot(select[...], stream[...], preferred_element_type=f32).astype(bf16)

    handoff(0, 1, level).start()

    @pl.when(level == 0)
    def _():
        for k in range(1, chips):
            for q in range(2):
                handoff(k, q, flip(level, k)).start()

    @pl.when(level > 0)
    def _():
        for k in range(chips - 1, 0, -1):
            for q in range(2):
                handoff(k, q, flip(level, k)).start()

    rows_in[level, 0:cap, own_columns] = placed[block(sp_id), :]

    def ready(k):
        for slot in (1, 2, 4, 5):
            pass_on(k, slot).wait_recv()
        rows = rows_in[k].astype(f32)
        power = jnp.mean(rows * rows, axis=1, keepdims=True)
        normed[...] = (rows * lax.rsqrt(power + norm_eps) * gain[...]).astype(bf16)

    def expand():
        tile = 256
        rows = normed[...]
        for first in range(0, units, tile):
            span = slice(first, first + tile)
            gate_pre = jnp.dot(rows, gate[:, span], preferred_element_type=f32)
            up_pre = jnp.dot(rows, up[:, span], preferred_element_type=f32)
            hidden[:, span] = (gate_pre / (1.0 + jnp.exp(-gate_pre)) * up_pre).astype(bf16)

    def contract(k):
        rows = hidden[...]

        def fill(owner):
            part[k, :, columns(owner)] = jnp.dot(
                rows, down[:, columns(owner)], preferred_element_type=f32
            ).astype(bf16)

        fill(across)
        push(k, 1).start()
        push(k, 3).start()
        fill(near)
        push(k, 0).start()
        fill(far)
        push(k, 2).start()
        fill(tp_id)

    run("streamed")
    for index, ref in enumerate((gate, up, down)):
        arrival(ref, expert_sem.at[index]).wait()
    for k in range(chips):
        ready(k)
        expand()
        run(f"between {k}")
        contract(k)
        run(f"after {k}")

    total = stream[...].astype(f32)
    for k in range(chips):
        source = flip(level, k)
        for q in range(2):
            if k > 0 or q > 0:
                arrival(returned.at[block(ends(source, q)), :], y_recv.at[source, q]).wait()
        span = pl.ds(pl.multiple_of(source * 2 * cap, 2 * cap), 2 * cap)
        for j in range(TOP):
            picked = jnp.dot(hot[j, :, span], returned[span, :], preferred_element_type=f32)
            total = total + picked * mix_column[j][:, :1]
    out_ref[...] = total
    arrival(landed, t_send).wait()
    arrival(landed, r_send).wait()
    sent = pl.ds(0, (sp - 1) * cap)
    arrival(returned.at[sent, :], z_send).wait()
    arrival(returned.at[sent, :], y_send).wait()
    arrival(spread_landed, o_send).wait()
    share(0).wait_send()
    for d in range(1, chips):

        @pl.when(level + d < chips)
        def _():
            lift(d).wait_send()

        @pl.when(level >= d)
        def _():
            share(d).wait_send()
            for slot in range(3):
                spread(d, slot).wait_send()


def fused_layer(
    sp,
    tp,
    query_major,
    query_minor,
    latent_rows,
    rope_keys,
    key_up_major,
    value_up_major,
    key_up_minor,
    value_up_minor,
    out_major,
    out_minor,
    residual,
    norm_gain,
    expert_ids,
    expert_weights,
    gate_proj,
    up_proj,
    down_proj,
):
    tok_rows, latent = latent_rows.shape
    rope_width = rope_keys.shape[1]
    width = residual.shape[1]
    features = tp * width
    units = gate_proj.shape[2]
    chips = sp // 2
    cap = 2 * tok_rows * TOP // sp
    slots = sp * cap
    heads = (key_up_major.shape[1] // NOPE_MAJOR, key_up_minor.shape[1] // NOPE_MINOR)
    count = heads[0] + heads[1]
    joined = latent + rope_width + -(latent + rope_width) % 128
    kept = key_up_major.shape[1] + key_up_minor.shape[1] + value_up_major.shape[1] + value_up_minor.shape[1]
    mixed = value_up_major.shape[1] + value_up_minor.shape[1]
    dma = pltpu.SemaphoreType.DMA
    bf16, f32 = jnp.bfloat16, jnp.float32
    table = jnp.asarray(rope_table(sp * tok_rows, rope_width))
    operands = (
        query_major,
        query_minor,
        latent_rows,
        rope_keys.T,
        table,
        key_up_major,
        value_up_major,
        key_up_minor,
        value_up_minor,
        out_major,
        out_minor,
        residual,
        expert_ids.T,
        expert_weights.T,
        norm_gain.reshape(1, -1),
        gate_proj,
        up_proj,
        down_proj,
    )
    vmem = pltpu.VMEM
    return pl.pallas_call(
        functools.partial(layer_kernel, sp, heads),
        out_shape=pltpu.VMEM((tok_rows, width), f32),
        in_specs=[pl.BlockSpec(memory_space=pl.ANY)] * len(operands),
        out_specs=pl.BlockSpec(memory_space=pltpu.VMEM),
        scratch_shapes=[
            vmem(query_major.shape, bf16),
            vmem(query_minor.shape, bf16),
            vmem((rope_width, tok_rows), bf16),
            vmem((tok_rows, 2 * rope_width), f32),
            vmem((latent, kept), bf16),
            vmem((mixed, features), bf16),
            vmem(residual.shape, bf16),
            vmem((TOP, tok_rows), jnp.int32),
            vmem((TOP, tok_rows), f32),
            vmem((1, features), f32),
            vmem((features, units), bf16),
            vmem((features, units), bf16),
            vmem((units, features), bf16),
            vmem((chips, 2, tok_rows, joined), bf16),
            vmem((count, tok_rows, 256), bf16),
            vmem((2 * tok_rows, kept), bf16),
            vmem((count, tok_rows, 128), f32),
            vmem((count, tok_rows, 2 * tok_rows), f32),
            vmem((count, tok_rows, 2 * tok_rows), bf16),
            vmem((count, tok_rows, 128), f32),
            vmem((count, tok_rows, 256), f32),
            vmem((tok_rows, mixed), bf16),
            vmem((tok_rows, features), bf16),
            vmem((6, tok_rows // 2, width), bf16),
            vmem((2, tok_rows // 2, width), bf16),
            vmem((tok_rows, width), bf16),
            vmem((slots, tok_rows), bf16),
            vmem((TOP, tok_rows, slots), bf16),
            vmem((TOP, tok_rows, tok_rows), f32),
            vmem((slots, width), bf16),
            vmem((chips, 2 * cap, features), bf16),
            vmem((2 * cap, features), bf16),
            vmem((2 * cap, units), bf16),
            vmem((chips, 2 * cap, features), bf16),
            vmem((chips, 6, cap, width), bf16),
            vmem((chips, 2, cap, width), bf16),
            vmem((chips, 2, cap, width), bf16),
            vmem((slots, width), bf16),
            dma((len(operands),)),
            dma((3,)),
            dma((chips,)),
            dma((chips,)),
            dma((chips, 3)),
            dma((chips, 3)),
            dma((chips,)),
            dma((chips,)),
            dma,
            dma((6,)),
            dma,
            dma((chips, 2)),
            dma,
            dma((chips, 6)),
            dma,
            dma((chips, 6)),
            dma,
            dma((chips, 2)),
        ],
        compiler_params=pltpu.CompilerParams(
            collective_id=4, has_side_effects=True, vmem_limit_bytes=60 * 1024 * 1024
        ),
    )(*operands).astype(bf16)


def run_experts(rows, gain, gate_proj, up_proj, down_proj):
    slots, features = rows.shape
    units = gate_proj.shape[2]
    tile = min(256, units)
    return pl.pallas_call(
        expert_kernel,
        grid=(units // tile,),
        out_shape=jax.ShapeDtypeStruct((slots, features), jnp.bfloat16),
        in_specs=[
            pl.BlockSpec((slots, features), lambda i: (0, 0)),
            pl.BlockSpec((1, features), lambda i: (0, 0)),
            pl.BlockSpec((1, features, tile), lambda i: (0, 0, i)),
            pl.BlockSpec((1, features, tile), lambda i: (0, 0, i)),
            pl.BlockSpec((1, tile, features), lambda i: (0, i, 0)),
        ],
        out_specs=pl.BlockSpec((slots, features), lambda i: (0, 0)),
        scratch_shapes=[
            pltpu.VMEM((slots, features), jnp.bfloat16),
            pltpu.VMEM((slots, features), jnp.float32),
        ],
        compiler_params=pltpu.CompilerParams(vmem_limit_bytes=60 * 1024 * 1024),
    )(rows, gain.reshape(1, -1), gate_proj, up_proj, down_proj)


def pad_columns(array, multiple):
    return jnp.pad(array, ((0, 0), (0, -array.shape[1] % multiple)))


def per_device(
    sp,
    tp,
    query_major,
    query_minor,
    latent_rows,
    rope_keys,
    key_up_major,
    value_up_major,
    key_up_minor,
    value_up_minor,
    out_major,
    out_minor,
    residual,
    norm_gain,
    expert_ids,
    expert_weights,
    gate_proj,
    up_proj,
    down_proj,
):
    tok_rows = query_major.shape[0]
    fast = tp == 4 and sp & (sp - 1) == 0
    fast = fast and tok_rows % 64 == 0 and (2 * tok_rows * TOP // sp) % 16 == 0
    fast = fast and key_up_major.shape[1] % 128 == 0 and key_up_minor.shape[1] % 128 == 0
    if fast:
        return fused_layer(
            sp,
            tp,
            query_major,
            query_minor,
            latent_rows,
            rope_keys,
            key_up_major,
            value_up_major,
            key_up_minor,
            value_up_minor,
            out_major,
            out_minor,
            residual,
            norm_gain,
            expert_ids,
            expert_weights,
            gate_proj,
            up_proj,
            down_proj,
        )
    row_start = lax.axis_index("sp") * tok_rows
    positions = row_start + jnp.arange(tok_rows, dtype=jnp.int32)
    rope_width = rope_keys.shape[1]
    latent = latent_rows.shape[1]
    rope_rot = rotary(rope_keys, positions).astype(jnp.bfloat16)
    heads_major = key_up_major.shape[1] // NOPE_MAJOR
    heads_minor = key_up_minor.shape[1] // NOPE_MINOR
    shaped_major = query_major.reshape(tok_rows, heads_major, NOPE_MAJOR + rope_width)
    shaped_minor = query_minor.reshape(tok_rows, heads_minor, NOPE_MINOR + rope_width)
    nope_major = shaped_major[:, :, :NOPE_MAJOR]
    nope_minor = shaped_minor[:, :, :NOPE_MINOR]
    turned_major = rotary(shaped_major[:, :, NOPE_MAJOR:], positions).astype(jnp.bfloat16)
    turned_minor = rotary(shaped_minor[:, :, NOPE_MINOR:], positions).astype(jnp.bfloat16)
    scale_major = (NOPE_MAJOR + rope_width) ** (-0.5)
    scale_minor = (NOPE_MINOR + rope_width) ** (-0.5)

    joined = jnp.concatenate(
        [latent_rows, rope_rot, jnp.zeros((tok_rows, -(latent + rope_width) % 128), jnp.bfloat16)], axis=1
    )
    dma = pltpu.SemaphoreType.DMA
    chips = sp // 2
    gathered = comm_call(
        functools.partial(gather_kernel, sp),
        jax.ShapeDtypeStruct((sp * tok_rows, joined.shape[1]), jnp.bfloat16),
        [dma((chips,)), dma((chips,)), dma((chips,)), dma((chips,))],
        0,
        (joined,),
    )
    tail_width = joined.shape[1] - latent

    def by_head(array, width):
        return jnp.pad(array.transpose(1, 0, 2), ((0, 0), (0, 0), (0, width - array.shape[2])))

    pack = 128 // NOPE_MINOR
    spread = nope_minor.transpose(1, 0, 2)
    member = (jnp.arange(heads_minor, dtype=jnp.int32) % pack)[:, None, None]
    spread = jnp.concatenate(
        [jnp.where(member == m, spread, jnp.zeros_like(spread)) for m in range(pack)], axis=2
    )
    nope_all = jnp.concatenate([by_head(nope_major, 128), spread], axis=0)
    rope_all = jnp.concatenate([by_head(turned_major, tail_width), by_head(turned_minor, tail_width)], axis=0)
    minor_weights = [pad_columns(key_up_minor, 128), pad_columns(value_up_minor, 128)]
    minor_width = minor_weights[0].shape[1]
    keys = sp * tok_rows
    vmem = pl.BlockSpec(memory_space=pltpu.VMEM)
    attn_major, attn_minor = pl.pallas_call(
        functools.partial(attention_kernel, ((heads_major, 1, scale_major), (heads_minor, pack, scale_minor))),
        out_shape=(
            jax.ShapeDtypeStruct((tok_rows, value_up_major.shape[1]), jnp.bfloat16),
            jax.ShapeDtypeStruct((tok_rows, minor_width), jnp.bfloat16),
        ),
        in_specs=[pl.BlockSpec(memory_space=pltpu.SMEM)] + [vmem] * 7,
        out_specs=(vmem, vmem),
        scratch_shapes=[
            pltpu.VMEM((keys, key_up_major.shape[1]), jnp.bfloat16),
            pltpu.VMEM((keys, value_up_major.shape[1]), jnp.bfloat16),
            pltpu.VMEM((keys, minor_width), jnp.bfloat16),
            pltpu.VMEM((keys, minor_width), jnp.bfloat16),
        ],
        compiler_params=pltpu.CompilerParams(vmem_limit_bytes=60 * 1024 * 1024),
    )(
        row_start.reshape(1).astype(jnp.int32),
        gathered,
        nope_all,
        rope_all,
        key_up_major,
        value_up_major,
        *minor_weights,
    )
    attn_minor = attn_minor[:, : value_up_minor.shape[1]]
    partial_value = jnp.dot(attn_major, out_major, preferred_element_type=jnp.float32)
    partial_value = partial_value + jnp.dot(
        attn_minor, out_minor, preferred_element_type=jnp.float32
    )
    width = residual.shape[1]
    stream_mid = comm_call(
        functools.partial(reduce_kernel, tp),
        jax.ShapeDtypeStruct((tok_rows, width), jnp.bfloat16),
        [pltpu.VMEM((tp - 1, tok_rows, width), jnp.bfloat16), dma((tp - 1,)), dma((tp - 1,))],
        1,
        (partial_value.astype(jnp.bfloat16), residual),
    )
    experts = sp
    capacity = 2 * tok_rows * TOP // experts
    slots = experts * capacity
    slot_list = slot_ids(expert_ids, experts, capacity)
    slot_numbers = jnp.arange(slots, dtype=jnp.int32)
    by_slot = slot_list.T
    select = (slot_numbers[:, None] == by_slot[0][None, :]).astype(jnp.bfloat16)
    for j in range(1, TOP):
        select = select + (slot_numbers[:, None] == by_slot[j][None, :]).astype(jnp.bfloat16)
    placed = jnp.dot(select, stream_mid, preferred_element_type=jnp.float32).astype(jnp.bfloat16)
    slots_t = 6 if tp == 4 else tp
    arrived = comm_call(
        functools.partial(dispatch_kernel, sp, tp),
        jax.ShapeDtypeStruct((slots, tp * width), jnp.bfloat16),
        [dma((sp,)), dma((sp,)), dma((sp, slots_t)), dma((sp, slots_t)), dma],
        2,
        (placed,),
    )
    down_part = run_experts(arrived, norm_gain, gate_proj, up_proj, down_proj)
    pieces = 6 if tp == 4 else 2 * (tp - 1)
    half = capacity // 2
    flat_out = comm_call(
        functools.partial(return_kernel, sp, tp),
        jax.ShapeDtypeStruct((slots, width), jnp.bfloat16),
        [
            pltpu.VMEM((sp, pieces, half, width), jnp.bfloat16),
            pltpu.VMEM((sp, 2, half, width), jnp.bfloat16),
            pltpu.VMEM((sp, capacity, width), jnp.bfloat16),
            dma((sp, pieces)),
            dma((sp, pieces)),
            dma((sp,)),
            dma((sp,)),
        ],
        3,
        (down_part,),
    )
    mixed = stream_mid.astype(jnp.float32)
    for j in range(TOP):
        hot = (slot_list[:, j : j + 1] == slot_numbers[None, :]).astype(jnp.bfloat16)
        mixed = mixed + jnp.dot(hot, flat_out, preferred_element_type=jnp.float32) * expert_weights[:, j : j + 1]
    return mixed.astype(jnp.bfloat16)


def solution(mesh):
    in_specs = (
        P("sp", "tp"),
        P("sp", "tp"),
        P("sp", None),
        P("sp", None),
        P(None, "tp"),
        P(None, "tp"),
        P(None, "tp"),
        P(None, "tp"),
        P("tp", None),
        P("tp", None),
        P("sp", "tp"),
        P(),
        P("sp", None),
        P("sp", None),
        P("sp", None, "tp"),
        P("sp", None, "tp"),
        P("sp", "tp", None),
    )
    out_specs = P("sp", "tp")
    return jax.shard_map(
        functools.partial(per_device, mesh.shape["sp"], mesh.shape["tp"]),
        mesh=mesh,
        in_specs=in_specs,
        out_specs=out_specs,
        check_vma=False,
    )
```

```python
import functools

import jax
import jax.numpy as jnp
import numpy as np
from jax import lax
from jax.experimental import pallas as pl
from jax.experimental.pallas import tpu as pltpu
from jax.sharding import PartitionSpec as P

NOPE_MAJOR = 128
NOPE_MINOR = 64
TOP = 2
MESH = pl.DeviceIdType.MESH

theta_base = 10000.0
norm_eps = 1e-06


def rotary(values, positions):
    half_width = values.shape[-1] // 2
    inverse_freq = 1.0 / theta_base ** (
        jnp.arange(half_width, dtype=jnp.float32) * (2.0 / values.shape[-1])
    )
    angles = positions.astype(jnp.float32)[:, None] * inverse_freq[None, :]
    view_shape = (angles.shape[0],) + (1,) * (values.ndim - 2) + (half_width,)
    cosine = jnp.cos(angles).reshape(view_shape)
    sine_table = jnp.sin(angles).reshape(view_shape)
    lower_half = values[..., :half_width].astype(jnp.float32)
    upper_half = values[..., half_width:].astype(jnp.float32)
    return jnp.concatenate(
        [
            lower_half * cosine - upper_half * sine_table,
            upper_half * cosine + lower_half * sine_table,
        ],
        axis=-1,
    )


def slot_ids(route_block, experts, capacity):
    pairs = route_block.reshape(-1)
    matches = pairs[:, None] == jnp.arange(experts, dtype=jnp.int32)[None, :]
    order = jnp.arange(pairs.shape[0], dtype=jnp.int32)
    earlier = (order[:, None] > order[None, :]).astype(jnp.bfloat16)
    ranks = jnp.dot(earlier, matches.astype(jnp.bfloat16), preferred_element_type=jnp.float32)
    rank = jnp.sum(jnp.where(matches, ranks, 0.0), axis=1).astype(jnp.int32)
    return (pairs * capacity + rank).reshape(route_block.shape)


def remote(src, dst, send_sem, recv_sem, sp_id, tp_id):
    return pltpu.make_async_remote_copy(
        src_ref=src,
        dst_ref=dst,
        send_sem=send_sem,
        recv_sem=recv_sem,
        device_id=(sp_id, tp_id),
        device_id_type=MESH,
    )


def greet(partners):
    barrier = pltpu.get_barrier_semaphore()
    for sp_id, tp_id in partners:
        pl.semaphore_signal(barrier, inc=1, device_id=(sp_id, tp_id), device_id_type=MESH)
    pl.semaphore_wait(barrier, len(partners))


def comm_call(body, out_shape, scratch, collective_id, operands, limit=60 * 1024 * 1024):
    return pl.pallas_call(
        body,
        out_shape=out_shape,
        in_specs=[pl.BlockSpec(memory_space=pltpu.VMEM)] * len(operands),
        out_specs=pl.BlockSpec(memory_space=pltpu.VMEM),
        scratch_shapes=scratch,
        compiler_params=pltpu.CompilerParams(
            collective_id=collective_id, has_side_effects=True, vmem_limit_bytes=limit
        ),
    )(*operands)


def gather_kernel(sp, x_ref, out_ref, up_send, up_recv, side_send, side_recv):
    rows = x_ref.shape[0]
    chips = sp // 2
    sp_id, tp_id = lax.axis_index("sp"), lax.axis_index("tp")
    level, core = sp_id // 2, lax.rem(sp_id, 2)
    sibling = 2 * level + 1 - core
    barrier = pltpu.get_barrier_semaphore()
    pl.semaphore_signal(barrier, inc=1, device_id=(sibling, tp_id), device_id_type=MESH)

    @pl.when(level > 0)
    def _():
        pl.semaphore_signal(barrier, inc=1, device_id=(sp_id - 2, tp_id), device_id_type=MESH)

    @pl.when(level < chips - 1)
    def _():
        pl.semaphore_signal(barrier, inc=1, device_id=(sp_id + 2, tp_id), device_id_type=MESH)

    pl.semaphore_wait(barrier, 1 + lax.min(level, 1) + lax.min(chips - 1 - level, 1))

    def rows_of(index):
        return pl.ds(pl.multiple_of(index * rows, rows), rows)

    def up_copy(step, src):
        place = out_ref.at[rows_of(sp_id - 2 * step), :]
        return remote(src if src is not None else place, place, up_send.at[step], up_recv.at[step], sp_id + 2, tp_id)

    def side_copy(step, src):
        place = out_ref.at[rows_of(sp_id - 2 * step), :]
        return remote(src if src is not None else place, place, side_send.at[step], side_recv.at[step], sibling, tp_id)

    def arrival(sem, index):
        place = out_ref.at[rows_of(index), :]
        return pltpu.make_async_copy(place, place, sem)

    @pl.when(level < chips - 1)
    def _():
        up_copy(0, x_ref).start()

    side_copy(0, x_ref).start()
    out_ref[rows_of(sp_id), :] = x_ref[...]
    for other in range(1, chips):

        @pl.when(level + other < chips)
        def _():
            first = pl.multiple_of((level + other) * 2 * rows, 2 * rows)
            out_ref[pl.ds(first, 2 * rows), :] = jnp.zeros((2 * rows, out_ref.shape[1]), out_ref.dtype)

    for step in range(1, chips):

        @pl.when(level - step >= 0)
        def _():
            arrival(up_recv.at[step - 1], sp_id - 2 * step).wait()

            @pl.when(level < chips - 1)
            def _():
                up_copy(step, None).start()

            side_copy(step, None).start()

    for step in range(chips):

        @pl.when(level - step >= 0)
        def _():
            arrival(side_recv.at[step], sibling - 2 * step).wait()
            side_copy(step, x_ref if step == 0 else None).wait_send()

            @pl.when(level < chips - 1)
            def _():
                up_copy(step, x_ref if step == 0 else None).wait_send()


def reduce_kernel(tp, part_ref, res_ref, out_ref, landed, send_sem, recv_sem):
    width = res_ref.shape[1]
    sp_id, tp_id = lax.axis_index("sp"), lax.axis_index("tp")
    peers = [lax.rem(tp_id + d, tp) for d in range(1, tp)]
    greet([(sp_id, p) for p in peers])

    def columns(index):
        return pl.ds(pl.multiple_of(index * width, width), width)

    copies = []
    for d in range(1, tp):
        copy = remote(
            part_ref.at[:, columns(peers[d - 1])],
            landed.at[d - 1],
            send_sem.at[d - 1],
            recv_sem.at[d - 1],
            sp_id,
            peers[d - 1],
        )
        copy.start()
        copies.append(copy)
    total = part_ref[:, columns(tp_id)].astype(jnp.float32)
    for d in range(1, tp):
        copies[d - 1].wait()
        total = total + landed[d - 1].astype(jnp.float32)
    out_ref[...] = (res_ref[...].astype(jnp.float32) + total).astype(jnp.bfloat16)


def near_first(count):
    order = [0]
    for d in range(1, count // 2 + 1):
        order.append(d)
        if count - d != d:
            order.append(count - d)
    return order


def square(tp_id):
    low = lax.rem(tp_id, 2)
    high = tp_id // 2
    return 2 * high + 1 - low, 2 * (1 - high) + low, 2 * (1 - high) + 1 - low


def dispatch_kernel(sp, tp, x_ref, out_ref, z_send, z_recv, t_send, t_recv, own_sem):
    cap = x_ref.shape[0] // sp
    width = x_ref.shape[1]
    half = cap // 2
    sp_id, tp_id = lax.axis_index("sp"), lax.axis_index("tp")
    greet(
        [(lax.rem(sp_id + d, sp), tp_id) for d in range(1, sp)]
        + [(sp_id, lax.rem(tp_id + d, tp)) for d in range(1, tp)]
    )

    def place(source, owner, part=None):
        first = source * cap
        if part is not None:
            first = first + part * half
        count = cap if part is None else half
        return out_ref.at[
            pl.ds(pl.multiple_of(first, half), count),
            pl.ds(pl.multiple_of(owner * width, width), width),
        ]

    def rows(source, part=None):
        first = source * cap
        if part is not None:
            first = first + part * half
        return x_ref.at[pl.ds(pl.multiple_of(first, half), cap if part is None else half), :]

    order = near_first(sp)
    z_copies = {}
    for d in order[1:]:
        target = lax.rem(sp_id + d, sp)
        z_copies[d] = remote(rows(target), place(sp_id, tp_id), z_send.at[d], z_recv.at[d], target, tp_id)
        z_copies[d].start()
    own = pltpu.make_async_copy(rows(sp_id), place(sp_id, tp_id), own_sem)
    own.start()

    def source_of(d):
        return lax.rem(sp_id + sp - d, sp)

    started = []
    if tp == 4:
        near, far, across = square(tp_id)

        def send(d, part, target, slot, owner):
            copy = remote(
                place(source_of(d), owner, part),
                place(source_of(d), owner, part),
                t_send.at[d, slot],
                t_recv.at[d, slot],
                sp_id,
                target,
            )
            copy.start()
            started.append(copy)
            return copy

        def relay(entry):
            d, to_near, to_far = entry
            to_near[0].wait_recv()
            fourth = send(d, 0, far, 4, near)
            to_far[1].wait_recv()
            fifth = send(d, 1, near, 5, far)
            return [to_near[1], to_far[0], fourth, fifth]

        waiting, rest = None, []
        for d in order:
            if d == 0:
                own.wait()
            else:
                z_copies[d].wait_recv()
            to_near = [send(d, 0, near, 0, tp_id), None]
            to_far = [None, send(d, 1, far, 3, tp_id)]
            to_near[1] = send(d, 1, near, 1, tp_id)
            to_far[0] = send(d, 0, far, 2, tp_id)
            if waiting is not None:
                rest += relay(waiting)
            waiting = (d, to_near, to_far)
        rest += relay(waiting)
        for copy in rest:
            copy.wait_recv()
    else:
        for d in order:
            if d == 0:
                own.wait()
            else:
                z_copies[d].wait_recv()
            for t in range(1, tp):
                copy = remote(
                    place(source_of(d), tp_id),
                    place(source_of(d), tp_id),
                    t_send.at[d, t],
                    t_recv.at[d, t],
                    sp_id,
                    lax.rem(tp_id + t, tp),
                )
                copy.start()
                started.append(copy)
        for copy in started:
            copy.wait_recv()
    for copy in started:
        copy.wait_send()
    for d in order[1:]:
        z_copies[d].wait_send()


def return_kernel(sp, tp, x_ref, out_ref, landed, turned, summed, t_send, t_recv, z_send, z_recv):
    cap = x_ref.shape[0] // sp
    width = out_ref.shape[1]
    half = cap // 2
    sp_id, tp_id = lax.axis_index("sp"), lax.axis_index("tp")
    greet(
        [(lax.rem(sp_id + d, sp), tp_id) for d in range(1, sp)]
        + [(sp_id, lax.rem(tp_id + d, tp)) for d in range(1, tp)]
    )

    def rows_at(target, part=None):
        first = target * cap
        if part is not None:
            first = first + part * half
        return pl.ds(pl.multiple_of(first, half), cap if part is None else half)

    def columns(owner):
        return pl.ds(pl.multiple_of(owner * width, width), width)

    order = near_first(sp)[::-1]
    started, z_copies = [], []

    def push(src, dst, d, slot, target):
        copy = remote(src, dst, t_send.at[d, slot], t_recv.at[d, slot], sp_id, target)
        copy.start()
        started.append(copy)
        return copy

    def deliver(d, target):
        if d == 0:
            return
        copy = remote(
            summed.at[d], out_ref.at[rows_at(sp_id), :], z_send.at[d], z_recv.at[d], target, tp_id
        )
        copy.start()
        z_copies.append(copy)

    def f32(value):
        return value.astype(jnp.float32)

    def place_sum(d, part, value):
        piece = pl.ds(part * half, half)
        summed[d, piece, :] = value.astype(jnp.bfloat16)
        if d == 0:
            out_ref[rows_at(sp_id, part), :] = value.astype(jnp.bfloat16)

    targets = {d: lax.rem(sp_id + d, sp) for d in order}
    if tp == 4:
        near, far, across = square(tp_id)
        first = {}

        def open_block(d):
            target = targets[d]
            first[d] = [
                push(x_ref.at[rows_at(target, 0), columns(across)], landed.at[d, 1], d, 1, near),
                push(x_ref.at[rows_at(target, 1), columns(across)], landed.at[d, 3], d, 3, far),
                push(x_ref.at[rows_at(target, 0), columns(near)], landed.at[d, 0], d, 0, near),
                push(x_ref.at[rows_at(target, 1), columns(far)], landed.at[d, 2], d, 2, far),
            ]

        second = {}

        def turn_block(d):
            target = targets[d]
            first[d][0].wait_recv()
            turned[d, 0] = (f32(x_ref[rows_at(target, 0), columns(far)]) + f32(landed[d, 1])).astype(jnp.bfloat16)
            first[d][1].wait_recv()
            turned[d, 1] = (f32(x_ref[rows_at(target, 1), columns(near)]) + f32(landed[d, 3])).astype(jnp.bfloat16)
            second[d] = [
                push(turned.at[d, 0], landed.at[d, 4], d, 4, far),
                push(turned.at[d, 1], landed.at[d, 5], d, 5, near),
            ]

        def close_block(d):
            target = targets[d]
            first[d][2].wait_recv()
            second[d][0].wait_recv()
            place_sum(d, 0, f32(x_ref[rows_at(target, 0), columns(tp_id)]) + f32(landed[d, 0]) + f32(landed[d, 4]))
            first[d][3].wait_recv()
            second[d][1].wait_recv()
            place_sum(d, 1, f32(x_ref[rows_at(target, 1), columns(tp_id)]) + f32(landed[d, 2]) + f32(landed[d, 5]))
            deliver(d, target)

        count = len(order)
        for i in range(count + 2):
            if i < count:
                open_block(order[i])
            if 0 <= i - 1 < count:
                turn_block(order[i - 1])
            if 0 <= i - 2 < count:
                close_block(order[i - 2])
    else:
        pushed = {}
        for d in order:
            pushed[d] = []
            for t in range(1, tp):
                owner = lax.rem(tp_id + t, tp)
                for part in range(2):
                    slot = 2 * (t - 1) + part
                    pushed[d].append(
                        push(x_ref.at[rows_at(targets[d], part), columns(owner)], landed.at[d, slot], d, slot, owner)
                    )
        for d in order:
            for part in range(2):
                value = f32(x_ref[rows_at(targets[d], part), columns(tp_id)])
                for t in range(1, tp):
                    pushed[d][2 * (t - 1) + part].wait_recv()
                    value = value + f32(landed[d, 2 * (t - 1) + part])
                place_sum(d, part, value)
            deliver(d, targets[d])
    for copy in started:
        copy.wait_send()
    for copy in z_copies:
        copy.wait()


def attention_kernel(
    groups,
    start_ref,
    joined_ref,
    nope_ref,
    rope_ref,
    key_major_ref,
    value_major_ref,
    key_minor_ref,
    value_minor_ref,
    out_major_ref,
    out_minor_ref,
    key_a,
    value_a,
    key_b,
    value_b,
):
    latent = key_major_ref.shape[0]
    tok_rows = nope_ref.shape[1]
    rows_f = joined_ref[:, :latent]
    tail = joined_ref[:, latent:]
    for kept, weight in (
        (key_a, key_major_ref),
        (value_a, value_major_ref),
        (key_b, key_minor_ref),
        (value_b, value_minor_ref),
    ):
        kept[...] = jnp.dot(rows_f, weight[...], preferred_element_type=jnp.float32).astype(jnp.bfloat16)
    total_keys = joined_ref.shape[0]
    shape = (tok_rows, total_keys)
    visible = lax.broadcasted_iota(jnp.int32, shape, 1) <= start_ref[0] + lax.broadcasted_iota(jnp.int32, shape, 0)
    contract = (((1,), (1,)), ((), ()))
    index = 0
    for kept_key, kept_value, out_ref, heads, pack, scale in (
        (key_a, value_a, out_major_ref, *groups[0]),
        (key_b, value_b, out_minor_ref, *groups[1]),
    ):
        tile = kept_key.shape[1] // (-(-heads // pack))
        lanes = lax.broadcasted_iota(jnp.int32, (tok_rows, tile), 1)
        for first in range(0, heads, pack):
            columns = pl.ds(first // pack * tile, tile)
            result = None
            for member in range(min(pack, heads - first)):
                scores = lax.dot_general(
                    nope_ref[index], kept_key[:, columns], contract, preferred_element_type=jnp.float32
                ) + lax.dot_general(rope_ref[index], tail, contract, preferred_element_type=jnp.float32)
                scores = jnp.where(visible, scores * scale, -jnp.inf)
                weights = jnp.exp(scores - jnp.max(scores, axis=1, keepdims=True))
                totals = jnp.sum(weights, axis=1, keepdims=True)
                summed = jnp.dot(
                    weights.astype(jnp.bfloat16), kept_value[:, columns], preferred_element_type=jnp.float32
                ) / totals
                result = summed if result is None else jnp.where(lanes < member * (tile // pack), result, summed)
                index += 1
            out_ref[:, columns] = result.astype(jnp.bfloat16)


def expert_kernel(x_ref, gain_ref, gate_ref, up_ref, down_ref, out_ref, normed, total):
    step = pl.program_id(0)

    @pl.when(step == 0)
    def _():
        rows_f = x_ref[...].astype(jnp.float32)
        power = jnp.mean(rows_f * rows_f, axis=1, keepdims=True)
        normed[...] = (rows_f * lax.rsqrt(power + norm_eps) * gain_ref[...]).astype(jnp.bfloat16)

    rows = normed[...]
    gate_pre = jnp.dot(rows, gate_ref[0], preferred_element_type=jnp.float32)
    up_pre = jnp.dot(rows, up_ref[0], preferred_element_type=jnp.float32)
    hidden = (gate_pre / (1.0 + jnp.exp(-gate_pre)) * up_pre).astype(jnp.bfloat16)
    part = jnp.dot(hidden, down_ref[0], preferred_element_type=jnp.float32)
    last = pl.num_programs(0) - 1

    @pl.when((step == 0) & (last > 0))
    def _():
        total[...] = part

    @pl.when((step > 0) & (step < last))
    def _():
        total[...] += part

    @pl.when((step == last) & (last > 0))
    def _():
        out_ref[...] = (total[...] + part).astype(jnp.bfloat16)

    @pl.when(last == 0)
    def _():
        out_ref[...] = part.astype(jnp.bfloat16)


def flip(index, offset):
    step = 1
    while step <= offset:
        if offset & step:
            index = index + step * (1 - 2 * lax.rem(index // step, 2))
        step *= 2
    return index


def rope_table(count, width):
    half_width = width // 2
    inverse_freq = (1.0 / theta_base ** (np.arange(half_width, dtype=np.float32) * (2.0 / width))).astype(np.float32)
    angles = np.arange(count, dtype=np.float32)[:, None] * inverse_freq[None, :]
    cosine, sine = np.cos(angles), np.sin(angles)
    return np.concatenate([cosine, cosine, -sine, sine], axis=1).astype(np.float32)


def orders(chips):
    if chips != 4:
        return [tuple(range(chips))] * chips
    return [(0, 1, 2, 3), (0, 1, 2, 3), (0, 1, 3, 2), (0, 1, 2, 3)]


def plans(chips):
    last = chips - 1
    simple = {"streamed": [("open", 0), ("relay", 0)]}
    for k in range(last):
        simple[f"between {k}"] = [("open", k + 1)]
        simple[f"after {k}"] = [("relay", k + 1)] + ([("turn", k - 1)] if k else [])
    simple[f"after {last}"] = [("turn", last - 1)] if last else []
    simple[f"after {last}"] += [("turn", last)] + [("close", k) for k in range(chips)]
    if chips != 4:
        return [simple] * chips
    ending = {
        "between 3": [("turn", 2)],
        "after 3": [("send", 1), ("close", 2), ("turn", 3), ("close", 3), ("turn", 1), ("close", 1)],
    }
    bottom = {
        "streamed": [("open", 0), ("relay", 0)],
        "between 0": [("open", 1)],
        "after 0": [("relay", 1), ("turn", 0)],
        "between 1": [("close", 0), ("open", 2)],
        "after 1": [("open", 3), ("relay", 2)],
        "between 2": [("relay", 3), ("turn", 1)],
        "after 2": [("close", 1)],
        "between 3": [("turn", 2)],
        "after 3": [("close", 2), ("turn", 3), ("close", 3)],
    }
    lower = {
        "streamed": [("open", 0), ("open", 1), ("relay", 0)],
        "between 0": [("relay", 1), ("open", 2)],
        "between 1": [("open", 3), ("relay", 2), ("turn", 0)],
        "between 2": [("relay", 3)],
        "after 2": [("close", 0)],
    }
    upper = {
        "pushed": [("open", 0)],
        "streamed": [("relay", 0), ("open", 1), ("open", 2)],
        "between 0": [("relay", 1)],
        "after 0": [("relay", 2)],
        "between 1": [("open", 3), ("turn", 0)],
        "after 1": [("relay", 3), ("close", 0)],
        "between 2": [("turn", 1)],
        "after 2": [("close", 1)],
        "between 3": [("turn", 3)],
        "after 3": [("close", 3), ("turn", 2), ("close", 2)],
    }
    top = {
        "pushed": [("open", 0)],
        "streamed": [("relay", 0), ("open", 1), ("open", 3), ("open", 2)],
        "between 0": [("relay", 1)],
        "after 0": [("relay", 3)],
        "between 1": [("relay", 2), ("turn", 0)],
        "after 1": [("close", 0)],
        "between 2": [("turn", 1)],
        "after 2": [("close", 1)],
        "between 3": [("turn", 2)],
        "after 3": [("close", 2), ("turn", 3), ("close", 3)],
    }
    return [bottom, lower | ending, upper, top]


def layer_kernel(
    sp,
    heads,
    q_major_ref,
    q_minor_ref,
    latent_ref,
    rope_ref,
    table_ref,
    key_major_ref,
    value_major_ref,
    key_minor_ref,
    value_minor_ref,
    out_major_ref,
    out_minor_ref,
    res_ref,
    ids_ref,
    mix_ref,
    gain_ref,
    gate_ref,
    up_ref,
    down_ref,
    out_ref,
    q_major,
    q_minor,
    rope_raw,
    table,
    weights,
    projection,
    residual,
    ids,
    mix,
    gain,
    gate,
    up,
    down,
    blocks,
    queries,
    kept,
    tops,
    scores,
    chances,
    fades,
    gathered_out,
    mixed,
    spread_part,
    spread_landed,
    spread_turned,
    stream,
    select,
    hot,
    mix_column,
    placed,
    rows_in,
    normed,
    hidden,
    part,
    landed,
    turned,
    summed,
    returned,
    load_sem,
    expert_sem,
    l_send,
    l_recv,
    q_send,
    q_recv,
    s_send,
    s_recv,
    o_send,
    o_recv,
    z_send,
    z_recv,
    t_send,
    t_recv,
    r_send,
    r_recv,
    y_send,
    y_recv,
):
    heads_major, heads_minor = heads
    tok_rows, latent = latent_ref.shape
    rope_width = rope_ref.shape[0]
    chips = sp // 2
    tp = 4
    quarter = tok_rows // tp
    pack = 128 // NOPE_MINOR
    sp_id, tp_id = lax.axis_index("sp"), lax.axis_index("tp")
    level, core = sp_id // 2, lax.rem(sp_id, 2)
    sibling = flip(sp_id, 1)
    near, far, across = square(tp_id)
    f32, bf16 = jnp.float32, jnp.bfloat16

    loads = []

    def load(src, dst):
        copy = pltpu.make_async_copy(src, dst, load_sem.at[len(loads)])
        copy.start()
        loads.append(copy)
        return copy

    own_rows = pl.ds(pl.multiple_of(sp_id * tok_rows, tok_rows), tok_rows)
    early = [
        load(latent_ref, blocks.at[0, 0, :, pl.ds(0, latent)]),
        load(rope_ref, rope_raw),
        load(table_ref.at[own_rows, :], table),
    ]
    asked = [load(q_major_ref, q_major), load(q_minor_ref, q_minor)]
    spans, first = [], 0
    for ref in (key_major_ref, key_minor_ref, value_major_ref, value_minor_ref):
        span = pl.ds(first, ref.shape[1])
        asked.append(load(ref, weights.at[:, span]))
        spans.append(span)
        first += ref.shape[1]
    split = out_major_ref.shape[0]
    routing = [load(ids_ref, ids), load(mix_ref, mix), load(gain_ref, gain)]
    late = [
        load(out_major_ref, projection.at[pl.ds(0, split), :]),
        load(out_minor_ref, projection.at[pl.ds(split, out_minor_ref.shape[0]), :]),
        load(res_ref, residual),
    ]

    barrier = pltpu.get_barrier_semaphore()
    for offset in range(1, sp):
        pl.semaphore_signal(barrier, inc=1, device_id=(flip(sp_id, offset), tp_id), device_id_type=MESH)
    for peer in (near, far, across):
        pl.semaphore_signal(barrier, inc=1, device_id=(sp_id, peer), device_id_type=MESH)

    lane = lax.broadcasted_iota(jnp.int32, (tok_rows, 128), 1)
    low = lane < rope_width

    def rotator(cosine, back, ahead):
        def rotate(x):
            return x * cosine + pltpu.roll(x, 128 - rope_width // 2, 1) * back + pltpu.roll(x, rope_width // 2, 1) * ahead

        return rotate

    for copy in early:
        copy.wait()
    trig = table[...]
    flipped = pltpu.roll(trig, 64, 1)
    half = rope_width // 2
    rotate_low = rotator(
        jnp.where(low, trig, 1.0),
        jnp.where(lane < half, flipped, 0.0),
        jnp.where((lane >= half) & low, flipped, 0.0),
    )
    rotate_high = rotator(
        jnp.where(low, 1.0, flipped),
        jnp.where(low | (lane >= 64 + half), 0.0, trig),
        jnp.where(lane >= 64 + half, trig, 0.0),
    )
    raw = rope_raw[...].astype(f32)
    raw = jnp.concatenate([raw, jnp.zeros((128 - rope_width, tok_rows), f32)], axis=0).T
    blocks[0, 0, :, latent:] = rotate_low(raw).astype(bf16)
    pl.semaphore_wait(barrier, sp - 1 + 3)

    own_quarter = pl.ds(pl.multiple_of(tp_id * quarter, quarter), quarter)

    def lift(d):
        return remote(
            blocks.at[0, 0, own_quarter, :],
            blocks.at[d, 0, own_quarter, :],
            l_send.at[d],
            l_recv.at[d],
            sp_id + 2 * d,
            tp_id,
        )

    def spread(d, slot):
        place = blocks.at[d, 0, own_quarter, :]
        return remote(place, place, q_send.at[d, slot], q_recv.at[d, slot], sp_id, (near, far, across)[slot])

    def share(d):
        return remote(blocks.at[d, 0], blocks.at[d, 1], s_send.at[d], s_recv.at[d], sibling, tp_id)

    for d in range(1, chips):

        @pl.when(level + d < chips)
        def _():
            lift(d).start()

    share(0).start()

    for copy in asked:
        copy.wait()
    pieces = 4
    for index, (src, dst) in enumerate(((gate_ref, gate), (up_ref, up), (down_ref, down))):
        count = dst.shape[0] // pieces
        for piece in range(pieces):
            span = pl.ds(piece * count, count)
            copy = pltpu.make_async_copy(src.at[0, span, :], dst.at[span, :], expert_sem.at[index])
            copy.start()
    def column(ref, index):
        return ref[:, index * 128 : index * 128 + 128].astype(f32)

    def only_low(x):
        return jnp.where(low, x, 0.0).astype(bf16)

    for pair in range(heads_major // 2):
        one, two = column(q_major, 3 * pair + 1), column(q_major, 3 * pair + 2)
        queries[2 * pair, :, :128] = q_major[:, pair * 384 : pair * 384 + 128]
        queries[2 * pair, :, 128:] = only_low(rotate_low(one))
        queries[2 * pair + 1, :, :128] = jnp.where(low, pltpu.roll(one, 64, 1), pltpu.roll(two, 64, 1)).astype(bf16)
        queries[2 * pair + 1, :, 128:] = only_low(pltpu.roll(rotate_high(two), 64, 1))
    for h in range(heads_minor):
        whole = rotate_high(column(q_minor, h))
        moved = pltpu.roll(whole, 64, 1)
        queries[heads_major + h, :, 128:] = only_low(moved)
        if h % pack == 0:
            queries[heads_major + h, :, :128] = only_low(whole)
        else:
            queries[heads_major + h, :, :128] = jnp.where(low, 0.0, moved).astype(bf16)

    keys = 2 * tok_rows
    log2e = 1.4426950408889634
    contract = (((1,), (1,)), ((), ()))

    def project(d, q):
        span = pl.ds(q * tok_rows, tok_rows)
        rows = blocks[d, q, :, :latent]
        kept[d, span, :] = jnp.dot(rows, weights[...], preferred_element_type=f32).astype(bf16)

    everyone = range(heads_major + heads_minor)

    def tile_of(h):
        return h if h < heads_major else (h - heads_major) // pack

    def attend(d):
        tails = jnp.concatenate([blocks[d, 0, :, latent:], blocks[d, 1, :, latent:]], axis=0)
        for h in everyone:
            nope = NOPE_MAJOR if h < heads_major else NOPE_MINOR
            key_at = tile_of(h) * 128 + (0 if h < heads_major else spans[1].start)
            key = jnp.concatenate([kept[d, :, key_at : key_at + 128], tails], axis=1)
            scale = (nope + rope_width) ** (-0.5) * log2e
            value = lax.dot_general(queries[h], key, contract, preferred_element_type=f32) * scale
            if d == 0:
                spot = lax.broadcasted_iota(jnp.int32, (tok_rows, keys), 1)
                row = lax.broadcasted_iota(jnp.int32, (tok_rows, keys), 0)
                limit = jnp.where(spot < tok_rows, row, keys * core - 1)
                value = jnp.where(spot <= limit, value, -jnp.inf)
            scores[h] = value
        for h in everyone:
            value = scores[h]
            peak = jnp.max(value, axis=1, keepdims=True)
            if d > 0:
                before = tops[h][:, :1]
                peak = jnp.maximum(before, peak)
                fades[h] = jnp.broadcast_to(jnp.exp2(before - peak), (tok_rows, 128))
            chances[h] = jnp.exp2(value - peak).astype(bf16)
            tops[h] = jnp.broadcast_to(peak, (tok_rows, 128))
        ones = jnp.ones((keys, 128), bf16)
        for h in everyone:
            value_at = tile_of(h) * 128 + (spans[2].start if h < heads_major else spans[3].start)
            value = jnp.concatenate([kept[d, :, value_at : value_at + 128], ones], axis=1)
            summed = jnp.dot(chances[h], value, preferred_element_type=f32)
            if d == 0:
                gathered_out[h] = summed
            else:
                fade = fades[h]
                gathered_out[h, :, :128] = summed[:, :128] + gathered_out[h, :, :128] * fade
                gathered_out[h, :, 128:] = summed[:, 128:] + gathered_out[h, :, 128:] * fade

    slots = placed.shape[0]
    cap = slots // sp
    width = stream.shape[1]

    def prepare_routing():
        for copy in routing:
            copy.wait()
        lanes = lax.broadcasted_iota(jnp.int32, (sp, tok_rows), 0)
        matches = [(lanes == ids[j : j + 1, :]).astype(f32) for j in range(TOP)]
        order = (tok_rows, tok_rows)
        before = lax.broadcasted_iota(jnp.int32, order, 0) < lax.broadcasted_iota(jnp.int32, order, 1)
        named = functools.reduce(lambda a, b: a + b, matches)
        earlier = jnp.dot(named.astype(bf16), before.astype(bf16), preferred_element_type=f32)
        slot_rows = lax.broadcasted_iota(jnp.int32, (slots, tok_rows), 0)
        either = None
        for j in range(TOP):
            rank = jnp.sum(matches[j] * earlier, axis=0, keepdims=True).astype(jnp.int32)
            earlier = earlier + matches[j]
            chosen = jnp.where(slot_rows == ids[j : j + 1, :] * cap + rank, 1.0, 0.0)
            hot[j] = chosen.T.astype(bf16)
            mix_column[j] = jnp.broadcast_to(mix[j : j + 1, :], order).T
            either = chosen if either is None else either + chosen
        select[...] = either.astype(bf16)

    def columns(owner):
        return pl.ds(pl.multiple_of(owner * width, width), width)

    def arrival(place, sem):
        return pltpu.make_async_copy(place, place, sem)

    own_columns = columns(tp_id)

    def block(index):
        return pl.ds(pl.multiple_of(index * cap, cap), cap)

    def ends(target_level, q):
        return 2 * target_level + flip(core, q)

    def handoff(k, q, target_level):
        return remote(
            placed.at[block(ends(target_level, q)), :],
            rows_in.at[level, pl.ds(q * cap, cap), own_columns],
            z_send,
            z_recv.at[level, q],
            ends(target_level, q),
            tp_id,
        )

    parts = {0: (0, 0, 0), 1: (1, 0, 0), 2: (0, 0, 1), 3: (1, 0, 1), 4: (0, 1, 1), 5: (1, 1, 0)}

    def pass_on(k, slot):
        q, borrowed, to_far = parts[slot]
        owner = tp_id
        if borrowed:
            owner = near if slot == 4 else far
        place = rows_in.at[k, pl.ds(q * cap, cap), columns(owner)]
        target = far if to_far else near
        return remote(place, place, t_send, t_recv.at[k, slot], sp_id, target)

    def open_chunk(k):
        @pl.when(level != k)
        def _():
            arrival(rows_in.at[k, pl.ds(0, cap), own_columns], z_recv.at[k, 0]).wait()

        pass_on(k, 0).start()
        pass_on(k, 2).start()
        arrival(rows_in.at[k, pl.ds(cap, cap), own_columns], z_recv.at[k, 1]).wait()
        pass_on(k, 3).start()
        pass_on(k, 1).start()

    def relay(k):
        pass_on(k, 0).wait_recv()
        pass_on(k, 4).start()
        pass_on(k, 3).wait_recv()
        pass_on(k, 5).start()

    def push(k, slot):
        src, target = {
            0: (part.at[k, pl.ds(0, cap), columns(near)], near),
            1: (part.at[k, pl.ds(0, cap), columns(across)], near),
            2: (part.at[k, pl.ds(cap, cap), columns(far)], far),
            3: (part.at[k, pl.ds(cap, cap), columns(across)], far),
            4: (turned.at[k, 0], far),
            5: (turned.at[k, 1], near),
        }[slot]
        return remote(src, landed.at[k, slot], r_send, r_recv.at[k, slot], sp_id, target)

    def wide(value):
        return value.astype(f32)

    def turn(k):
        push(k, 1).wait_recv()
        turned[k, 0] = (wide(part[k, :cap, columns(far)]) + wide(landed[k, 1])).astype(bf16)
        push(k, 4).start()
        push(k, 3).wait_recv()
        turned[k, 1] = (wide(part[k, cap:, columns(near)]) + wide(landed[k, 3])).astype(bf16)
        push(k, 5).start()

    def back(k, q):
        return remote(
            summed.at[k, q],
            returned.at[block(sp_id), :],
            y_send,
            y_recv.at[level, q],
            ends(k, q),
            tp_id,
        )

    def close(k):
        for q in range(2):
            push(k, 2 * q).wait_recv()
            push(k, 4 + q).wait_recv()
            value = wide(part[k, q * cap : q * cap + cap, own_columns])
            value = (value + wide(landed[k, 2 * q]) + wide(landed[k, 4 + q])).astype(bf16)
            summed[k, q] = value
            if q == 1:
                back(k, q).start()
                continue

            @pl.when(level == k)
            def _():
                returned[block(sp_id), :] = summed[k, 0]

            @pl.when(level != k)
            def _():
                back(k, 0).start()

    def send(k):
        for slot in (1, 3, 0, 2):
            push(k, slot).start()

    actions = {"send": send, "open": open_chunk, "relay": relay, "turn": turn, "close": close}

    def run(point):
        for here, plan in enumerate(plans(chips)):
            events = plan.get(point, ())
            if events:

                @pl.when(level == here)
                def _():
                    for action, k in events:
                        actions[action](k)

    def forward(d):
        @pl.when(level >= d)
        def _():
            arrival(blocks.at[d, 0, own_quarter, :], l_recv.at[d]).wait()
            for slot in range(3):
                spread(d, slot).start()

    for d in range(1, chips // 2):
        forward(d)
    project(0, 0)
    share(0).wait_recv()
    project(0, 1)
    for d in range(chips // 2, chips - 1):
        forward(d)
    attend(0)
    forward(chips - 1)
    def collect(d):
        @pl.when(level >= d)
        def _():
            for slot in range(3):
                spread(d, slot).wait_recv()
            share(d).start()
            project(d, 0)

    def process(d):
        @pl.when(level >= d)
        def _():
            share(d).wait_recv()
            project(d, 1)
            attend(d)

    collect(1)
    prepare_routing()
    process(1)
    for d in range(2, chips):
        collect(d)
    for d in range(2, chips):
        process(d)

    def share_of(h):
        return gathered_out[h, :, :128] / gathered_out[h, :, 128:]

    for h in range(heads_major):
        mixed[:, h * 128 : h * 128 + 128] = share_of(h).astype(bf16)
    for tile in range(-(-heads_minor // pack)):
        result = None
        for member in range(min(pack, heads_minor - tile * pack)):
            h = heads_major + tile * pack + member
            value = share_of(h)
            result = value if result is None else jnp.where(lane < member * NOPE_MINOR, result, value)
        first = (heads_major + tile) * 128
        mixed[:, first : first + 128] = result.astype(bf16)

    for copy in late:
        copy.wait()

    mid = tok_rows // 2
    mids = (pl.ds(0, mid), pl.ds(mid, mid))
    rows = mixed[...]

    def fill_out(owner):
        spread_part[:, columns(owner)] = jnp.dot(rows, projection[:, columns(owner)], preferred_element_type=f32).astype(bf16)

    def push_out(src, slot, target):
        copy = remote(src, spread_landed.at[slot], o_send, o_recv.at[slot], sp_id, target)
        copy.start()
        return copy

    fill_out(across)
    second = push_out(spread_part.at[mids[0], columns(across)], 1, near)
    fourth = push_out(spread_part.at[mids[1], columns(across)], 3, far)
    fill_out(near)
    first = push_out(spread_part.at[mids[0], columns(near)], 0, near)
    fill_out(far)
    third = push_out(spread_part.at[mids[1], columns(far)], 2, far)
    fill_out(tp_id)
    second.wait_recv()
    spread_turned[0] = (spread_part[mids[0], columns(far)].astype(f32) + spread_landed[1].astype(f32)).astype(bf16)
    fifth = push_out(spread_turned.at[0], 4, far)
    fourth.wait_recv()
    spread_turned[1] = (spread_part[mids[1], columns(near)].astype(f32) + spread_landed[3].astype(f32)).astype(bf16)
    sixth = push_out(spread_turned.at[1], 5, near)
    run("pushed")
    for q, plain, bent in ((0, first, fifth), (1, third, sixth)):
        plain.wait_recv()
        value = spread_part[mids[q], columns(tp_id)].astype(f32) + residual[mids[q], :].astype(f32)
        value = value + spread_landed[2 * q].astype(f32)
        bent.wait_recv()
        stream[mids[q], :] = (value + spread_landed[4 + q].astype(f32)).astype(bf16)

    units = gate.shape[1]
    placed[...] = jnp.dot(select[...], stream[...], preferred_element_type=f32).astype(bf16)

    handoff(0, 1, level).start()

    for k in range(chips - 1, 0, -1):
        for q in range(2):
            handoff(k, q, flip(level, k)).start()
    rows_in[level, 0:cap, own_columns] = placed[block(sp_id), :]

    def ready(k):
        for slot in (1, 2, 4, 5):
            pass_on(k, slot).wait_recv()
        rows = rows_in[k].astype(f32)
        power = jnp.mean(rows * rows, axis=1, keepdims=True)
        normed[...] = (rows * lax.rsqrt(power + norm_eps) * gain[...]).astype(bf16)

    def expand():
        tile = 256
        rows = normed[...]
        for first in range(0, units, tile):
            span = slice(first, first + tile)
            gate_pre = jnp.dot(rows, gate[:, span], preferred_element_type=f32)
            up_pre = jnp.dot(rows, up[:, span], preferred_element_type=f32)
            hidden[:, span] = (gate_pre / (1.0 + jnp.exp(-gate_pre)) * up_pre).astype(bf16)

    def contract(k, late):
        rows = hidden[...]

        def fill(owner):
            part[k, :, columns(owner)] = jnp.dot(
                rows, down[:, columns(owner)], preferred_element_type=f32
            ).astype(bf16)

        def leave(*chosen):
            def start():
                for slot in chosen:
                    push(k, slot).start()

            if late:
                pl.when(level != 1)(start)
            else:
                start()

        fill(across)
        leave(1, 3)
        fill(near)
        leave(0)
        fill(far)
        leave(2)
        fill(tp_id)

    run("streamed")
    for index, ref in enumerate((gate, up, down)):
        arrival(ref, expert_sem.at[index]).wait()
    choices = orders(chips)
    for step in range(chips):
        k = choices[0][step]
        for here in range(1, chips):
            k = jnp.where(level == here, choices[here][step], k)
        ready(k)
        expand()
        run(f"between {step}")
        contract(k, chips == 4 and step == 1)
        run(f"after {step}")

    total = stream[...].astype(f32)
    for k in range(chips):
        source = flip(level, k)
        for q in range(2):
            if k > 0 or q > 0:
                arrival(returned.at[block(ends(source, q)), :], y_recv.at[source, q]).wait()
        span = pl.ds(pl.multiple_of(source * 2 * cap, 2 * cap), 2 * cap)
        for j in range(TOP):
            picked = jnp.dot(hot[j, :, span], returned[span, :], preferred_element_type=f32)
            total = total + picked * mix_column[j][:, :1]
    out_ref[...] = total
    arrival(landed, t_send).wait()
    arrival(landed, r_send).wait()
    sent = pl.ds(0, (sp - 1) * cap)
    arrival(returned.at[sent, :], z_send).wait()
    arrival(returned.at[sent, :], y_send).wait()
    arrival(spread_landed, o_send).wait()
    share(0).wait_send()
    for d in range(1, chips):

        @pl.when(level + d < chips)
        def _():
            lift(d).wait_send()

        @pl.when(level >= d)
        def _():
            share(d).wait_send()
            for slot in range(3):
                spread(d, slot).wait_send()


def fused_layer(
    sp,
    tp,
    query_major,
    query_minor,
    latent_rows,
    rope_keys,
    key_up_major,
    value_up_major,
    key_up_minor,
    value_up_minor,
    out_major,
    out_minor,
    residual,
    norm_gain,
    expert_ids,
    expert_weights,
    gate_proj,
    up_proj,
    down_proj,
):
    tok_rows, latent = latent_rows.shape
    rope_width = rope_keys.shape[1]
    width = residual.shape[1]
    features = tp * width
    units = gate_proj.shape[2]
    chips = sp // 2
    cap = 2 * tok_rows * TOP // sp
    slots = sp * cap
    heads = (key_up_major.shape[1] // NOPE_MAJOR, key_up_minor.shape[1] // NOPE_MINOR)
    count = heads[0] + heads[1]
    joined = latent + rope_width + -(latent + rope_width) % 128
    kept = key_up_major.shape[1] + key_up_minor.shape[1] + value_up_major.shape[1] + value_up_minor.shape[1]
    mixed = value_up_major.shape[1] + value_up_minor.shape[1]
    dma = pltpu.SemaphoreType.DMA
    bf16, f32 = jnp.bfloat16, jnp.float32
    table = jnp.asarray(rope_table(sp * tok_rows, rope_width))
    operands = (
        query_major,
        query_minor,
        latent_rows,
        rope_keys.T,
        table,
        key_up_major,
        value_up_major,
        key_up_minor,
        value_up_minor,
        out_major,
        out_minor,
        residual,
        expert_ids.T,
        expert_weights.T,
        norm_gain.reshape(1, -1),
        gate_proj,
        up_proj,
        down_proj,
    )
    vmem = pltpu.VMEM
    return pl.pallas_call(
        functools.partial(layer_kernel, sp, heads),
        out_shape=pltpu.VMEM((tok_rows, width), f32),
        in_specs=[pl.BlockSpec(memory_space=pl.ANY)] * len(operands),
        out_specs=pl.BlockSpec(memory_space=pltpu.VMEM),
        scratch_shapes=[
            vmem(query_major.shape, bf16),
            vmem(query_minor.shape, bf16),
            vmem((rope_width, tok_rows), bf16),
            vmem((tok_rows, 2 * rope_width), f32),
            vmem((latent, kept), bf16),
            vmem((mixed, features), bf16),
            vmem(residual.shape, bf16),
            vmem((TOP, tok_rows), jnp.int32),
            vmem((TOP, tok_rows), f32),
            vmem((1, features), f32),
            vmem((features, units), bf16),
            vmem((features, units), bf16),
            vmem((units, features), bf16),
            vmem((chips, 2, tok_rows, joined), bf16),
            vmem((count, tok_rows, 256), bf16),
            vmem((chips, 2 * tok_rows, kept), bf16),
            vmem((count, tok_rows, 128), f32),
            vmem((count, tok_rows, 2 * tok_rows), f32),
            vmem((count, tok_rows, 2 * tok_rows), bf16),
            vmem((count, tok_rows, 128), f32),
            vmem((count, tok_rows, 256), f32),
            vmem((tok_rows, mixed), bf16),
            vmem((tok_rows, features), bf16),
            vmem((6, tok_rows // 2, width), bf16),
            vmem((2, tok_rows // 2, width), bf16),
            vmem((tok_rows, width), bf16),
            vmem((slots, tok_rows), bf16),
            vmem((TOP, tok_rows, slots), bf16),
            vmem((TOP, tok_rows, tok_rows), f32),
            vmem((slots, width), bf16),
            vmem((chips, 2 * cap, features), bf16),
            vmem((2 * cap, features), bf16),
            vmem((2 * cap, units), bf16),
            vmem((chips, 2 * cap, features), bf16),
            vmem((chips, 6, cap, width), bf16),
            vmem((chips, 2, cap, width), bf16),
            vmem((chips, 2, cap, width), bf16),
            vmem((slots, width), bf16),
            dma((len(operands),)),
            dma((3,)),
            dma((chips,)),
            dma((chips,)),
            dma((chips, 3)),
            dma((chips, 3)),
            dma((chips,)),
            dma((chips,)),
            dma,
            dma((6,)),
            dma,
            dma((chips, 2)),
            dma,
            dma((chips, 6)),
            dma,
            dma((chips, 6)),
            dma,
            dma((chips, 2)),
        ],
        compiler_params=pltpu.CompilerParams(
            collective_id=4, has_side_effects=True, vmem_limit_bytes=60 * 1024 * 1024
        ),
    )(*operands).astype(bf16)


def run_experts(rows, gain, gate_proj, up_proj, down_proj):
    slots, features = rows.shape
    units = gate_proj.shape[2]
    tile = min(256, units)
    return pl.pallas_call(
        expert_kernel,
        grid=(units // tile,),
        out_shape=jax.ShapeDtypeStruct((slots, features), jnp.bfloat16),
        in_specs=[
            pl.BlockSpec((slots, features), lambda i: (0, 0)),
            pl.BlockSpec((1, features), lambda i: (0, 0)),
            pl.BlockSpec((1, features, tile), lambda i: (0, 0, i)),
            pl.BlockSpec((1, features, tile), lambda i: (0, 0, i)),
            pl.BlockSpec((1, tile, features), lambda i: (0, i, 0)),
        ],
        out_specs=pl.BlockSpec((slots, features), lambda i: (0, 0)),
        scratch_shapes=[
            pltpu.VMEM((slots, features), jnp.bfloat16),
            pltpu.VMEM((slots, features), jnp.float32),
        ],
        compiler_params=pltpu.CompilerParams(vmem_limit_bytes=60 * 1024 * 1024),
    )(rows, gain.reshape(1, -1), gate_proj, up_proj, down_proj)


def pad_columns(array, multiple):
    return jnp.pad(array, ((0, 0), (0, -array.shape[1] % multiple)))


def per_device(
    sp,
    tp,
    query_major,
    query_minor,
    latent_rows,
    rope_keys,
    key_up_major,
    value_up_major,
    key_up_minor,
    value_up_minor,
    out_major,
    out_minor,
    residual,
    norm_gain,
    expert_ids,
    expert_weights,
    gate_proj,
    up_proj,
    down_proj,
):
    tok_rows = query_major.shape[0]
    fast = tp == 4 and sp & (sp - 1) == 0
    fast = fast and tok_rows % 64 == 0 and (2 * tok_rows * TOP // sp) % 16 == 0
    fast = fast and key_up_major.shape[1] % 128 == 0 and key_up_minor.shape[1] % 128 == 0
    if fast:
        return fused_layer(
            sp,
            tp,
            query_major,
            query_minor,
            latent_rows,
            rope_keys,
            key_up_major,
            value_up_major,
            key_up_minor,
            value_up_minor,
            out_major,
            out_minor,
            residual,
            norm_gain,
            expert_ids,
            expert_weights,
            gate_proj,
            up_proj,
            down_proj,
        )
    row_start = lax.axis_index("sp") * tok_rows
    positions = row_start + jnp.arange(tok_rows, dtype=jnp.int32)
    rope_width = rope_keys.shape[1]
    latent = latent_rows.shape[1]
    rope_rot = rotary(rope_keys, positions).astype(jnp.bfloat16)
    heads_major = key_up_major.shape[1] // NOPE_MAJOR
    heads_minor = key_up_minor.shape[1] // NOPE_MINOR
    shaped_major = query_major.reshape(tok_rows, heads_major, NOPE_MAJOR + rope_width)
    shaped_minor = query_minor.reshape(tok_rows, heads_minor, NOPE_MINOR + rope_width)
    nope_major = shaped_major[:, :, :NOPE_MAJOR]
    nope_minor = shaped_minor[:, :, :NOPE_MINOR]
    turned_major = rotary(shaped_major[:, :, NOPE_MAJOR:], positions).astype(jnp.bfloat16)
    turned_minor = rotary(shaped_minor[:, :, NOPE_MINOR:], positions).astype(jnp.bfloat16)
    scale_major = (NOPE_MAJOR + rope_width) ** (-0.5)
    scale_minor = (NOPE_MINOR + rope_width) ** (-0.5)

    joined = jnp.concatenate(
        [latent_rows, rope_rot, jnp.zeros((tok_rows, -(latent + rope_width) % 128), jnp.bfloat16)], axis=1
    )
    dma = pltpu.SemaphoreType.DMA
    chips = sp // 2
    gathered = comm_call(
        functools.partial(gather_kernel, sp),
        jax.ShapeDtypeStruct((sp * tok_rows, joined.shape[1]), jnp.bfloat16),
        [dma((chips,)), dma((chips,)), dma((chips,)), dma((chips,))],
        0,
        (joined,),
    )
    tail_width = joined.shape[1] - latent

    def by_head(array, width):
        return jnp.pad(array.transpose(1, 0, 2), ((0, 0), (0, 0), (0, width - array.shape[2])))

    pack = 128 // NOPE_MINOR
    spread = nope_minor.transpose(1, 0, 2)
    member = (jnp.arange(heads_minor, dtype=jnp.int32) % pack)[:, None, None]
    spread = jnp.concatenate(
        [jnp.where(member == m, spread, jnp.zeros_like(spread)) for m in range(pack)], axis=2
    )
    nope_all = jnp.concatenate([by_head(nope_major, 128), spread], axis=0)
    rope_all = jnp.concatenate([by_head(turned_major, tail_width), by_head(turned_minor, tail_width)], axis=0)
    minor_weights = [pad_columns(key_up_minor, 128), pad_columns(value_up_minor, 128)]
    minor_width = minor_weights[0].shape[1]
    keys = sp * tok_rows
    vmem = pl.BlockSpec(memory_space=pltpu.VMEM)
    attn_major, attn_minor = pl.pallas_call(
        functools.partial(attention_kernel, ((heads_major, 1, scale_major), (heads_minor, pack, scale_minor))),
        out_shape=(
            jax.ShapeDtypeStruct((tok_rows, value_up_major.shape[1]), jnp.bfloat16),
            jax.ShapeDtypeStruct((tok_rows, minor_width), jnp.bfloat16),
        ),
        in_specs=[pl.BlockSpec(memory_space=pltpu.SMEM)] + [vmem] * 7,
        out_specs=(vmem, vmem),
        scratch_shapes=[
            pltpu.VMEM((keys, key_up_major.shape[1]), jnp.bfloat16),
            pltpu.VMEM((keys, value_up_major.shape[1]), jnp.bfloat16),
            pltpu.VMEM((keys, minor_width), jnp.bfloat16),
            pltpu.VMEM((keys, minor_width), jnp.bfloat16),
        ],
        compiler_params=pltpu.CompilerParams(vmem_limit_bytes=60 * 1024 * 1024),
    )(
        row_start.reshape(1).astype(jnp.int32),
        gathered,
        nope_all,
        rope_all,
        key_up_major,
        value_up_major,
        *minor_weights,
    )
    attn_minor = attn_minor[:, : value_up_minor.shape[1]]
    partial_value = jnp.dot(attn_major, out_major, preferred_element_type=jnp.float32)
    partial_value = partial_value + jnp.dot(
        attn_minor, out_minor, preferred_element_type=jnp.float32
    )
    width = residual.shape[1]
    stream_mid = comm_call(
        functools.partial(reduce_kernel, tp),
        jax.ShapeDtypeStruct((tok_rows, width), jnp.bfloat16),
        [pltpu.VMEM((tp - 1, tok_rows, width), jnp.bfloat16), dma((tp - 1,)), dma((tp - 1,))],
        1,
        (partial_value.astype(jnp.bfloat16), residual),
    )
    experts = sp
    capacity = 2 * tok_rows * TOP // experts
    slots = experts * capacity
    slot_list = slot_ids(expert_ids, experts, capacity)
    slot_numbers = jnp.arange(slots, dtype=jnp.int32)
    by_slot = slot_list.T
    select = (slot_numbers[:, None] == by_slot[0][None, :]).astype(jnp.bfloat16)
    for j in range(1, TOP):
        select = select + (slot_numbers[:, None] == by_slot[j][None, :]).astype(jnp.bfloat16)
    placed = jnp.dot(select, stream_mid, preferred_element_type=jnp.float32).astype(jnp.bfloat16)
    slots_t = 6 if tp == 4 else tp
    arrived = comm_call(
        functools.partial(dispatch_kernel, sp, tp),
        jax.ShapeDtypeStruct((slots, tp * width), jnp.bfloat16),
        [dma((sp,)), dma((sp,)), dma((sp, slots_t)), dma((sp, slots_t)), dma],
        2,
        (placed,),
    )
    down_part = run_experts(arrived, norm_gain, gate_proj, up_proj, down_proj)
    pieces = 6 if tp == 4 else 2 * (tp - 1)
    half = capacity // 2
    flat_out = comm_call(
        functools.partial(return_kernel, sp, tp),
        jax.ShapeDtypeStruct((slots, width), jnp.bfloat16),
        [
            pltpu.VMEM((sp, pieces, half, width), jnp.bfloat16),
            pltpu.VMEM((sp, 2, half, width), jnp.bfloat16),
            pltpu.VMEM((sp, capacity, width), jnp.bfloat16),
            dma((sp, pieces)),
            dma((sp, pieces)),
            dma((sp,)),
            dma((sp,)),
        ],
        3,
        (down_part,),
    )
    mixed = stream_mid.astype(jnp.float32)
    for j in range(TOP):
        hot = (slot_list[:, j : j + 1] == slot_numbers[None, :]).astype(jnp.bfloat16)
        mixed = mixed + jnp.dot(hot, flat_out, preferred_element_type=jnp.float32) * expert_weights[:, j : j + 1]
    return mixed.astype(jnp.bfloat16)


def solution(mesh):
    in_specs = (
        P("sp", "tp"),
        P("sp", "tp"),
        P("sp", None),
        P("sp", None),
        P(None, "tp"),
        P(None, "tp"),
        P(None, "tp"),
        P(None, "tp"),
        P("tp", None),
        P("tp", None),
        P("sp", "tp"),
        P(),
        P("sp", None),
        P("sp", None),
        P("sp", None, "tp"),
        P("sp", None, "tp"),
        P("sp", "tp", None),
    )
    out_specs = P("sp", "tp")
    return jax.shard_map(
        functools.partial(per_device, mesh.shape["sp"], mesh.shape["tp"]),
        mesh=mesh,
        in_specs=in_specs,
        out_specs=out_specs,
        check_vma=False,
    )
```
